256 devices in a mesh: sp: 32 (over z, x), tp: 8 (over y, core).
Axes of the slice: x: 4, y: 4, z: 8, core: 2. Of those that a mesh axis runs over, the one named last changes fastest.
Arguments:
- tokens: bfloat16 [16384, 2048], P('sp', 'tp'), may hold values from -400 to 400
- lru_in: bfloat16 [2048, 1024], P(None, 'tp'), may hold values from -0.125 to 0.125
- lru_gate_in: bfloat16 [2048, 1024], P(None, 'tp'), may hold values from -0.125 to 0.125
- query_w: bfloat16 [2048, 1024], P(None, 'tp'), may hold values from -1 to 1
- key_w: bfloat16 [2048, 1024], P(None, 'tp'), may hold values from -10 to 10
- value_w: bfloat16 [2048, 1024], P(None, 'tp'), may hold values from -0.125 to 0.125
- conv_weight: bfloat16 [4, 1024], replicated, may hold values from -3 to 3
- recur_gate_w: bfloat16 [16, 64, 64], replicated, may hold values from -0.75 to 0.75
- input_gate_w: bfloat16 [16, 64, 64], replicated, may hold values from -0.75 to 0.75
- rate_param: float32 [1024], replicated, may hold values from 0 to 16
- decay_extra: float32 [16384, 1024], P('sp', 'tp'), may hold values from -2 to 0
- forget_cum: float32 [16384, 8], P('sp', 'tp'), may hold values from -1538 to 0, as said below
- out_lru: bfloat16 [1024, 2048], P('tp'), may hold values from -0.1875 to 0.1875
- out_fox: bfloat16 [1024, 2048], P('tp'), may hold values from -0.1875 to 0.1875
Outputs:
- mixed_out: bfloat16 [16384, 2048], P('sp', 'tp')
The draws below stay inside these ranges and needn't reach their ends.
Inputs may be any that keep to these rules, and one draw needn't show every extreme that they name: `forget_cum`: non-increasing along positions in every head.
All inputs are finite; a program needn't handle non-finite values.
Results may differ from the reference program's by a relative error of at most 0.014.
Values may be sent and summed in bfloat16 or wider, within the bound.
A program may use at most 64 MiB of HBM per device.

```python
import math
import jax
import jax.numpy as jnp
from jax import lax

D = 2048
LRU_W = 1024
LRU_BLOCKS = 16
BLOCK_W = 64
CONV_W = 4
FOX_HEADS = 8
HEAD_DIM = 128
FOX_W = 1024
TOKENS_PER_SHARD = 512
SEQUENCE_TOKENS = 16384


decay_sharpness = 8.0


def draw_tokens(key, part):
    random_subkeys = jax.random.split(key, 4)
    feature_scale = jnp.exp(jnp.linspace(0.0, math.log(4.0), D) + jax.random.uniform(random_subkeys[0], (D,), jnp.float32, -0.5, 0.5))
    row_scale = jnp.exp(jax.random.uniform(random_subkeys[1], (SEQUENCE_TOKENS, 1), jnp.float32, 0.0, math.log(10.0)))
    reference_level = jax.random.truncated_normal(random_subkeys[2], -4.0, 4.0, (SEQUENCE_TOKENS, D), jnp.float32)
    return (reference_level * feature_scale[None, :] * row_scale).astype(jnp.bfloat16)


def shared_query(key):
    return jax.random.truncated_normal(jax.random.fold_in(key, 11), -6.0, 6.0, (D, FOX_W), jnp.float32) * D ** (-0.5)


def draw_query_w(key, part):
    return shared_query(key).astype(jnp.bfloat16)


def draw_key_w(key, part):
    independent = jax.random.truncated_normal(jax.random.fold_in(key, 12), -6.0, 6.0, (D, FOX_W), jnp.float32) * D ** (-0.5)
    combined = 3.0 * independent
    return combined.astype(jnp.bfloat16)


def draw_rate_param(key, part):
    random_subkeys = jax.random.split(key, 3)
    ranking = jax.random.permutation(random_subkeys[0], LRU_W)
    slow_mask = ranking < LRU_W // 2
    slow_rate = jnp.exp(jax.random.uniform(random_subkeys[1], (LRU_W,), jnp.float32, math.log(0.2), math.log(0.8))) / (0.5 * decay_sharpness * SEQUENCE_TOKENS)
    fast_len = jnp.exp(jax.random.uniform(random_subkeys[2], (LRU_W,), jnp.float32, math.log(TOKENS_PER_SHARD / 16.0), math.log(TOKENS_PER_SHARD / 5.0)))
    fast_rate = 1.0 / (0.5 * decay_sharpness * fast_len)
    softplus_value = jnp.where(slow_mask, slow_rate, fast_rate)
    return -jnp.log(jnp.expm1(softplus_value))


def draw_decay_extra(key, part):
    random_subkeys = jax.random.split(key, 4)
    multiplier = jnp.exp(jax.random.uniform(random_subkeys[0], (SEQUENCE_TOKENS // TOKENS_PER_SHARD,), jnp.float32, math.log(0.4), math.log(1.6)))
    jaggedness = jax.random.uniform(random_subkeys[1], (SEQUENCE_TOKENS, LRU_W), jnp.float32, 0.2, 1.8)
    reference_level = -jnp.repeat(multiplier, TOKENS_PER_SHARD)[:, None] * jaggedness * (0.4 / SEQUENCE_TOKENS)
    spike_position = jax.random.randint(random_subkeys[2], (3,), 0, SEQUENCE_TOKENS)
    spike_penalty = jnp.log(jax.random.uniform(random_subkeys[3], (3,), jnp.float32, 0.6, 0.8))
    spike_events = jnp.zeros((SEQUENCE_TOKENS,), jnp.float32).at[spike_position].add(spike_penalty)
    return reference_level + spike_events[:, None]


def draw_forget_cum(key, part):
    random_subkeys = jax.random.split(key, 7)
    ranking = jax.random.permutation(random_subkeys[0], FOX_HEADS)
    slow_mask = ranking < FOX_HEADS // 2
    slow_rate = jnp.exp(jax.random.uniform(random_subkeys[1], (FOX_HEADS,), jnp.float32, math.log(0.3), math.log(1.0))) / SEQUENCE_TOKENS
    fast_len = jnp.exp(jax.random.uniform(random_subkeys[2], (FOX_HEADS,), jnp.float32, math.log(TOKENS_PER_SHARD / 16.0), math.log(TOKENS_PER_SHARD / 5.0)))
    head_decay_rate = jnp.where(slow_mask, slow_rate, 1.0 / fast_len)
    multiplier = jnp.exp(jax.random.uniform(random_subkeys[3], (SEQUENCE_TOKENS // TOKENS_PER_SHARD,), jnp.float32, math.log(0.4), math.log(1.6)))
    jaggedness = jax.random.uniform(random_subkeys[4], (SEQUENCE_TOKENS, FOX_HEADS), jnp.float32, 0.2, 1.8)
    spike_position = jax.random.randint(random_subkeys[5], (3,), 0, SEQUENCE_TOKENS)
    spike_penalty = jnp.log(jax.random.uniform(random_subkeys[6], (3,), jnp.float32, 0.6, 0.8))
    spike_events = jnp.zeros((SEQUENCE_TOKENS,), jnp.float32).at[spike_position].add(spike_penalty)
    logarithmic_steps = -head_decay_rate[None, :] * jnp.repeat(multiplier, TOKENS_PER_SHARD)[:, None] * jaggedness + spike_events[:, None]
    return jnp.cumsum(logarithmic_steps, axis=0)


def strengthened(values, own_key, source, target, parts, factor):
    def block_of(dim):
        return (jnp.arange(values.shape[dim]) // (values.shape[dim] // parts)).reshape((-1,) + (1,) * (values.ndim - 1 - dim))

    one_side = jax.random.permutation(own_key, parts)[block_of(target)]
    far = (block_of(target) + parts // 2) % parts
    return jnp.where((block_of(source) == one_side) | (block_of(source) == far), factor * values, values)


def block_levels(key, extent, cuts, smallest, top_value):
    level = 1.0
    for dim, parts in cuts:
        heights = jax.random.uniform(jax.random.fold_in(jax.random.fold_in(key, 6), dim), (parts,), jnp.float32, smallest / len(cuts), top_value / len(cuts))
        level = level * jnp.repeat(jnp.exp(heights), extent[dim] // parts).reshape((-1,) + (1,) * (len(extent) - 1 - dim))
    return level


def centred(own_key, extent, deviation, most, cuts=(), dtype=jnp.bfloat16):
    array = jax.random.normal(own_key, extent, jnp.float32) * deviation
    if len(cuts) > 0:
        array = block_levels(own_key, extent, cuts, -0.22, 0.18) * array
    return jnp.clip(array, min=-most, max=most).astype(dtype)


def noise_with(rng, extent, deviation, reach, shards, heavy, kind=jnp.bfloat16):
    values = deviation * jax.random.normal(rng, extent, jnp.float32)
    if shards:
        values = values * block_levels(rng, extent, shards, -0.22, 0.18)
    return jnp.clip(strengthened(values, jax.random.fold_in(rng, 3), *heavy), -reach, reach).astype(kind)


def setup_inputs(seed: int = 0) -> dict:
    streams_of = jax.random.split(jax.random.key(seed), 15)
    tokens = draw_tokens(jax.random.fold_in(streams_of[14], 71), 0)
    lru_in = centred(streams_of[1], (D, LRU_W), D ** -0.5, 0.125, ((1, 8),))
    lru_gate_in = centred(streams_of[2], (D, LRU_W), D ** -0.5, 0.125, ((1, 8),))
    query_w = draw_query_w(jax.random.fold_in(streams_of[14], 71), 0)
    key_w = draw_key_w(jax.random.fold_in(streams_of[14], 71), 0)
    value_w = centred(streams_of[5], (D, FOX_W), D ** -0.5, 0.125, ((1, 8),))
    conv_weight = centred(streams_of[6], (CONV_W, LRU_W), CONV_W ** -0.5, 3.0)
    recur_gate_w = centred(streams_of[7], (LRU_BLOCKS, BLOCK_W, BLOCK_W), BLOCK_W ** -0.5, 0.75)
    input_gate_w = centred(streams_of[8], (LRU_BLOCKS, BLOCK_W, BLOCK_W), BLOCK_W ** -0.5, 0.75)
    rate_param = draw_rate_param(jax.random.fold_in(streams_of[14], 71), 0)
    decay_extra = draw_decay_extra(jax.random.fold_in(streams_of[14], 71), 0)
    forget_cum = draw_forget_cum(jax.random.fold_in(streams_of[14], 71), 0)
    out_lru = noise_with(streams_of[12], (LRU_W, D), (LRU_W + FOX_W) ** -0.5, 0.1875, ((0, 8),), (0, 1, 8, 2.0))
    out_fox = noise_with(streams_of[13], (FOX_W, D), (LRU_W + FOX_W) ** -0.5, 0.1875, ((0, 8),), (0, 1, 8, 2.0))
    return {"tokens": tokens, "lru_in": lru_in, "lru_gate_in": lru_gate_in, "query_w": query_w, "key_w": key_w, "value_w": value_w, "conv_weight": conv_weight, "recur_gate_w": recur_gate_w, "input_gate_w": input_gate_w, "rate_param": rate_param, "decay_extra": decay_extra, "forget_cum": forget_cum, "out_lru": out_lru, "out_fox": out_fox}


decay_sharpness = 8.0
epsilon_norm = 1e-06

def combine_pairs(earlier, later):
    decay_one, state_one = earlier
    decay_two, state_two = later
    return (decay_one * decay_two, decay_two * state_one + state_two)

def reference(tokens, lru_in, lru_gate_in, query_w, key_w, value_w, conv_weight, recur_gate_w, input_gate_w, rate_param, decay_extra, forget_cum, out_lru, out_fox):
    token_f32 = tokens.astype(jnp.float32)
    row_scale = lax.rsqrt(lax.optimization_barrier(jnp.mean(token_f32 * token_f32, axis=1, keepdims=True)) + epsilon_norm)

    def project(weight):
        return (jnp.dot(tokens, weight, preferred_element_type=jnp.float32) * row_scale).astype(jnp.bfloat16)
    lru_input = project(lru_in)
    gate_input = project(lru_gate_in)
    queries = project(query_w)
    keys_all = project(key_w)
    values_all = project(value_w)
    padded = jnp.pad(lru_input, ((CONV_W - 1, 0), (0, 0)))
    conv_sum = jnp.zeros((SEQUENCE_TOKENS, LRU_W), jnp.float32)
    for tap_idx in range(CONV_W):
        conv_sum = conv_sum + conv_weight[tap_idx].astype(jnp.float32)[None, :] * padded[tap_idx:tap_idx + SEQUENCE_TOKENS].astype(jnp.float32)
    conv_out = conv_sum.astype(jnp.bfloat16)
    blocked = conv_out.astype(jnp.float32).reshape(SEQUENCE_TOKENS, LRU_BLOCKS, BLOCK_W)
    recur_gate = jax.nn.sigmoid(jnp.einsum('tnc,ncd->tnd', blocked, recur_gate_w.astype(jnp.float32)).reshape(SEQUENCE_TOKENS, LRU_W))
    input_gate = jax.nn.sigmoid(jnp.einsum('tnc,ncd->tnd', blocked, input_gate_w.astype(jnp.float32)).reshape(SEQUENCE_TOKENS, LRU_W))
    log_decay = -decay_sharpness * jax.nn.softplus(-rate_param)[None, :] * recur_gate + decay_extra
    driven = jnp.sqrt(-jnp.expm1(2.0 * log_decay)) * input_gate * conv_out.astype(jnp.float32)
    unused_decay, states = lax.associative_scan(combine_pairs, (jnp.exp(log_decay), driven), axis=0)
    lru_out = (states * jax.nn.gelu(gate_input.astype(jnp.float32))).astype(jnp.bfloat16)
    block_len = math.gcd(SEQUENCE_TOKENS, 512)
    block_count = SEQUENCE_TOKENS // block_len
    positions = jnp.arange(SEQUENCE_TOKENS).astype(jnp.int32)
    score_scale = HEAD_DIM ** (-0.5)
    heads_q = queries.reshape(SEQUENCE_TOKENS, FOX_HEADS, HEAD_DIM).transpose(1, 0, 2)
    heads_k = keys_all.reshape(SEQUENCE_TOKENS, FOX_HEADS, HEAD_DIM).transpose(1, 0, 2)
    heads_v = values_all.reshape(SEQUENCE_TOKENS, FOX_HEADS, HEAD_DIM).transpose(1, 0, 2)
    heads_c = forget_cum.T

    def one_head(entries):
        head_q, head_k, head_v, head_c = entries
        query_blocks = head_q.reshape(block_count, block_len, HEAD_DIM)
        cum_blocks = head_c.reshape(block_count, block_len)
        pos_blocks = positions.reshape(block_count, block_len)

        def one_block(block_entries):
            block_q, block_c, block_pos = block_entries
            scores = jnp.dot(block_q, head_k.T, preferred_element_type=jnp.float32) * score_scale
            scores = scores + block_c[:, None] - head_c[None, :]
            causal = block_pos[:, None] >= positions[None, :]
            scores = jnp.where(causal, scores, -jnp.inf)
            maxima = lax.optimization_barrier(jnp.max(scores, axis=1, keepdims=True))
            probs = jnp.where(causal, jnp.exp(scores - maxima), 0.0)
            totals = lax.optimization_barrier(jnp.sum(probs, axis=1, keepdims=True))
            weighted = jnp.dot(probs.astype(jnp.bfloat16), head_v, preferred_element_type=jnp.float32)
            return (weighted / totals).astype(jnp.bfloat16)
        return lax.map(one_block, (query_blocks, cum_blocks, pos_blocks)).reshape(SEQUENCE_TOKENS, HEAD_DIM)
    fox_heads = lax.map(one_head, (heads_q, heads_k, heads_v, heads_c))
    fox_out = fox_heads.transpose(1, 0, 2).reshape(SEQUENCE_TOKENS, FOX_W)
    mixed_out = jnp.dot(lru_out, out_lru, preferred_element_type=jnp.float32) + jnp.dot(fox_out, out_fox, preferred_element_type=jnp.float32)
    return mixed_out.astype(jnp.bfloat16)
```

```python
import math

import jax
import jax.numpy as jnp
from jax import lax
from jax.experimental import pallas as pl
from jax.experimental.pallas import tpu as pltpu
from jax.sharding import PartitionSpec as P

D = 2048
HEAD_DIM = 128


decay_sharpness = 8.0
epsilon_norm = 1e-06


def in_order(tiles, dim):
    dims = list(tiles.shape[1:])
    dims[dim] *= tiles.shape[0]
    return jnp.moveaxis(tiles, 0, dim).reshape(dims)


def sent_to_all(x, axis):
    copies = jnp.broadcast_to(x, (lax.axis_size(axis), *x.shape))
    return lax.all_to_all(copies, axis, split_axis=0, concat_axis=0, tiled=True)


def gather_directly(x, axis, dim):
    return in_order(sent_to_all(x, axis), dim)


def from_behind(block, axis, distance):
    devices = range(lax.axis_size(axis))
    route = [(i - distance, i) for i in devices if i - distance in devices]
    return lax.ppermute(block, axis, route)


def collected_together(x, axis):
    leaves = jax.tree.leaves(x)
    turns = sorted(range(len(leaves)), key=lambda k: -leaves[k].size)
    width = (1, *leaves[turns[0]].shape)[-1]
    lines = [
        jnp.pad(leaves[k].reshape(-1), (0, -leaves[k].size % width)).reshape(-1, width)
        for k in turns
    ]
    both, at, found = (sent_to_all(jnp.concatenate(lines), axis), 0, {})
    for k, line in zip(turns, lines):
        slab = both[:, at : at + len(line)].reshape(len(both), -1)
        found[k] = slab[:, : leaves[k].size].reshape(-1, *leaves[k].shape)
        at += len(line)
    numbers = iter(range(len(leaves)))
    return jax.tree.map(lambda _: found[next(numbers)], x)


def joined_by_halves(pieces, combine):
    while len(jax.tree.leaves(pieces)[0]) > 1:
        pieces = jax.vmap(combine)(
            *(jax.tree.map(lambda part: part[side::2], pieces) for side in (0, 1))
        )
    return jax.tree.map(lambda part: part[0], pieces)


def prefix_2(x, axis, combine, identity):
    devices, mine = (lax.axis_size(axis), lax.axis_index(axis))
    passed = jnp.arange(devices) < mine

    def kept(part, zero, own):
        part = jnp.where(
            passed.reshape(-1, *(1 for _ in own.shape)), part, jnp.asarray(zero, own.dtype)
        )
        return part

    pieces = collected_together(x, axis)
    return joined_by_halves(jax.tree.map(kept, pieces, identity, x), combine)


def sent_together(arrays, axis, dim, along):
    both = jnp.concatenate(arrays, axis=along)
    filled, at, gathered = (lax.all_gather(both, axis, axis=dim, tiled=True), 0, [])
    for a in arrays:
        gathered.append(lax.slice_in_dim(filled, at, at + a.shape[along], axis=along))
        at += a.shape[along]
    return tuple(gathered)


def cut_along(x, dim, devices):
    dims = x.shape
    tiles = x.reshape(*dims[:dim], devices, dims[dim] // devices, *dims[dim + 1 :])
    return jnp.moveaxis(tiles, dim, 0)


def sent_and_summed(x, axis, dim):
    tiles = cut_along(x, dim, lax.axis_size(axis))
    arrived = lax.all_to_all(tiles, axis, split_axis=0, concat_axis=0, tiled=True)
    return arrived.astype(jnp.float32).sum(axis=0)


def combine_pairs(earlier, later):
    decay_one, state_one = earlier
    decay_two, state_two = later
    return (decay_one * decay_two, decay_two * state_one + state_two)


MESH = pl.DeviceIdType.MESH
ZS, XS = 8, 4
BLK = 512
KROWS = BLK + 16
TILE = 256
LOG2E = 1.4426950408889634
NEG = -1e30


def remote(src, dst, send, recv, **where):
    return pltpu.make_async_remote_copy(
        src_ref=src, dst_ref=dst, send_sem=send, recv_sem=recv, device_id=where, device_id_type=MESH
    )


def eye_mask():
    return lax.broadcasted_iota(jnp.int32, (128, 128), 0) == lax.broadcasted_iota(
        jnp.int32, (128, 128), 1
    )


def packed_rows(column):
    eye = eye_mask()
    return jnp.concatenate(
        [
            jnp.sum(jnp.where(eye, column[g * 128 : (g + 1) * 128], 0.0), axis=0, keepdims=True)
            for g in range(4)
        ],
        axis=0,
    )


def unpacked_row(row):
    return jnp.sum(
        jnp.where(eye_mask(), jnp.broadcast_to(row, (128, 128)), 0.0), axis=1, keepdims=True
    )


def attention_kernel(
    q_ref, k_ref, v_ref, f_ref, o_ref,
    kv, qb, bias, m_ref, l_ref, acc, o_send, st_send, o_recv, st_recv,
    send_p, recv_p, send_m, recv_m, send_q, recv_q, send_o, recv_o, send_s, recv_s,
):
    sp = lax.axis_index("sp")
    z, x = lax.div(sp, XS), lax.rem(sp, XS)
    up = lax.rem(z + 1, ZS) * XS + x
    down = lax.rem(z + ZS - 1, ZS) * XS + x

    def beside(r):
        return z * XS + lax.rem(x + r, XS)

    barrier = pltpu.get_barrier_semaphore()
    for other in (up, down, beside(1), beside(2), beside(3)):
        pl.semaphore_signal(barrier, inc=1, device_id={"sp": other}, device_id_type=MESH)
    pl.semaphore_wait(barrier, 5)

    kv[0, :BLK, :] = k_ref[...]
    forget = f_ref[...]
    high = forget.astype(jnp.bfloat16).astype(jnp.float32)
    middle = (forget - high).astype(jnp.bfloat16).astype(jnp.float32)
    low = forget - high - middle
    kv[0, BLK:KROWS, :] = jnp.concatenate(
        [high, middle, low, jnp.zeros_like(low)], axis=0
    ).astype(jnp.bfloat16)
    kv[0, KROWS:, :] = v_ref[...]
    own_rows = pl.ds(pl.multiple_of(x * BLK, BLK), BLK)
    qb[own_rows, :] = q_ref[...]

    keys, vals = pl.ds(0, KROWS), pl.ds(KROWS, BLK)
    plus = [(0, 1, keys), (0, 1, vals), (1, 2, keys), (1, 2, vals), (2, 3, keys), (2, 3, vals), (3, 7, keys)]
    minus = [(0, 4, keys), (0, 4, vals), (4, 5, keys), (4, 5, vals), (5, 6, keys), (5, 6, vals), (6, 7, vals)]
    plus = [
        remote(kv.at[a, rows], kv.at[b, rows], send_p.at[i], recv_p.at[i], sp=up)
        for i, (a, b, rows) in enumerate(plus)
    ]
    minus = [
        remote(kv.at[a, rows], kv.at[b, rows], send_m.at[i], recv_m.at[i], sp=down)
        for i, (a, b, rows) in enumerate(minus)
    ]
    query_copies = {
        r: remote(q_ref, qb.at[own_rows], send_q.at[r], recv_q.at[r], sp=beside(r)) for r in (1, 2, 3)
    }
    for i in (0, 1):
        plus[i].start()
        minus[i].start()
    for r in (1, 3, 2):
        query_copies[r].start()

    m_ref[...] = jnp.full_like(m_ref, NEG)
    l_ref[...] = jnp.zeros_like(l_ref)
    acc[...] = jnp.zeros_like(acc)

    def set_bias(slot):
        parts = kv[slot, BLK:KROWS, :].astype(jnp.float32)
        whole = parts[0:4] + parts[4:8] + parts[8:12]
        for g in range(4):
            bias[slot : slot + 1, g * 128 : (g + 1) * 128] = whole[g : g + 1] * -LOG2E

    scale = HEAD_DIM ** (-0.5) * LOG2E

    def tile(i, slot, masked=None):
        rows = pl.ds(pl.multiple_of(i * TILE, TILE), TILE)
        scores = lax.dot_general(
            qb[rows, :], kv[slot, :BLK, :], (((1,), (1,)), ((), ())), preferred_element_type=jnp.float32
        )
        scores = scores * scale + bias[slot : slot + 1, :]
        if masked is not None:
            seen = lax.broadcasted_iota(jnp.int32, scores.shape, 0) + masked * TILE
            scores = jnp.where(seen >= lax.broadcasted_iota(jnp.int32, scores.shape, 1), scores, NEG)
        old = m_ref[rows, :]
        new = jnp.maximum(old, jnp.max(scores, axis=1, keepdims=True))
        rescale = jnp.exp2(old - new)
        probs = jnp.exp2(scores - jnp.concatenate([new] * (BLK // 128), axis=1))
        total = l_ref[rows, :] * rescale
        for g in range(BLK // 128):
            total = total + probs[:, g * 128 : (g + 1) * 128]
        l_ref[rows, :] = total
        m_ref[rows, :] = new
        acc[rows, :] = acc[rows, :] * rescale + jnp.dot(
            probs.astype(jnp.bfloat16), kv[slot, KROWS:, :], preferred_element_type=jnp.float32
        )

    tiles = BLK // TILE

    def visit(slot, first=0, last=XS * tiles):
        def body(i, carry):
            tile(i, slot)
            return carry

        lax.fori_loop(first, last, body, 0)

    set_bias(0)
    for t in range(tiles):
        tile(x * tiles + t, 0, masked=t)
    for r in (1, 3, 2):
        query_copies[r].wait_recv()
    visit(0, first=(x + 1) * tiles)

    for d in (1, 2, 3):
        at = 2 * (d - 1)
        for i in (at, at + 1):
            plus[i].wait_recv()
            if i + 2 < 7:
                plus[i + 2].start()
            minus[i].wait_recv()
            if d < 3:
                minus[i + 2].start()
            elif i == at + 1:
                minus[6].start()

        @pl.when(z >= d)
        def _():
            set_bias(d)
            visit(d)

        @pl.when(z + d >= ZS)
        def _():
            set_bias(3 + d)
            visit(3 + d)

    plus[6].wait_recv()
    minus[6].wait_recv()

    @pl.when(z >= 4)
    def _():
        set_bias(7)
        visit(7)

    out_copies = {
        r: (
            remote(o_send.at[r], o_recv.at[r], send_o.at[r], recv_o.at[r], sp=beside(r)),
            remote(st_send.at[r], st_recv.at[r], send_s.at[r], recv_s.at[r], sp=beside(r)),
        )
        for r in (1, 2, 3)
    }

    def stats(rows):
        total = jnp.broadcast_to(jnp.sum(l_ref[rows, :], axis=1, keepdims=True), (BLK, 128))
        return packed_rows(m_ref[rows, :]), packed_rows(total)

    for r in (2, 1, 3):
        rows = pl.ds(pl.multiple_of(lax.rem(x + r, XS) * BLK, BLK), BLK)
        o_send[r] = acc[rows, :].astype(jnp.bfloat16)
        st_send[r] = jnp.concatenate(stats(rows), axis=0)
        for copy in out_copies[r]:
            copy.start()

    tops, sums = [None] * 4, [None] * 4
    tops[0], sums[0] = stats(own_rows)
    for r in (1, 3, 2):
        for copy in out_copies[r]:
            copy.wait_recv()
        both = st_recv[r]
        tops[r], sums[r] = both[0:4], both[4:8]
    top = jnp.maximum(jnp.maximum(tops[0], tops[1]), jnp.maximum(tops[2], tops[3]))
    shares = [jnp.exp2(t - top) for t in tops]
    whole = shares[0] * sums[0] + shares[1] * sums[1] + shares[2] * sums[2] + shares[3] * sums[3]
    shares = [s / whole for s in shares]
    for g in range(4):
        part = pl.ds(g * 128, 128)
        mine = pl.ds(pl.multiple_of(x * BLK + g * 128, 128), 128)
        total = unpacked_row(shares[0][g : g + 1]) * acc[mine, :]
        for r in (1, 2, 3):
            total = total + unpacked_row(shares[r][g : g + 1]) * o_recv[r, part, :].astype(jnp.float32)
        o_ref[part, :] = total.astype(jnp.bfloat16)

    for copy in plus + minus + list(query_copies.values()):
        copy.wait_send()
    for r in (1, 2, 3):
        for copy in out_copies[r]:
            copy.wait_send()


def attention(q, k, v, f):
    vmem = pl.BlockSpec(memory_space=pltpu.VMEM)
    dma = pltpu.SemaphoreType.DMA
    return pl.pallas_call(
        attention_kernel,
        out_shape=jax.ShapeDtypeStruct((BLK, HEAD_DIM), jnp.bfloat16),
        in_specs=[vmem] * 4,
        out_specs=vmem,
        scratch_shapes=[
            pltpu.VMEM((ZS, KROWS + BLK, 128), jnp.bfloat16),
            pltpu.VMEM((XS * BLK, 128), jnp.bfloat16),
            pltpu.VMEM((ZS, BLK), jnp.float32),
            pltpu.VMEM((XS * BLK, 128), jnp.float32),
            pltpu.VMEM((XS * BLK, 128), jnp.float32),
            pltpu.VMEM((XS * BLK, 128), jnp.float32),
            pltpu.VMEM((XS, BLK, 128), jnp.bfloat16),
            pltpu.VMEM((XS, 8, 128), jnp.float32),
            pltpu.VMEM((XS, BLK, 128), jnp.bfloat16),
            pltpu.VMEM((XS, 8, 128), jnp.float32),
            dma((7,)), dma((7,)), dma((7,)), dma((7,)),
            dma((4,)), dma((4,)), dma((4,)), dma((4,)), dma((4,)), dma((4,)),
        ],
        compiler_params=pltpu.CompilerParams(collective_id=1, has_side_effects=True),
        cost_estimate=pl.CostEstimate(flops=2_000_000_000, bytes_accessed=1_000_000, transcendentals=8_000_000),
    )(q, k, v, f)


def shards(
    tokens,
    lru_in,
    lru_gate_in,
    query_w,
    key_w,
    value_w,
    conv_weight,
    recur_gate_w,
    input_gate_w,
    rate_param,
    decay_extra,
    forget_cum,
    out_lru,
    out_fox,
):
    tok_rows = tokens.shape[0]
    lru_cols = lru_in.shape[1]
    fox_cols = query_w.shape[1]
    tp_index = lax.axis_index("tp")
    weight_all = jnp.concatenate([lru_in, lru_gate_in, query_w, key_w, value_w], 1)
    portion = gather_directly(tokens, "tp", 1)
    weight_part = weight_all
    portion_f32 = portion.astype(jnp.float32)
    projected = jnp.dot(portion, weight_part, preferred_element_type=jnp.float32)
    squares = jnp.sum(portion_f32 * portion_f32, axis=1)
    row_scale = lax.rsqrt(squares / D + epsilon_norm)
    scaled = (projected * row_scale[:, None]).astype(jnp.bfloat16)
    lru_input = scaled[:, :lru_cols]
    gate_input = scaled[:, lru_cols : 2 * lru_cols]
    queries = scaled[:, 2 * lru_cols : 2 * lru_cols + fox_cols]
    keys_dev = scaled[:, 2 * lru_cols + fox_cols : 2 * lru_cols + 2 * fox_cols]
    values_dev = scaled[:, 2 * lru_cols + 2 * fox_cols :]
    taps = conv_weight.shape[0]
    own_conv = lax.dynamic_slice_in_dim(conv_weight, tp_index * lru_cols, lru_cols, 1)
    earlier_rows = from_behind(lru_input[tok_rows - (taps - 1) :], "sp", 1)
    padded = jnp.concatenate([earlier_rows, lru_input], 0)
    conv_sum = jnp.zeros((tok_rows, lru_cols), jnp.float32)
    for tap_idx in range(taps):
        conv_sum = conv_sum + own_conv[tap_idx].astype(jnp.float32)[None, :] * padded[
            tap_idx : tap_idx + tok_rows
        ].astype(jnp.float32)
    conv_out = conv_sum.astype(jnp.bfloat16)
    block_width = recur_gate_w.shape[1]
    blocks_dev = lru_cols // block_width
    own_recur = lax.dynamic_slice_in_dim(recur_gate_w, tp_index * blocks_dev, blocks_dev, 0)
    own_input = lax.dynamic_slice_in_dim(input_gate_w, tp_index * blocks_dev, blocks_dev, 0)
    blocked = conv_out.reshape(tok_rows, blocks_dev, block_width)
    recur_gate = jax.nn.sigmoid(
        jnp.einsum("tnc,ncd->tnd", blocked, own_recur, preferred_element_type=jnp.float32).reshape(
            tok_rows, lru_cols
        )
    )
    input_gate = jax.nn.sigmoid(
        jnp.einsum("tnc,ncd->tnd", blocked, own_input, preferred_element_type=jnp.float32).reshape(
            tok_rows, lru_cols
        )
    )
    own_rate = lax.dynamic_slice_in_dim(rate_param, tp_index * lru_cols, lru_cols, 0)
    log_decay = -decay_sharpness * jax.nn.softplus(-own_rate)[None, :] * recur_gate + decay_extra
    driven = jnp.sqrt(-jnp.expm1(2.0 * log_decay)) * input_gate * conv_out.astype(jnp.float32)
    prefix, local_states = lax.associative_scan(combine_pairs, (jnp.exp(log_decay), driven), axis=0)
    identity = (jnp.ones((lru_cols,), jnp.float32), jnp.zeros((lru_cols,), jnp.float32))
    incoming = prefix_2(
        (prefix[tok_rows - 1], local_states[tok_rows - 1]), "sp", combine_pairs, identity
    )
    states = local_states + prefix * incoming[1][None, :]
    lru_out = (states * jax.nn.gelu(gate_input.astype(jnp.float32))).astype(jnp.bfloat16)
    fox_out = attention(queries, keys_dev, values_dev, forget_cum.reshape(4, 128))
    branch = jnp.concatenate([lru_out, fox_out], 1)
    weight_rows = jnp.concatenate([out_lru, out_fox], 0)
    weight_part = weight_rows
    mixed_out = sent_and_summed(
        lax.dot_general(
            weight_part, branch, (((0,), (1,)), ((), ())), preferred_element_type=jnp.float32
        ).astype(jnp.bfloat16),
        "tp",
        0,
    )
    return mixed_out.T.astype(jnp.bfloat16)


def solution(mesh):
    placed = (
        P("sp", "tp"),
        P(None, "tp"),
        P(None, "tp"),
        P(None, "tp"),
        P(None, "tp"),
        P(None, "tp"),
        P(),
        P(),
        P(),
        P(),
        P("sp", "tp"),
        P("sp", "tp"),
        P("tp", None),
        P("tp", None),
    )
    return jax.shard_map(
        shards, mesh=mesh, in_specs=placed, out_specs=P("sp", "tp"), check_vma=False
    )
```

```python
import jax
import jax.numpy as jnp
from jax import lax
from jax.experimental import pallas as pl
from jax.experimental.pallas import tpu as pltpu
from jax.sharding import PartitionSpec as P

MESH = pl.DeviceIdType.MESH
D = 2048
HEAD_DIM = 128
SP, TP = 32, 8
ZS, XS, YS = 8, 4, 4
BLK = 512
HALF = BLK // 2
FEAT = D // TP
OUT = D // TP
KROWS = BLK + 16
LOG2E = 1.4426950408889634
NEG = -1e30
COPIES = 112

decay_sharpness = 8.0
epsilon_norm = 1e-06


def eye_mask():
    return lax.broadcasted_iota(jnp.int32, (128, 128), 0) == lax.broadcasted_iota(
        jnp.int32, (128, 128), 1
    )


def packed_rows(column):
    eye = eye_mask()
    return jnp.concatenate(
        [
            jnp.sum(jnp.where(eye, column[g * 128 : (g + 1) * 128], 0.0), axis=0, keepdims=True)
            for g in range(4)
        ],
        axis=0,
    )


def unpacked_row(row):
    return jnp.sum(
        jnp.where(eye_mask(), jnp.broadcast_to(row, (128, 128)), 0.0), axis=1, keepdims=True
    )


def dot(a, b):
    return jnp.dot(a, b, preferred_element_type=jnp.float32)


def log1p_unit(u):
    s = u / (2.0 + u)
    square = s * s
    total = jnp.full_like(s, 1.0 / 19.0)
    for k in range(17, 0, -2):
        total = total * square + 1.0 / k
    return 2.0 * s * total


def minus_expm1(x):
    near = jnp.full_like(x, 1.0 / 362880.0)
    for k in (40320.0, 5040.0, 720.0, 120.0, 24.0, 6.0, 2.0, 1.0):
        near = near * x + 1.0 / k
    return jnp.where(x > -0.5, -near * x, 1.0 - jnp.exp(x))


class Gather:
    def __init__(self, copy, own, slots, up, down, partner):
        first, second = pl.ds(0, HALF), pl.ds(HALF, HALF)
        self.own, self.slots = own, slots

        def send(a, b, rows, to):
            source = own if a is None else slots.at[a]
            return copy(source.at[rows], slots.at[b, rows], tp=to)

        self.copies = [
            send(None, 0, pl.ds(0, BLK), partner),
            send(None, 1, first, up),
            send(None, 1, second, up),
            send(None, 2, second, down),
            send(None, 2, first, down),
            send(1, 3, first, up),
            send(2, 3, second, down),
            send(1, 4, first, partner),
            send(1, 4, second, partner),
            send(2, 5, first, partner),
            send(2, 5, second, partner),
            send(3, 6, first, partner),
            send(3, 6, second, partner),
        ]

    def start(self, *which):
        for i in which:
            self.copies[i].start()

    def arrived(self, *which):
        for i in which:
            self.copies[i].wait_recv()

    def begin(self):
        self.start(1, 3, 0, 2, 4)

    def relay(self):
        self.arrived(1)
        self.start(5, 7)
        self.arrived(3)
        self.start(6, 10)
        self.arrived(2)
        self.start(8)
        self.arrived(4)
        self.start(9)

    def relay_last(self):
        self.arrived(5)
        self.start(11)
        self.arrived(6)
        self.start(12)

    def finish(self):
        for copy in self.copies:
            copy.wait_send()


def layer_kernel(
    tok_ref, lru_w_hbm, gate_w_hbm, query_w_hbm, key_w_hbm, value_w_hbm,
    conv_ref, recur_ref, input_ref, rate_ref, extra_ref, f_ref, out_lru_ref, out_fox_ref,
    o_ref,
    weights, tokg, acc_kv, acc_rest, squares,
    kv, qb, bias, m_ref, l_ref, acc, o_send, st_send, o_recv, st_recv,
    lru_own, halo, gate_own, decays, drives, row_tiles, col_tiles,
    lru_out, lru_g, fox_out, fox_g, w_out, acc_out,
    send_sems, recv_sems, load_sems,
):
    sp, tp = lax.axis_index("sp"), lax.axis_index("tp")
    z, x = lax.div(sp, XS), lax.rem(sp, XS)
    y, c = lax.div(tp, 2), lax.rem(tp, 2)
    above = lax.rem(z + 1, ZS) * XS + x
    below = lax.rem(z + ZS - 1, ZS) * XS + x
    partner = y * 2 + 1 - c

    def along_y(r, core):
        return lax.rem(y + r, YS) * 2 + core

    def along_x(r):
        return z * XS + lax.rem(x + r, XS)

    def along_z(r):
        return lax.rem(z + r, ZS) * XS + x

    following, preceding = lax.rem(sp + 1, SP), lax.rem(sp + SP - 1, SP)
    used = [0]

    def copy(src, dst, **where):
        i = used[0]
        used[0] += 1
        return pltpu.make_async_remote_copy(
            src_ref=src, dst_ref=dst, send_sem=send_sems.at[i], recv_sem=recv_sems.at[i],
            device_id=where, device_id_type=MESH,
        )

    loads = [
        pltpu.make_async_copy(w, weights.at[i], load_sems.at[i])
        for i, w in enumerate((key_w_hbm, value_w_hbm, query_w_hbm, lru_w_hbm, gate_w_hbm))
    ]
    for load in loads:
        load.start()

    barrier = pltpu.get_barrier_semaphore()
    for r in range(1, TP):
        pl.semaphore_signal(
            barrier, inc=1, device_id={"tp": lax.rem(tp + r, TP)}, device_id_type=MESH
        )
    others = [along_x(r) for r in range(1, XS)] + [along_z(r) for r in range(1, ZS)]
    for other in others + [following, preceding]:
        pl.semaphore_signal(barrier, inc=1, device_id={"sp": other}, device_id_type=MESH)
    pl.semaphore_wait(barrier, TP - 1 + XS - 1 + ZS - 1 + 2)

    tokens = Gather(copy, tok_ref, tokg, along_y(1, c), along_y(3, c), partner)
    tokens.begin()

    def features(r, core):
        return pl.ds(pl.multiple_of(along_y(r, core) * FEAT, FEAT), FEAT)

    def project(block, other, r, group, target, first=False):
        rows = [features(r, c), features(r, 1 - c)]
        right = jnp.concatenate(
            [jnp.concatenate([weights[i, part, :] for part in rows], axis=0) for i in group], axis=1
        )
        product = dot(jnp.concatenate([block[...], other[...]], axis=1), right)
        target[...] = product if first else target[...] + product

    def count_squares(block, other, first=False):
        total = jnp.zeros_like(squares) if first else squares[...]
        for piece in (block, other):
            for g in range(FEAT // 128):
                value = piece[:, g * 128 : (g + 1) * 128].astype(jnp.float32)
                total = total + value * value
        squares[...] = total

    for load in loads:
        load.wait()
    tokens.arrived(0)
    own_pair = (tok_ref, tokg.at[0])
    project(*own_pair, 0, (0, 1), acc_kv, first=True)
    project(*own_pair, 0, (2, 3, 4), acc_rest, first=True)
    count_squares(*own_pair, first=True)
    tokens.relay()
    up_pair, down_pair, far_pair = [(tokg.at[a], tokg.at[a + 3]) for a in (1, 2, 3)]
    tokens.arrived(7, 8)
    project(*up_pair, 3, (0, 1), acc_kv)
    project(*up_pair, 3, (2, 3, 4), acc_rest)
    count_squares(*up_pair)
    tokens.arrived(9, 10)
    project(*down_pair, 1, (0, 1), acc_kv)
    project(*down_pair, 1, (2, 3, 4), acc_rest)
    count_squares(*down_pair)
    tokens.relay_last()
    tokens.arrived(11, 12)
    count_squares(*far_pair)
    row_scale = lax.rsqrt(
        jnp.sum(squares[...], axis=1, keepdims=True) * (1.0 / D) + epsilon_norm
    )
    project(*far_pair, 2, (0, 1), acc_kv)
    keys_values = (acc_kv[...] * row_scale).astype(jnp.bfloat16)
    kv[0, :BLK, :] = keys_values[:, :128]
    kv[0, KROWS:, :] = keys_values[:, 128:]
    forget = f_ref[...]
    high = forget.astype(jnp.bfloat16).astype(jnp.float32)
    middle = (forget - high).astype(jnp.bfloat16).astype(jnp.float32)
    low = forget - high - middle
    kv[0, BLK:KROWS, :] = jnp.concatenate(
        [high, middle, low, jnp.zeros_like(low)], axis=0
    ).astype(jnp.bfloat16)

    keys, vals = pl.ds(0, KROWS), pl.ds(KROWS, BLK)
    plus = [(0, 1, keys), (0, 1, vals), (1, 2, keys), (1, 2, vals), (2, 3, keys), (2, 3, vals), (3, 7, keys)]
    minus = [(0, 4, keys), (0, 4, vals), (4, 5, keys), (4, 5, vals), (5, 6, keys), (5, 6, vals), (6, 7, vals)]
    plus = [copy(kv.at[a, rows], kv.at[b, rows], sp=above) for a, b, rows in plus]
    minus = [copy(kv.at[a, rows], kv.at[b, rows], sp=below) for a, b, rows in minus]
    for i in (0, 1):
        plus[i].start()
        minus[i].start()

    project(*far_pair, 2, (2, 3, 4), acc_rest)
    rest = (acc_rest[...] * row_scale).astype(jnp.bfloat16)
    own_rows = pl.ds(pl.multiple_of(x * BLK, BLK), BLK)
    qb[own_rows, :] = rest[:, :128]
    lru_own[...] = rest[:, 128:256]
    gate_own[...] = rest[:, 256:]
    query_copies = {r: copy(qb.at[own_rows], qb.at[own_rows], sp=along_x(r)) for r in (1, 2, 3)}
    for r in (1, 3, 2):
        query_copies[r].start()
    tail = copy(lru_own.at[pl.ds(BLK - 16, 16)], halo, sp=following)
    tail.start()

    weight_copies = []
    for r in range(1, TP):
        to = lax.rem(tp + r, TP)
        columns = pl.ds(pl.multiple_of(to * OUT, OUT), OUT)
        for k, ref in enumerate((out_lru_ref, out_fox_ref)):
            weight_copies.append(copy(ref.at[:, columns], w_out.at[k, tp], tp=to))
    for each in weight_copies:
        each.start()
    own_columns = pl.ds(pl.multiple_of(tp * OUT, OUT), OUT)
    for k, ref in enumerate((out_lru_ref, out_fox_ref)):
        w_out[k, tp] = ref[:, own_columns]

    m_ref[...] = jnp.full_like(m_ref, NEG)
    l_ref[...] = jnp.zeros_like(l_ref)
    acc[...] = jnp.zeros_like(acc)

    def set_bias(slot):
        parts = kv[slot, BLK:KROWS, :].astype(jnp.float32)
        whole = parts[0:4] + parts[4:8] + parts[8:12]
        for g in range(4):
            bias[slot : slot + 1, g * 128 : (g + 1) * 128] = whole[g : g + 1] * -LOG2E

    scale = HEAD_DIM ** (-0.5) * LOG2E

    def attend(i, slot, masked=False):
        rows = pl.ds(pl.multiple_of(i * BLK, BLK), BLK)
        scores = lax.dot_general(
            qb[rows, :], kv[slot, :BLK, :], (((1,), (1,)), ((), ())), preferred_element_type=jnp.float32
        )
        scores = scores * scale + bias[slot : slot + 1, :]
        if masked:
            earlier = lax.broadcasted_iota(jnp.int32, scores.shape, 0) >= lax.broadcasted_iota(
                jnp.int32, scores.shape, 1
            )
            scores = jnp.where(earlier, scores, NEG)
        old = m_ref[rows, :]
        new = jnp.maximum(old, jnp.max(scores, axis=1, keepdims=True))
        rescale = jnp.exp2(old - new)
        probs = jnp.exp2(scores - jnp.concatenate([new] * (BLK // 128), axis=1))
        total = l_ref[rows, :] * rescale
        for g in range(BLK // 128):
            total = total + probs[:, g * 128 : (g + 1) * 128]
        l_ref[rows, :] = total
        m_ref[rows, :] = new
        acc[rows, :] = acc[rows, :] * rescale + dot(probs.astype(jnp.bfloat16), kv[slot, KROWS:, :])

    def visit(slot, first=0):
        def body(i, carry):
            attend(i, slot)
            return carry

        lax.fori_loop(first, XS, body, 0)

    set_bias(0)
    attend(x, 0, masked=True)

    tail.wait_recv()
    lru_input = lru_own[...].astype(jnp.float32)
    before = halo[8:16, :].astype(jnp.float32) * jnp.where(sp > 0, 1.0, 0.0)
    joined = jnp.concatenate([before, lru_input], axis=0)
    channels = pl.ds(pl.multiple_of(tp * 128, 128), 128)
    taps = conv_ref[:, channels].astype(jnp.float32)
    conv = jnp.zeros((BLK, 128), jnp.float32)
    for j in range(4):
        shifted = joined if j == 3 else pltpu.roll(joined, 3 - j, 0)
        conv = conv + taps[j : j + 1, :] * shifted[8:, :]
    conv = conv.astype(jnp.bfloat16)
    column = lax.broadcasted_iota(jnp.int32, (64, 128), 1)
    row = lax.broadcasted_iota(jnp.int32, (64, 128), 0)
    left = jnp.where(column == row, 1.0, 0.0).astype(jnp.bfloat16)
    right = jnp.where(column == row + 64, 1.0, 0.0).astype(jnp.bfloat16)

    def block_diagonal(ref):
        return jnp.concatenate([dot(ref[2 * tp], left), dot(ref[2 * tp + 1], right)], axis=0)

    gates_w = jnp.concatenate([block_diagonal(recur_ref), block_diagonal(input_ref)], axis=1)
    gates = dot(conv, gates_w.astype(jnp.bfloat16))
    gates = 1.0 / (1.0 + jnp.exp(-gates))
    rate = log1p_unit(jnp.exp(-rate_ref[pl.ds(tp, 1), :]))
    log_decay = (-decay_sharpness * rate) * gates[:, :128] + extra_ref[...]
    drive = jnp.sqrt(minus_expm1(2.0 * log_decay)) * gates[:, 128:] * conv.astype(jnp.float32)
    decay = jnp.exp(log_decay)
    place = lax.broadcasted_iota(jnp.int32, (BLK, 128), 0)
    step = 1
    while step < BLK:
        if step < 8:
            inside = place >= step
            decay_back = jnp.where(inside, pltpu.roll(decay, step, 0), 1.0)
            drive_back = jnp.where(inside, pltpu.roll(drive, step, 0), 0.0)
        else:
            decay_back = jnp.concatenate([jnp.ones((step, 128), jnp.float32), decay[:-step]], axis=0)
            drive_back = jnp.concatenate([jnp.zeros((step, 128), jnp.float32), drive[:-step]], axis=0)
        drive = decay * drive_back + drive
        decay = decay * decay_back
        step *= 2
    decays[...] = decay
    drives[...] = drive

    def tile_of(a, b):
        return jnp.concatenate([a, b, jnp.zeros((6, 128), jnp.float32)], axis=0)

    row_tiles[0] = tile_of(decays[BLK - 1 :, :], drives[BLK - 1 :, :])
    row_copies = {r: copy(row_tiles.at[0], row_tiles.at[r], sp=along_x(r)) for r in (1, 2, 3)}
    for r in (1, 3, 2):
        row_copies[r].start()

    for r in (1, 3, 2):
        query_copies[r].wait_recv()
    visit(0, first=x + 1)

    column_copies = {r: copy(col_tiles.at[0], col_tiles.at[r], sp=along_z(r)) for r in range(1, ZS)}
    branch = Gather(copy, lru_out, lru_g, along_y(1, c), along_y(3, c), partner)
    one, zero = jnp.ones((1, 128), jnp.float32), jnp.zeros((1, 128), jnp.float32)

    def total_of_row():
        for r in (1, 3, 2):
            row_copies[r].wait_recv()
        whole_decay, whole_state, state = one, zero, zero
        for k in range(XS):
            block = row_tiles[lax.rem(x + XS - k, XS)]
            a, b = block[0:1], block[1:2]
            state = jnp.where(k < x, a * state + b, state)
            whole_state = a * whole_state + b
            whole_decay = whole_decay * a
        col_tiles[0] = tile_of(whole_decay, whole_state)
        for r in range(1, ZS):
            column_copies[r].start()

    def recurrence_out():
        for r in range(1, ZS):
            column_copies[r].wait_recv()
        state = zero
        for k in range(ZS):
            block = col_tiles[lax.rem(z + ZS - k, ZS)]
            state = jnp.where(k < z, block[0:1] * state + block[1:2], state)
        for k in range(XS):
            block = row_tiles[lax.rem(x + XS - k, XS)]
            state = jnp.where(k < x, block[0:1] * state + block[1:2], state)
        gate = gate_own[...].astype(jnp.float32)
        inner = 0.7978845608028654 * (gate + 0.044715 * gate * gate * gate)
        gelu = 0.5 * gate * (1.0 + jnp.tanh(inner))
        lru_out[...] = ((drives[...] + decays[...] * state) * gelu).astype(jnp.bfloat16)
        branch.begin()

    beside_attention = {1: total_of_row, 2: recurrence_out, 3: branch.relay}
    for d in (1, 2, 3):
        at = 2 * (d - 1)
        for i in (at, at + 1):
            plus[i].wait_recv()
            if i + 2 < 7:
                plus[i + 2].start()
            minus[i].wait_recv()
            if d < 3:
                minus[i + 2].start()
            elif i == at + 1:
                minus[6].start()

        @pl.when(z >= d)
        def _():
            set_bias(d)
            visit(d)

        @pl.when(z + d >= ZS)
        def _():
            set_bias(3 + d)
            visit(3 + d)

        beside_attention[d]()

    plus[6].wait_recv()
    minus[6].wait_recv()

    @pl.when(z >= 4)
    def _():
        set_bias(7)
        visit(7)

    out_copies = {
        r: (
            copy(o_send.at[r], o_recv.at[r], sp=along_x(r)),
            copy(st_send.at[r], st_recv.at[r], sp=along_x(r)),
        )
        for r in (1, 2, 3)
    }

    def stats(rows):
        total = jnp.broadcast_to(jnp.sum(l_ref[rows, :], axis=1, keepdims=True), (BLK, 128))
        return packed_rows(m_ref[rows, :]), packed_rows(total)

    for r in (2, 1, 3):
        rows = pl.ds(pl.multiple_of(lax.rem(x + r, XS) * BLK, BLK), BLK)
        o_send[r] = acc[rows, :].astype(jnp.bfloat16)
        st_send[r] = jnp.concatenate(stats(rows), axis=0)
        for each in out_copies[r]:
            each.start()

    branch.relay_last()

    def out_weights(k, r, core):
        return w_out[k, along_y(r, core)]

    sources = [(0, c), (0, 1 - c), (3, c), (3, 1 - c), (1, c), (1, 1 - c), (2, c), (2, 1 - c)]

    def branch_product(k, own, slots, which):
        lookup = [None, 0, 1, 4, 2, 5, 3, 6]
        blocks = [own[...] if lookup[i] is None else slots[lookup[i]] for i in which]
        rights = [out_weights(k, *sources[i]) for i in which]
        return dot(jnp.concatenate(blocks, axis=1), jnp.concatenate(rights, axis=0))

    for each in weight_copies:
        each.wait_recv()
    branch.arrived(0, 7, 8, 9, 10, 11, 12)
    acc_out[...] = branch_product(0, lru_out, lru_g, range(8))

    tops, sums = [None] * 4, [None] * 4
    tops[0], sums[0] = stats(own_rows)
    for r in (1, 3, 2):
        for each in out_copies[r]:
            each.wait_recv()
        both = st_recv[r]
        tops[r], sums[r] = both[0:4], both[4:8]
    top = jnp.maximum(jnp.maximum(tops[0], tops[1]), jnp.maximum(tops[2], tops[3]))
    shares = [jnp.exp2(t - top) for t in tops]
    whole = shares[0] * sums[0] + shares[1] * sums[1] + shares[2] * sums[2] + shares[3] * sums[3]
    shares = [s / whole for s in shares]
    for g in range(4):
        part = pl.ds(g * 128, 128)
        mine = pl.ds(pl.multiple_of(x * BLK + g * 128, 128), 128)
        total = unpacked_row(shares[0][g : g + 1]) * acc[mine, :]
        for r in (1, 2, 3):
            total = total + unpacked_row(shares[r][g : g + 1]) * o_recv[r, part, :].astype(jnp.float32)
        fox_out[part, :] = total.astype(jnp.bfloat16)

    heads = Gather(copy, fox_out, fox_g, along_y(1, c), along_y(3, c), partner)
    heads.begin()
    heads.arrived(0)
    acc_out[...] += branch_product(1, fox_out, fox_g, (0, 1))
    heads.relay()
    heads.arrived(7, 8, 9, 10)
    acc_out[...] += branch_product(1, fox_out, fox_g, (2, 3, 4, 5))
    heads.relay_last()
    heads.arrived(11, 12)
    o_ref[...] = (acc_out[...] + branch_product(1, fox_out, fox_g, (6, 7))).astype(jnp.bfloat16)

    for each in plus + minus + [tail] + weight_copies:
        each.wait_send()
    for group in (query_copies, row_copies, column_copies):
        for each in group.values():
            each.wait_send()
    for pair in out_copies.values():
        for each in pair:
            each.wait_send()
    for group in (tokens, branch, heads):
        group.finish()


def layer(
    tokens, lru_in, lru_gate_in, query_w, key_w, value_w, conv_weight, recur_gate_w, input_gate_w,
    rate_param, decay_extra, forget_cum, out_lru, out_fox,
):
    vmem = pl.BlockSpec(memory_space=pltpu.VMEM)
    hbm = pl.BlockSpec(memory_space=pl.ANY)
    bf16, f32 = jnp.bfloat16, jnp.float32
    return pl.pallas_call(
        layer_kernel,
        out_shape=jax.ShapeDtypeStruct((BLK, OUT), bf16),
        in_specs=[vmem] + [hbm] * 5 + [vmem] * 8,
        out_specs=vmem,
        scratch_shapes=[
            pltpu.VMEM((5, D, 128), bf16),
            pltpu.VMEM((7, BLK, FEAT), bf16),
            pltpu.VMEM((BLK, 256), f32),
            pltpu.VMEM((BLK, 384), f32),
            pltpu.VMEM((BLK, 128), f32),
            pltpu.VMEM((ZS, KROWS + BLK, 128), bf16),
            pltpu.VMEM((XS * BLK, 128), bf16),
            pltpu.VMEM((ZS, BLK), f32),
            pltpu.VMEM((XS * BLK, 128), f32),
            pltpu.VMEM((XS * BLK, 128), f32),
            pltpu.VMEM((XS * BLK, 128), f32),
            pltpu.VMEM((XS, BLK, 128), bf16),
            pltpu.VMEM((XS, 8, 128), f32),
            pltpu.VMEM((XS, BLK, 128), bf16),
            pltpu.VMEM((XS, 8, 128), f32),
            pltpu.VMEM((BLK, 128), bf16),
            pltpu.VMEM((16, 128), bf16),
            pltpu.VMEM((BLK, 128), bf16),
            pltpu.VMEM((BLK, 128), f32),
            pltpu.VMEM((BLK, 128), f32),
            pltpu.VMEM((XS, 8, 128), f32),
            pltpu.VMEM((ZS, 8, 128), f32),
            pltpu.VMEM((BLK, 128), bf16),
            pltpu.VMEM((7, BLK, 128), bf16),
            pltpu.VMEM((BLK, 128), bf16),
            pltpu.VMEM((7, BLK, 128), bf16),
            pltpu.VMEM((2, TP, 128, OUT), bf16),
            pltpu.VMEM((BLK, OUT), f32),
            pltpu.SemaphoreType.DMA((COPIES,)),
            pltpu.SemaphoreType.DMA((COPIES,)),
            pltpu.SemaphoreType.DMA((5,)),
        ],
        compiler_params=pltpu.CompilerParams(collective_id=1, has_side_effects=True),
        cost_estimate=pl.CostEstimate(flops=5_000_000_000, bytes_accessed=8_000_000, transcendentals=9_000_000),
    )(
        tokens, lru_in, lru_gate_in, query_w, key_w, value_w, conv_weight, recur_gate_w, input_gate_w,
        rate_param.reshape(TP, 128), decay_extra, forget_cum.reshape(4, 128), out_lru, out_fox,
    )


def solution(mesh):
    placed = (
        P("sp", "tp"),
        P(None, "tp"),
        P(None, "tp"),
        P(None, "tp"),
        P(None, "tp"),
        P(None, "tp"),
        P(),
        P(),
        P(),
        P(),
        P("sp", "tp"),
        P("sp", "tp"),
        P("tp", None),
        P("tp", None),
    )
    return jax.shard_map(
        layer, mesh=mesh, in_specs=placed, out_specs=P("sp", "tp"), check_vma=False
    )
```

```python
import jax
import jax.numpy as jnp
from jax import lax
from jax.experimental import pallas as pl
from jax.experimental.pallas import tpu as pltpu
from jax.sharding import PartitionSpec as P

MESH = pl.DeviceIdType.MESH
D = 2048
HEAD_DIM = 128
SP, TP = 32, 8
ZS, XS, YS = 8, 4, 4
BLK = 512
HALF = BLK // 2
FEAT = D // TP
OUT = D // TP
HROWS = HALF + 16
PIECE = HROWS + HALF
LOG2E = 1.4426950408889634
NEG = -1e30
COPIES = 152

decay_sharpness = 8.0
epsilon_norm = 1e-06


def eye_mask():
    return lax.broadcasted_iota(jnp.int32, (128, 128), 0) == lax.broadcasted_iota(
        jnp.int32, (128, 128), 1
    )


def packed_rows(column):
    eye = eye_mask()
    return jnp.concatenate(
        [
            jnp.sum(jnp.where(eye, column[g * 128 : (g + 1) * 128], 0.0), axis=0, keepdims=True)
            for g in range(4)
        ],
        axis=0,
    )


def unpacked_row(row):
    return jnp.sum(
        jnp.where(eye_mask(), jnp.broadcast_to(row, (128, 128)), 0.0), axis=1, keepdims=True
    )


def dot(a, b):
    return jnp.dot(a, b, preferred_element_type=jnp.float32)


def log1p_unit(u):
    s = u / (2.0 + u)
    square = s * s
    total = jnp.full_like(s, 1.0 / 19.0)
    for k in range(17, 0, -2):
        total = total * square + 1.0 / k
    return 2.0 * s * total


def minus_expm1(x):
    near = jnp.full_like(x, 1.0 / 362880.0)
    for k in (40320.0, 5040.0, 720.0, 120.0, 24.0, 6.0, 2.0, 1.0):
        near = near * x + 1.0 / k
    return jnp.where(x > -0.5, -near * x, 1.0 - jnp.exp(x))


class Gather:
    def __init__(self, copy, own, slots, up, down, partner, start=0, rows=BLK):
        half = rows // 2
        first, second = pl.ds(start, half), pl.ds(start + half, half)

        def send(a, b, part, to):
            source = own if a is None else slots.at[a]
            return copy(source.at[part], slots.at[b, part], tp=to)

        self.copies = [
            send(None, 0, pl.ds(start, rows), partner),
            send(None, 1, first, up),
            send(None, 1, second, up),
            send(None, 2, second, down),
            send(None, 2, first, down),
            send(1, 3, first, up),
            send(2, 3, second, down),
            send(1, 4, first, partner),
            send(1, 4, second, partner),
            send(2, 5, first, partner),
            send(2, 5, second, partner),
            send(3, 6, first, partner),
            send(3, 6, second, partner),
        ]

    def start(self, *which):
        for i in which:
            self.copies[i].start()

    def arrived(self, *which):
        for i in which:
            self.copies[i].wait_recv()

    def begin(self):
        self.start(1, 3, 0, 2, 4)

    def relay_first(self):
        self.arrived(1)
        self.start(5, 7)
        self.arrived(3)
        self.start(6, 10)

    def relay_second(self):
        self.arrived(2)
        self.start(8)
        self.arrived(4)
        self.start(9)

    def relay(self):
        self.relay_first()
        self.relay_second()

    def relay_last(self):
        self.arrived(5)
        self.start(11)
        self.arrived(6)
        self.start(12)

    def finish(self):
        for copy in self.copies:
            copy.wait_send()


def layer_kernel(
    tok_hbm, lru_w_hbm, gate_w_hbm, query_w_hbm, key_w_hbm, value_w_hbm,
    conv_ref, recur_hbm, input_hbm, rate_ref, extra_hbm, f_ref, out_lru_ref, out_fox_ref,
    o_ref,
    tok_ref, recur_ref, input_ref, extra_ref, weights, tokg, acc_kv, acc_rest, scores_a, scores_b, squares,
    kv, qb, bias, m_ref, l_ref, acc, o_send, st_send, o_relay, o_recv, st_recv,
    lru_own, halo, gate_own, decays, drives, row_tiles, col_tiles,
    lru_out, lru_g, fox_out, fox_g, w_out, acc_out, out_rows,
    send_sems, recv_sems, load_sems,
):
    sp, tp = lax.axis_index("sp"), lax.axis_index("tp")
    z, x = lax.div(sp, XS), lax.rem(sp, XS)
    y, c = lax.div(tp, 2), lax.rem(tp, 2)
    above = lax.rem(z + 1, ZS) * XS + x
    below = lax.rem(z + ZS - 1, ZS) * XS + x
    partner = y * 2 + 1 - c

    def along_y(r, core):
        return lax.rem(y + r, YS) * 2 + core

    def along_x(r):
        return z * XS + lax.rem(x + r, XS)

    def along_z(r):
        return lax.rem(z + r, ZS) * XS + x

    following, preceding = lax.rem(sp + 1, SP), lax.rem(sp + SP - 1, SP)
    used = [0]

    def copy(src, dst, **where):
        i = used[0]
        used[0] += 1
        return pltpu.make_async_remote_copy(
            src_ref=src, dst_ref=dst, send_sem=send_sems.at[i], recv_sem=recv_sems.at[i],
            device_id=where, device_id_type=MESH,
        )

    tok_load = pltpu.make_async_copy(tok_hbm, tok_ref, load_sems.at[5])
    tok_load.start()
    loads = [
        pltpu.make_async_copy(w, weights.at[i], load_sems.at[i])
        for i, w in enumerate((key_w_hbm, value_w_hbm, lru_w_hbm, query_w_hbm, gate_w_hbm))
    ]
    own_blocks = pl.ds(2 * tp, 2)
    own_columns = pl.ds(pl.multiple_of(tp * OUT, OUT), OUT)
    later_loads = [
        pltpu.make_async_copy(extra_hbm, extra_ref, load_sems.at[6]),
        pltpu.make_async_copy(recur_hbm.at[own_blocks], recur_ref, load_sems.at[7]),
        pltpu.make_async_copy(input_hbm.at[own_blocks], input_ref, load_sems.at[8]),
        pltpu.make_async_copy(out_lru_ref.at[:, own_columns], w_out.at[0, tp], load_sems.at[9]),
        pltpu.make_async_copy(out_fox_ref.at[:, own_columns], w_out.at[1, tp], load_sems.at[10]),
    ]
    for load in loads + later_loads:
        load.start()

    barrier = pltpu.get_barrier_semaphore()
    for r in range(1, TP):
        pl.semaphore_signal(
            barrier, inc=1, device_id={"tp": lax.rem(tp + r, TP)}, device_id_type=MESH
        )
    others = [along_x(r) for r in range(1, XS)] + [along_z(r) for r in range(1, ZS)]
    for other in others + [following, preceding]:
        pl.semaphore_signal(barrier, inc=1, device_id={"sp": other}, device_id_type=MESH)
    pl.semaphore_wait(barrier, TP - 1 + XS - 1 + ZS - 1 + 2)

    tokens = [
        Gather(copy, tok_ref, tokg, along_y(1, c), along_y(3, c), partner, h * HALF, HALF) for h in (0, 1)
    ]
    tok_load.wait()
    tokens[0].begin()
    forget = f_ref[...]
    high = forget.astype(jnp.bfloat16).astype(jnp.float32)
    middle = (forget - high).astype(jnp.bfloat16).astype(jnp.float32)
    low = forget - high - middle
    for h in (0, 1):
        lines = [part[2 * h : 2 * h + 2] for part in (high, middle, low)]
        kv[h, HALF:HROWS, :] = jnp.concatenate(
            lines + [jnp.zeros((10, 128), jnp.float32)], axis=0
        ).astype(jnp.bfloat16)

    def features(r, core):
        return pl.ds(pl.multiple_of(along_y(r, core) * FEAT, FEAT), FEAT)

    def pair(slot, h):
        rows = pl.ds(h * HALF, HALF)
        block = tok_ref if slot == 0 else tokg.at[slot]
        other = tokg.at[0] if slot == 0 else tokg.at[slot + 3]
        return block[rows, :], other[rows, :]

    distance = {0: 0, 1: 3, 2: 1, 3: 2}

    def project(slot, h, group, target):
        rows = [features(distance[slot], c), features(distance[slot], 1 - c)]
        right = jnp.concatenate(
            [jnp.concatenate([weights[i, part, :] for part in rows], axis=0) for i in group], axis=1
        )
        product = dot(jnp.concatenate(pair(slot, h), axis=1), right)
        half = pl.ds(h * HALF, HALF)
        target[half, :] = product if slot == 0 else target[half, :] + product

    def count_squares(slot, h):
        half = pl.ds(h * HALF, HALF)
        total = jnp.zeros((HALF, 128), jnp.float32) if slot == 0 else squares[half, :]
        for piece in pair(slot, h):
            for g in range(FEAT // 128):
                value = piece[:, g * 128 : (g + 1) * 128].astype(jnp.float32)
                total = total + value * value
        squares[half, :] = total

    def take(slot, h):
        project(slot, h, (0, 1, 2), acc_kv)
        project(slot, h, (3, 4), acc_rest)
        count_squares(slot, h)

    plus = [(0, 2), (1, 3), (2, 4), (3, 5), (4, 6), (5, 7), (6, 14)]
    minus = [(0, 8), (1, 9), (8, 10), (9, 11), (10, 12), (11, 13), (13, 15)]
    plus = [copy(kv.at[a], kv.at[b], sp=above) for a, b in plus]
    minus = [copy(kv.at[a], kv.at[b], sp=below) for a, b in minus]
    tail = copy(lru_own.at[pl.ds(BLK - 16, 16)], halo, sp=following)
    query_rows = [pl.ds(pl.multiple_of(x * BLK + h * HALF, HALF), HALF) for h in (0, 1)]
    query_copies = [
        {r: copy(qb.at[rows], qb.at[rows], sp=along_x(r)) for r in (1, 2, 3)} for rows in query_rows
    ]

    def conclude(h):
        half = pl.ds(h * HALF, HALF)
        count_squares(3, h)
        row_scale = lax.rsqrt(
            jnp.sum(squares[half, :], axis=1, keepdims=True) * (1.0 / D) + epsilon_norm
        )
        project(3, h, (0, 1, 2), acc_kv)
        ready = (acc_kv[half, :] * row_scale).astype(jnp.bfloat16)
        lru_own[half, :] = ready[:, 256:]
        if h == 1:
            tail.start()
        kv[h, :HALF, :] = ready[:, :128]
        kv[h, HROWS:, :] = ready[:, 128:256]
        plus[h].start()
        minus[h].start()
        project(3, h, (3, 4), acc_rest)
        rest = (acc_rest[half, :] * row_scale).astype(jnp.bfloat16)
        qb[query_rows[h], :] = rest[:, :128]
        gate_own[half, :] = rest[:, 128:]
        for r in (1, 3, 2):
            query_copies[h][r].start()

    for load in loads:
        load.wait()
    early, late = tokens
    early.arrived(0)
    take(0, 0)
    early.relay_first()
    late.begin()
    early.relay_second()
    early.arrived(7, 8)
    take(1, 0)
    early.arrived(9, 10)
    take(2, 0)
    early.relay_last()
    late.arrived(0)
    take(0, 1)
    late.relay_first()
    early.arrived(11, 12)
    conclude(0)
    late.relay_second()
    late.arrived(7, 8)
    take(1, 1)
    late.arrived(9, 10)
    take(2, 1)
    late.relay_last()
    late.arrived(11, 12)
    conclude(1)

    weight_copies = []
    for r in range(1, TP):
        to = lax.rem(tp + r, TP)
        columns = pl.ds(pl.multiple_of(to * OUT, OUT), OUT)
        for k, ref in enumerate((out_lru_ref, out_fox_ref)):
            weight_copies.append(copy(ref.at[:, columns], w_out.at[k, tp], tp=to))
    for each in weight_copies:
        each.start()
    own_rows = pl.ds(pl.multiple_of(x * BLK, BLK), BLK)
    m_ref[...] = jnp.full_like(m_ref, NEG)
    l_ref[...] = jnp.zeros_like(l_ref)
    acc[...] = jnp.zeros_like(acc)

    def set_bias(slot):
        parts = kv[slot, HALF:HROWS, :].astype(jnp.float32)
        whole = parts[0:2] + parts[2:4] + parts[4:6]
        for g in range(2):
            bias[slot : slot + 1, g * 128 : (g + 1) * 128] = whole[g : g + 1] * -LOG2E

    scale = HEAD_DIM ** (-0.5) * LOG2E

    def joint(parts, axis):
        return parts[0] if len(parts) == 1 else jnp.concatenate(parts, axis=axis)

    def score(buffer, i, slots):
        rows = pl.ds(pl.multiple_of(i * BLK, BLK), BLK)
        buffer[:, : HALF * len(slots)] = lax.dot_general(
            qb[rows, :],
            joint([kv[slot, :HALF, :] for slot in slots], 0),
            (((1,), (1,)), ((), ())),
            preferred_element_type=jnp.float32,
        )

    def absorb(buffer, i, slots, masked=False):
        rows = pl.ds(pl.multiple_of(i * BLK, BLK), BLK)
        width = HALF * len(slots)
        offsets = joint([bias[slot : slot + 1, :] for slot in slots], 1)
        scores = buffer[:, :width] * scale + offsets
        if masked:
            earlier = lax.broadcasted_iota(jnp.int32, scores.shape, 0) >= lax.broadcasted_iota(
                jnp.int32, scores.shape, 1
            )
            scores = jnp.where(earlier, scores, NEG)
        old = m_ref[rows, :]
        new = jnp.maximum(old, jnp.max(scores, axis=1, keepdims=True))
        rescale = jnp.exp2(old - new)
        probs = jnp.exp2(scores - jnp.concatenate([new] * (width // 128), axis=1))
        total = l_ref[rows, :] * rescale
        for g in range(width // 128):
            total = total + probs[:, g * 128 : (g + 1) * 128]
        l_ref[rows, :] = total
        m_ref[rows, :] = new
        acc[rows, :] = acc[rows, :] * rescale + dot(
            probs.astype(jnp.bfloat16), joint([kv[slot, HROWS:, :] for slot in slots], 0)
        )

    def attend(i, slots, masked=False):
        score(scores_a, i, slots)
        absorb(scores_a, i, slots, masked)

    def visit_rest(slots, first):
        def body(i, carry):
            attend(i, slots)
            return carry

        lax.fori_loop(first, XS, body, 0)

    def visit(*slots):
        for slot in slots:
            set_bias(slot)
        score(scores_a, 0, slots)

        def body(k, carry):
            score(scores_b, 2 * k + 1, slots)
            absorb(scores_a, 2 * k, slots)
            score(scores_a, jnp.minimum(2 * k + 2, XS - 1), slots)
            absorb(scores_b, 2 * k + 1, slots)
            return carry

        lax.fori_loop(0, XS // 2, body, 0)

    def receive(i):
        plus[i].wait_recv()
        if i < 5:
            plus[i + 2].start()
        minus[i].wait_recv()
        if i < 4:
            minus[i + 2].start()
        elif i == 5:
            minus[6].start()

    def take_keys(i):
        d = i // 2 + 1
        if d == 4:

            @pl.when(z >= 4)
            def _():
                visit(14, 15)

            return

        @pl.when(z + d >= ZS)
        def _():
            visit(i + 2, i + 8)

        @pl.when((z >= d) & (z + d < ZS))
        def _():
            visit(i + 2)

    set_bias(0)
    set_bias(1)
    attend(x, (0, 1), masked=True)
    receive(0)

    tail.wait_recv()
    for load in later_loads:
        load.wait()
    lru_input = lru_own[...].astype(jnp.float32)
    before = halo[8:16, :].astype(jnp.float32) * jnp.where(sp > 0, 1.0, 0.0)
    joined = jnp.concatenate([before, lru_input], axis=0)
    channels = pl.ds(pl.multiple_of(tp * 128, 128), 128)
    taps = conv_ref[:, channels].astype(jnp.float32)
    conv = jnp.zeros((BLK, 128), jnp.float32)
    for j in range(4):
        shifted = joined if j == 3 else pltpu.roll(joined, 3 - j, 0)
        conv = conv + taps[j : j + 1, :] * shifted[8:, :]
    conv = conv.astype(jnp.bfloat16)
    column = lax.broadcasted_iota(jnp.int32, (64, 128), 1)
    row = lax.broadcasted_iota(jnp.int32, (64, 128), 0)
    left = jnp.where(column == row, 1.0, 0.0).astype(jnp.bfloat16)
    right = jnp.where(column == row + 64, 1.0, 0.0).astype(jnp.bfloat16)

    def block_diagonal(ref):
        return jnp.concatenate([dot(ref[0], left), dot(ref[1], right)], axis=0)

    gates_w = jnp.concatenate([block_diagonal(recur_ref), block_diagonal(input_ref)], axis=1)
    gates = dot(conv, gates_w.astype(jnp.bfloat16))
    gates = 1.0 / (1.0 + jnp.exp(-gates))
    rate = log1p_unit(jnp.exp(-rate_ref[pl.ds(tp, 1), :]))
    log_decay = (-decay_sharpness * rate) * gates[:, :128] + extra_ref[...]
    drive = jnp.sqrt(minus_expm1(2.0 * log_decay)) * gates[:, 128:] * conv.astype(jnp.float32)
    decay = jnp.exp(log_decay)
    place = lax.broadcasted_iota(jnp.int32, (BLK, 128), 0)
    step = 1
    while step < BLK:
        if step < 8:
            inside = place >= step
            decay_back = jnp.where(inside, pltpu.roll(decay, step, 0), 1.0)
            drive_back = jnp.where(inside, pltpu.roll(drive, step, 0), 0.0)
        else:
            decay_back = jnp.concatenate([jnp.ones((step, 128), jnp.float32), decay[:-step]], axis=0)
            drive_back = jnp.concatenate([jnp.zeros((step, 128), jnp.float32), drive[:-step]], axis=0)
        drive = decay * drive_back + drive
        decay = decay * decay_back
        step *= 2
    decays[...] = decay
    drives[...] = drive

    def tile_of(a, b):
        return jnp.concatenate([a, b, jnp.zeros((6, 128), jnp.float32)], axis=0)

    row_tiles[0] = tile_of(decays[BLK - 1 :, :], drives[BLK - 1 :, :])
    row_copies = {r: copy(row_tiles.at[0], row_tiles.at[r], sp=along_x(r)) for r in (1, 2, 3)}
    for r in (1, 3, 2):
        row_copies[r].start()

    receive(1)
    for queries in query_copies:
        for r in (1, 3, 2):
            queries[r].wait_recv()
    visit_rest((0, 1), x + 1)

    column_copies = {r: copy(col_tiles.at[0], col_tiles.at[r], sp=along_z(r)) for r in range(1, ZS)}
    branch = Gather(copy, lru_out, lru_g, along_y(1, c), along_y(3, c), partner)
    one, zero = jnp.ones((1, 128), jnp.float32), jnp.zeros((1, 128), jnp.float32)

    def total_of_row():
        for r in (1, 3, 2):
            row_copies[r].wait_recv()
        whole_decay, whole_state, state = one, zero, zero
        for k in range(XS):
            block = row_tiles[lax.rem(x + XS - k, XS)]
            a, b = block[0:1], block[1:2]
            state = jnp.where(k < x, a * state + b, state)
            whole_state = a * whole_state + b
            whole_decay = whole_decay * a
        col_tiles[0] = tile_of(whole_decay, whole_state)
        for r in range(1, ZS):
            column_copies[r].start()

    def recurrence_out():
        for r in range(1, ZS):
            column_copies[r].wait_recv()
        state = zero
        for k in range(ZS):
            block = col_tiles[lax.rem(z + ZS - k, ZS)]
            state = jnp.where(k < z, block[0:1] * state + block[1:2], state)
        for k in range(XS):
            block = row_tiles[lax.rem(x + XS - k, XS)]
            state = jnp.where(k < x, block[0:1] * state + block[1:2], state)
        gate = gate_own[...].astype(jnp.float32)
        inner = 0.7978845608028654 * (gate + 0.044715 * gate * gate * gate)
        gelu = 0.5 * gate * (1.0 + jnp.tanh(inner))
        lru_out[...] = ((drives[...] + decays[...] * state) * gelu).astype(jnp.bfloat16)
        branch.begin()

    beside = {0: total_of_row, 2: recurrence_out, 4: branch.relay}
    for i in range(7):
        take_keys(i)
        if i in beside:
            beside[i]()
        if i < 4:
            receive(i + 2)
        elif i == 5:
            receive(6)

    right, left = along_x(1), along_x(3)
    out_copies = []
    for h in (0, 1):
        rows = pl.ds(h * HALF, HALF)
        quarters = [pl.ds(h * HALF + k * 128, 128) for k in (0, 1)]
        out_copies.append(
            {
                "relay": [
                    copy(o_send.at[2, part], o_relay.at[k, part], sp=to)
                    for k, (part, to) in enumerate(zip(quarters, (right, left)))
                ],
                "near": [copy(o_send.at[r, rows], o_recv.at[r, rows], sp=along_x(r)) for r in (1, 3)],
                "far": [
                    copy(o_relay.at[k, part], o_recv.at[2, part], sp=to)
                    for k, (part, to) in enumerate(zip(quarters, (right, left)))
                ],
            }
        )
    stat_copies = [copy(st_send.at[r], st_recv.at[r], sp=along_x(r)) for r in (1, 2, 3)]

    def stats(rows):
        total = jnp.broadcast_to(jnp.sum(l_ref[rows, :], axis=1, keepdims=True), (BLK, 128))
        return packed_rows(m_ref[rows, :]), packed_rows(total)

    def send_out(h, kind):
        for each in out_copies[h][kind]:
            each.start()

    def got_out(h, kind):
        for each in out_copies[h][kind]:
            each.wait_recv()

    def rows_of(r):
        return pl.ds(pl.multiple_of(lax.rem(x + r, XS) * BLK, BLK), BLK)

    o_send[2] = acc[rows_of(2), :].astype(jnp.bfloat16)
    send_out(0, "relay")
    for r in (1, 3):
        o_send[r] = acc[rows_of(r), :].astype(jnp.bfloat16)
    send_out(0, "near")
    send_out(1, "relay")
    for r in (1, 2, 3):
        st_send[r] = jnp.concatenate(stats(rows_of(r)), axis=0)
    for each in stat_copies:
        each.start()
    tops, sums = [None] * 4, [None] * 4
    tops[0], sums[0] = stats(own_rows)
    branch.relay_last()

    got_out(0, "relay")
    send_out(0, "far")
    send_out(1, "near")

    sources = [(0, c), (0, 1 - c), (3, c), (3, 1 - c), (1, c), (1, 1 - c), (2, c), (2, 1 - c)]

    def branch_product(k, own, slots, which, rows):
        lookup = [None, 0, 1, 4, 2, 5, 3, 6]
        blocks = [own[rows, :] if lookup[i] is None else slots[lookup[i], rows, :] for i in which]
        rights = [w_out[k, along_y(*sources[i])] for i in which]
        return dot(jnp.concatenate(blocks, axis=1), jnp.concatenate(rights, axis=0))

    for each in weight_copies:
        each.wait_recv()
    branch.arrived(0, 7, 8, 9, 10, 11, 12)
    got_out(1, "relay")
    send_out(1, "far")
    acc_out[...] = branch_product(0, lru_out, lru_g, range(8), pl.ds(0, BLK))

    for each in stat_copies:
        each.wait_recv()
    for r in (1, 2, 3):
        both = st_recv[r]
        tops[r], sums[r] = both[0:4], both[4:8]
    top = jnp.maximum(jnp.maximum(tops[0], tops[1]), jnp.maximum(tops[2], tops[3]))
    shares = [jnp.exp2(t - top) for t in tops]
    whole = shares[0] * sums[0] + shares[1] * sums[1] + shares[2] * sums[2] + shares[3] * sums[3]
    shares = [s / whole for s in shares]
    heads = [
        Gather(copy, fox_out, fox_g, along_y(1, c), along_y(3, c), partner, h * HALF, HALF) for h in (0, 1)
    ]

    def merge(h):
        got_out(h, "near")
        got_out(h, "far")
        for g in (2 * h, 2 * h + 1):
            part = pl.ds(g * 128, 128)
            mine = pl.ds(pl.multiple_of(x * BLK + g * 128, 128), 128)
            total = unpacked_row(shares[0][g : g + 1]) * acc[mine, :]
            for r in (1, 2, 3):
                total = total + unpacked_row(shares[r][g : g + 1]) * o_recv[r, part, :].astype(jnp.float32)
            fox_out[part, :] = total.astype(jnp.bfloat16)
        heads[h].begin()

    def head_product(h, which):
        rows = pl.ds(h * HALF, HALF)
        return branch_product(1, fox_out, fox_g, which, rows)

    halves = [pl.ds(h * HALF, HALF) for h in (0, 1)]
    out_loads = [
        pltpu.make_async_copy(out_rows.at[half], o_ref.at[half], load_sems.at[11 + h])
        for h, half in enumerate(halves)
    ]

    def write(h):
        heads[h].arrived(11, 12)
        out_rows[halves[h], :] = (acc_out[halves[h], :] + head_product(h, (6, 7))).astype(out_rows.dtype)
        out_loads[h].start()

    merge(0)
    merge(1)
    heads[0].relay()
    heads[0].arrived(0)
    acc_out[halves[0], :] += head_product(0, (0, 1))
    heads[1].relay_first()
    heads[0].relay_last()
    heads[1].relay_second()
    heads[1].arrived(0)
    acc_out[halves[1], :] += head_product(1, (0, 1))
    heads[0].arrived(7, 8, 9, 10)
    acc_out[halves[0], :] += head_product(0, (2, 3, 4, 5))
    write(0)
    heads[1].relay_last()
    heads[1].arrived(7, 8, 9, 10)
    acc_out[halves[1], :] += head_product(1, (2, 3, 4, 5))
    write(1)

    for each in plus + minus + [tail] + weight_copies + stat_copies:
        each.wait_send()
    for group in query_copies + [row_copies, column_copies]:
        for each in group.values():
            each.wait_send()
    for group in out_copies:
        for kind in group.values():
            for each in kind:
                each.wait_send()
    for group in tokens + [branch] + heads:
        group.finish()
    for each in out_loads:
        each.wait()


def layer(
    tokens, lru_in, lru_gate_in, query_w, key_w, value_w, conv_weight, recur_gate_w, input_gate_w,
    rate_param, decay_extra, forget_cum, out_lru, out_fox,
):
    vmem = pl.BlockSpec(memory_space=pltpu.VMEM)
    hbm = pl.BlockSpec(memory_space=pl.ANY)
    bf16, f32 = jnp.bfloat16, jnp.float32
    return pl.pallas_call(
        layer_kernel,
        out_shape=jax.ShapeDtypeStruct((BLK, OUT), bf16),
        in_specs=[hbm] * 6 + [vmem, hbm, hbm, vmem, hbm, vmem, hbm, hbm],
        out_specs=hbm,
        scratch_shapes=[
            pltpu.VMEM((BLK, FEAT), bf16),
            pltpu.VMEM((2, 64, 64), bf16),
            pltpu.VMEM((2, 64, 64), bf16),
            pltpu.VMEM((BLK, 128), f32),
            pltpu.VMEM((5, D, 128), bf16),
            pltpu.VMEM((7, BLK, FEAT), bf16),
            pltpu.VMEM((BLK, 384), f32),
            pltpu.VMEM((BLK, 256), f32),
            pltpu.VMEM((BLK, BLK), f32),
            pltpu.VMEM((BLK, BLK), f32),
            pltpu.VMEM((BLK, 128), f32),
            pltpu.VMEM((2 * ZS, PIECE, 128), bf16),
            pltpu.VMEM((XS * BLK, 128), bf16),
            pltpu.VMEM((2 * ZS, HALF), f32),
            pltpu.VMEM((XS * BLK, 128), f32),
            pltpu.VMEM((XS * BLK, 128), f32),
            pltpu.VMEM((XS * BLK, 128), f32),
            pltpu.VMEM((XS, BLK, 128), bf16),
            pltpu.VMEM((XS, 8, 128), f32),
            pltpu.VMEM((2, BLK, 128), bf16),
            pltpu.VMEM((XS, BLK, 128), bf16),
            pltpu.VMEM((XS, 8, 128), f32),
            pltpu.VMEM((BLK, 128), bf16),
            pltpu.VMEM((16, 128), bf16),
            pltpu.VMEM((BLK, 128), bf16),
            pltpu.VMEM((BLK, 128), f32),
            pltpu.VMEM((BLK, 128), f32),
            pltpu.VMEM((XS, 8, 128), f32),
            pltpu.VMEM((ZS, 8, 128), f32),
            pltpu.VMEM((BLK, 128), bf16),
            pltpu.VMEM((7, BLK, 128), bf16),
            pltpu.VMEM((BLK, 128), bf16),
            pltpu.VMEM((7, BLK, 128), bf16),
            pltpu.VMEM((2, TP, 128, OUT), bf16),
            pltpu.VMEM((BLK, OUT), f32),
            pltpu.VMEM((BLK, OUT), bf16),
            pltpu.SemaphoreType.DMA((COPIES,)),
            pltpu.SemaphoreType.DMA((COPIES,)),
            pltpu.SemaphoreType.DMA((13,)),
        ],
        compiler_params=pltpu.CompilerParams(collective_id=1, has_side_effects=True),
        cost_estimate=pl.CostEstimate(flops=5_000_000_000, bytes_accessed=8_000_000, transcendentals=9_000_000),
    )(
        tokens, lru_in, lru_gate_in, query_w, key_w, value_w, conv_weight, recur_gate_w, input_gate_w,
        rate_param.reshape(TP, 128), decay_extra, forget_cum.reshape(4, 128), out_lru, out_fox,
    )


def solution(mesh):
    placed = (
        P("sp", "tp"),
        P(None, "tp"),
        P(None, "tp"),
        P(None, "tp"),
        P(None, "tp"),
        P(None, "tp"),
        P(),
        P(),
        P(),
        P(),
        P("sp", "tp"),
        P("sp", "tp"),
        P("tp", None),
        P("tp", None),
    )
    return jax.shard_map(
        layer, mesh=mesh, in_specs=placed, out_specs=P("sp", "tp"), check_vma=False
    )
```

```python
import jax
import jax.numpy as jnp
from jax import lax
from jax.experimental import pallas as pl
from jax.experimental.pallas import tpu as pltpu
from jax.sharding import PartitionSpec as P

MESH = pl.DeviceIdType.MESH
D = 2048
HEAD_DIM = 128
SP, TP = 32, 8
ZS, XS, YS = 8, 4, 4
BLK = 512
HALF = BLK // 2
FEAT = D // TP
OUT = D // TP
HROWS = HALF + 16
PIECE = HROWS + HALF
LOG2E = 1.4426950408889634
NEG = -1e30
COPIES = 152

decay_sharpness = 8.0
epsilon_norm = 1e-06


def eye_mask():
    return lax.broadcasted_iota(jnp.int32, (128, 128), 0) == lax.broadcasted_iota(
        jnp.int32, (128, 128), 1
    )


def packed_rows(column):
    eye = eye_mask()
    return jnp.concatenate(
        [
            jnp.sum(jnp.where(eye, column[g * 128 : (g + 1) * 128], 0.0), axis=0, keepdims=True)
            for g in range(4)
        ],
        axis=0,
    )


def unpacked_row(row):
    return jnp.sum(
        jnp.where(eye_mask(), jnp.broadcast_to(row, (128, 128)), 0.0), axis=1, keepdims=True
    )


def dot(a, b):
    return jnp.dot(a, b, preferred_element_type=jnp.float32)


def log1p_unit(u):
    s = u / (2.0 + u)
    square = s * s
    total = jnp.full_like(s, 1.0 / 19.0)
    for k in range(17, 0, -2):
        total = total * square + 1.0 / k
    return 2.0 * s * total


def minus_expm1(x):
    near = jnp.full_like(x, 1.0 / 362880.0)
    for k in (40320.0, 5040.0, 720.0, 120.0, 24.0, 6.0, 2.0, 1.0):
        near = near * x + 1.0 / k
    return jnp.where(x > -0.5, -near * x, 1.0 - jnp.exp(x))


class Gather:
    def __init__(self, copy, own, slots, up, down, partner, start=0, rows=BLK):
        half = rows // 2
        first, second = pl.ds(start, half), pl.ds(start + half, half)

        def send(a, b, part, to):
            source = own if a is None else slots.at[a]
            return copy(source.at[part], slots.at[b, part], tp=to)

        self.copies = [
            send(None, 0, pl.ds(start, rows), partner),
            send(None, 1, first, up),
            send(None, 1, second, up),
            send(None, 2, second, down),
            send(None, 2, first, down),
            send(1, 3, first, up),
            send(2, 3, second, down),
            send(1, 4, first, partner),
            send(1, 4, second, partner),
            send(2, 5, first, partner),
            send(2, 5, second, partner),
            send(3, 6, first, partner),
            send(3, 6, second, partner),
        ]

    def start(self, *which):
        for i in which:
            self.copies[i].start()

    def arrived(self, *which):
        for i in which:
            self.copies[i].wait_recv()

    def begin(self):
        self.start(1, 3, 0, 2, 4)

    def relay_first(self):
        self.arrived(1)
        self.start(5, 7)
        self.arrived(3)
        self.start(6, 10)

    def relay_second(self):
        self.arrived(2)
        self.start(8)
        self.arrived(4)
        self.start(9)

    def relay(self):
        self.relay_first()
        self.relay_second()

    def relay_last(self):
        self.arrived(5)
        self.start(11)
        self.arrived(6)
        self.start(12)

    def finish(self):
        for copy in self.copies:
            copy.wait_send()


def layer_kernel(
    tok_hbm, lru_w_hbm, gate_w_hbm, query_w_hbm, key_w_hbm, value_w_hbm,
    conv_ref, recur_hbm, input_hbm, rate_ref, extra_hbm, f_ref, out_lru_ref, out_fox_ref,
    o_ref,
    tok_ref, recur_ref, input_ref, extra_ref, weights, tokg, acc_kv, acc_rest, scores_a, scores_b, squares,
    kv, qb, bias, m_ref, l_ref, acc, o_send, st_send, o_relay, o_recv, st_recv,
    lru_own, halo, gate_own, decays, drives, row_tiles, col_tiles,
    lru_out, lru_g, fox_out, fox_g, w_out, acc_out, out_rows,
    send_sems, recv_sems, load_sems, alive,
):
    sp, tp = lax.axis_index("sp"), lax.axis_index("tp")
    z, x = lax.div(sp, XS), lax.rem(sp, XS)
    y, c = lax.div(tp, 2), lax.rem(tp, 2)
    above = lax.rem(z + 1, ZS) * XS + x
    below = lax.rem(z + ZS - 1, ZS) * XS + x
    partner = y * 2 + 1 - c

    def along_y(r, core):
        return lax.rem(y + r, YS) * 2 + core

    def along_x(r):
        return z * XS + lax.rem(x + r, XS)

    def along_z(r):
        return lax.rem(z + r, ZS) * XS + x

    following, preceding = lax.rem(sp + 1, SP), lax.rem(sp + SP - 1, SP)
    used = [0]

    def copy(src, dst, **where):
        i = used[0]
        used[0] += 1
        return pltpu.make_async_remote_copy(
            src_ref=src, dst_ref=dst, send_sem=send_sems.at[i], recv_sem=recv_sems.at[i],
            device_id=where, device_id_type=MESH,
        )

    tok_load = pltpu.make_async_copy(tok_hbm, tok_ref, load_sems.at[5])
    tok_load.start()
    loads = [
        pltpu.make_async_copy(w, weights.at[i], load_sems.at[i])
        for i, w in enumerate((key_w_hbm, value_w_hbm, lru_w_hbm, query_w_hbm, gate_w_hbm))
    ]
    own_blocks = pl.ds(2 * tp, 2)
    own_columns = pl.ds(pl.multiple_of(tp * OUT, OUT), OUT)
    later_loads = [
        pltpu.make_async_copy(extra_hbm, extra_ref, load_sems.at[6]),
        pltpu.make_async_copy(recur_hbm.at[own_blocks], recur_ref, load_sems.at[7]),
        pltpu.make_async_copy(input_hbm.at[own_blocks], input_ref, load_sems.at[8]),
        pltpu.make_async_copy(out_lru_ref.at[:, own_columns], w_out.at[0, tp], load_sems.at[9]),
        pltpu.make_async_copy(out_fox_ref.at[:, own_columns], w_out.at[1, tp], load_sems.at[10]),
    ]
    for load in loads + later_loads:
        load.start()

    barrier = pltpu.get_barrier_semaphore()

    def tell(semaphore, **where):
        pl.semaphore_signal(semaphore, inc=1, device_id=where, device_id_type=MESH)

    for r in range(1, TP):
        tell(barrier, tp=lax.rem(tp + r, TP))
    for r in range(1, XS):
        tell(barrier, sp=along_x(r))
    for r in range(1, ZS):

        @pl.when(z + r < ZS)
        def _():
            tell(barrier, sp=along_z(r))

    last_of_row = (x == XS - 1) & (z < ZS - 1)
    first_of_row = (x == 0) & (z > 0)

    @pl.when(last_of_row)
    def _():
        tell(barrier, sp=following)

    pl.semaphore_wait(barrier, TP - 1 + XS - 1 + z + first_of_row.astype(jnp.int32))
    for r in range(1, ZS):

        @pl.when(z >= r)
        def _():
            tell(alive, sp=along_z(ZS - r))

    @pl.when(first_of_row)
    def _():
        tell(alive, sp=preceding)

    tokens = [
        Gather(copy, tok_ref, tokg, along_y(1, c), along_y(3, c), partner, h * HALF, HALF) for h in (0, 1)
    ]
    tok_load.wait()
    tokens[0].begin()
    forget = f_ref[...]
    high = forget.astype(jnp.bfloat16).astype(jnp.float32)
    middle = (forget - high).astype(jnp.bfloat16).astype(jnp.float32)
    low = forget - high - middle
    for h in (0, 1):
        lines = [part[2 * h : 2 * h + 2] for part in (high, middle, low)]
        kv[h, HALF:HROWS, :] = jnp.concatenate(
            lines + [jnp.zeros((10, 128), jnp.float32)], axis=0
        ).astype(jnp.bfloat16)

    def features(r, core):
        return pl.ds(pl.multiple_of(along_y(r, core) * FEAT, FEAT), FEAT)

    def pair(slot, h):
        rows = pl.ds(h * HALF, HALF)
        block = tok_ref if slot == 0 else tokg.at[slot]
        other = tokg.at[0] if slot == 0 else tokg.at[slot + 3]
        return block[rows, :], other[rows, :]

    distance = {0: 0, 1: 3, 2: 1, 3: 2}

    def project(slot, h, group, target):
        rows = [features(distance[slot], c), features(distance[slot], 1 - c)]
        right = jnp.concatenate(
            [jnp.concatenate([weights[i, part, :] for part in rows], axis=0) for i in group], axis=1
        )
        product = dot(jnp.concatenate(pair(slot, h), axis=1), right)
        half = pl.ds(h * HALF, HALF)
        target[half, :] = product if slot == 0 else target[half, :] + product

    def count_squares(slot, h):
        half = pl.ds(h * HALF, HALF)
        total = jnp.zeros((HALF, 128), jnp.float32) if slot == 0 else squares[half, :]
        for piece in pair(slot, h):
            for g in range(FEAT // 128):
                value = piece[:, g * 128 : (g + 1) * 128].astype(jnp.float32)
                total = total + value * value
        squares[half, :] = total

    def take(slot, h):
        project(slot, h, (0, 1, 2), acc_kv)
        project(slot, h, (3, 4), acc_rest)
        count_squares(slot, h)

    plus = [(0, 2), (1, 3), (2, 4), (3, 5), (4, 6), (5, 7)]
    minus = [(0, 8), (1, 9), (8, 10), (9, 11), (10, 12), (11, 13), (12, 14), (13, 15)]
    plus = [copy(kv.at[a], kv.at[b], sp=above) for a, b in plus]
    minus = [copy(kv.at[a], kv.at[b], sp=below) for a, b in minus]

    def wrapped(d):
        return lax.rem(z + d, ZS) < 4

    def send_plus(i):
        @pl.when((z < ZS - 1) & (z >= i // 2))
        def _():
            plus[i].start()

    def send_minus(i):
        @pl.when(wrapped(i // 2))
        def _():
            minus[i].start()

    tail = copy(lru_own.at[pl.ds(BLK - 16, 16)], halo, sp=following)
    query_rows = [pl.ds(pl.multiple_of(x * BLK + h * HALF, HALF), HALF) for h in (0, 1)]
    query_copies = [
        {r: copy(qb.at[rows], qb.at[rows], sp=along_x(r)) for r in (1, 2, 3)} for rows in query_rows
    ]

    def conclude(h):
        half = pl.ds(h * HALF, HALF)
        count_squares(3, h)
        row_scale = lax.rsqrt(
            jnp.sum(squares[half, :], axis=1, keepdims=True) * (1.0 / D) + epsilon_norm
        )
        project(3, h, (0, 1, 2), acc_kv)
        ready = (acc_kv[half, :] * row_scale).astype(jnp.bfloat16)
        lru_own[half, :] = ready[:, 256:]
        if h == 0:
            later = (ZS - 1 - z) + last_of_row.astype(jnp.int32)

            @pl.when(later > 0)
            def _():
                pl.semaphore_wait(alive, later)

        else:

            @pl.when(sp < SP - 1)
            def _():
                tail.start()

        kv[h, :HALF, :] = ready[:, :128]
        kv[h, HROWS:, :] = ready[:, 128:256]
        send_plus(h)
        send_minus(h)
        project(3, h, (3, 4), acc_rest)
        rest = (acc_rest[half, :] * row_scale).astype(jnp.bfloat16)
        qb[query_rows[h], :] = rest[:, :128]
        gate_own[half, :] = rest[:, 128:]
        for r in (1, 3, 2):
            query_copies[h][r].start()

    for load in loads:
        load.wait()
    early, late = tokens
    early.arrived(0)
    take(0, 0)
    early.relay_first()
    late.begin()
    early.relay_second()
    early.arrived(7, 8)
    take(1, 0)
    early.arrived(9, 10)
    take(2, 0)
    early.relay_last()
    late.arrived(0)
    take(0, 1)
    late.relay_first()
    early.arrived(11, 12)
    conclude(0)
    late.relay_second()
    late.arrived(7, 8)
    take(1, 1)
    late.arrived(9, 10)
    take(2, 1)
    late.relay_last()
    late.arrived(11, 12)
    conclude(1)

    weight_copies = []
    for r in range(1, TP):
        to = lax.rem(tp + r, TP)
        columns = pl.ds(pl.multiple_of(to * OUT, OUT), OUT)
        for k, ref in enumerate((out_lru_ref, out_fox_ref)):
            weight_copies.append(copy(ref.at[:, columns], w_out.at[k, tp], tp=to))
    for each in weight_copies:
        each.start()
    own_rows = pl.ds(pl.multiple_of(x * BLK, BLK), BLK)
    m_ref[...] = jnp.full_like(m_ref, NEG)
    l_ref[...] = jnp.zeros_like(l_ref)
    acc[...] = jnp.zeros_like(acc)

    def set_bias(slot):
        parts = kv[slot, HALF:HROWS, :].astype(jnp.float32)
        whole = parts[0:2] + parts[2:4] + parts[4:6]
        for g in range(2):
            bias[slot : slot + 1, g * 128 : (g + 1) * 128] = whole[g : g + 1] * -LOG2E

    scale = HEAD_DIM ** (-0.5) * LOG2E

    def joint(parts, axis):
        return parts[0] if len(parts) == 1 else jnp.concatenate(parts, axis=axis)

    def score(buffer, i, slots):
        rows = pl.ds(pl.multiple_of(i * BLK, BLK), BLK)
        buffer[:, : HALF * len(slots)] = lax.dot_general(
            qb[rows, :],
            joint([kv[slot, :HALF, :] for slot in slots], 0),
            (((1,), (1,)), ((), ())),
            preferred_element_type=jnp.float32,
        )

    def absorb(buffer, i, slots, masked=False):
        rows = pl.ds(pl.multiple_of(i * BLK, BLK), BLK)
        width = HALF * len(slots)
        offsets = joint([bias[slot : slot + 1, :] for slot in slots], 1)
        scores = buffer[:, :width] * scale + offsets
        if masked:
            earlier = lax.broadcasted_iota(jnp.int32, scores.shape, 0) >= lax.broadcasted_iota(
                jnp.int32, scores.shape, 1
            )
            scores = jnp.where(earlier, scores, NEG)
        old = m_ref[rows, :]
        new = jnp.maximum(old, jnp.max(scores, axis=1, keepdims=True))
        rescale = jnp.exp2(old - new)
        probs = jnp.exp2(scores - jnp.concatenate([new] * (width // 128), axis=1))
        total = l_ref[rows, :] * rescale
        for g in range(width // 128):
            total = total + probs[:, g * 128 : (g + 1) * 128]
        l_ref[rows, :] = total
        m_ref[rows, :] = new
        acc[rows, :] = acc[rows, :] * rescale + dot(
            probs.astype(jnp.bfloat16), joint([kv[slot, HROWS:, :] for slot in slots], 0)
        )

    def attend(i, slots, masked=False):
        score(scores_a, i, slots)
        absorb(scores_a, i, slots, masked)

    def visit_rest(slots, first):
        def body(i, carry):
            attend(i, slots)
            return carry

        lax.fori_loop(first, XS, body, 0)

    def visit(*slots):
        for slot in slots:
            set_bias(slot)
        score(scores_a, 0, slots)

        def body(k, carry):
            score(scores_b, 2 * k + 1, slots)
            absorb(scores_a, 2 * k, slots)
            score(scores_a, jnp.minimum(2 * k + 2, XS - 1), slots)
            absorb(scores_b, 2 * k + 1, slots)
            return carry

        lax.fori_loop(0, XS // 2, body, 0)

    def receive(i):
        d = i // 2 + 1
        if d < 4:

            @pl.when(z >= d)
            def _():
                plus[i].wait_recv()

            if d < 3:
                send_plus(i + 2)

        @pl.when(wrapped(d))
        def _():
            minus[i].wait_recv()
            if d < 4:
                minus[i + 2].start()

    def take_keys(i):
        d = i // 2 + 1
        if d == 4:

            @pl.when(z >= 4)
            def _():
                visit(14, 15)

            return

        @pl.when(z + d >= ZS)
        def _():
            visit(i + 2, i + 8)

        @pl.when((z >= d) & (z + d < ZS))
        def _():
            visit(i + 2)

    set_bias(0)
    set_bias(1)
    attend(x, (0, 1), masked=True)
    receive(0)

    @pl.when(sp > 0)
    def _():
        tail.wait_recv()

    @pl.when(sp == 0)
    def _():
        halo[...] = jnp.zeros_like(halo)

    for load in later_loads:
        load.wait()
    lru_input = lru_own[...].astype(jnp.float32)
    before = halo[8:16, :].astype(jnp.float32)
    joined = jnp.concatenate([before, lru_input], axis=0)
    channels = pl.ds(pl.multiple_of(tp * 128, 128), 128)
    taps = conv_ref[:, channels].astype(jnp.float32)
    conv = jnp.zeros((BLK, 128), jnp.float32)
    for j in range(4):
        shifted = joined if j == 3 else pltpu.roll(joined, 3 - j, 0)
        conv = conv + taps[j : j + 1, :] * shifted[8:, :]
    conv = conv.astype(jnp.bfloat16)
    column = lax.broadcasted_iota(jnp.int32, (64, 128), 1)
    row = lax.broadcasted_iota(jnp.int32, (64, 128), 0)
    left = jnp.where(column == row, 1.0, 0.0).astype(jnp.bfloat16)
    right = jnp.where(column == row + 64, 1.0, 0.0).astype(jnp.bfloat16)

    def block_diagonal(ref):
        return jnp.concatenate([dot(ref[0], left), dot(ref[1], right)], axis=0)

    gates_w = jnp.concatenate([block_diagonal(recur_ref), block_diagonal(input_ref)], axis=1)
    gates = dot(conv, gates_w.astype(jnp.bfloat16))
    gates = 1.0 / (1.0 + jnp.exp(-gates))
    rate = log1p_unit(jnp.exp(-rate_ref[pl.ds(tp, 1), :]))
    log_decay = (-decay_sharpness * rate) * gates[:, :128] + extra_ref[...]
    drive = jnp.sqrt(minus_expm1(2.0 * log_decay)) * gates[:, 128:] * conv.astype(jnp.float32)
    decay = jnp.exp(log_decay)
    place = lax.broadcasted_iota(jnp.int32, (BLK, 128), 0)
    step = 1
    while step < BLK:
        if step < 8:
            inside = place >= step
            decay_back = jnp.where(inside, pltpu.roll(decay, step, 0), 1.0)
            drive_back = jnp.where(inside, pltpu.roll(drive, step, 0), 0.0)
        else:
            decay_back = jnp.concatenate([jnp.ones((step, 128), jnp.float32), decay[:-step]], axis=0)
            drive_back = jnp.concatenate([jnp.zeros((step, 128), jnp.float32), drive[:-step]], axis=0)
        drive = decay * drive_back + drive
        decay = decay * decay_back
        step *= 2
    decays[...] = decay
    drives[...] = drive

    def tile_of(a, b):
        return jnp.concatenate([a, b, jnp.zeros((6, 128), jnp.float32)], axis=0)

    row_tiles[0] = tile_of(decays[BLK - 1 :, :], drives[BLK - 1 :, :])
    row_copies = {r: copy(row_tiles.at[0], row_tiles.at[r], sp=along_x(r)) for r in (1, 2, 3)}
    for r in (1, 3, 2):
        row_copies[r].start()

    receive(1)
    for queries in query_copies:
        for r in (1, 3, 2):
            queries[r].wait_recv()
    visit_rest((0, 1), x + 1)

    column_copies = {r: copy(col_tiles.at[0], col_tiles.at[r], sp=along_z(r)) for r in range(1, ZS)}
    branch = Gather(copy, lru_out, lru_g, along_y(1, c), along_y(3, c), partner)
    one, zero = jnp.ones((1, 128), jnp.float32), jnp.zeros((1, 128), jnp.float32)

    def total_of_row():
        for r in (1, 3, 2):
            row_copies[r].wait_recv()
        whole_decay, whole_state, state = one, zero, zero
        for k in range(XS):
            block = row_tiles[lax.rem(x + XS - k, XS)]
            a, b = block[0:1], block[1:2]
            state = jnp.where(k < x, a * state + b, state)
            whole_state = a * whole_state + b
            whole_decay = whole_decay * a
        col_tiles[0] = tile_of(whole_decay, whole_state)
        for r in range(1, ZS):

            @pl.when(z + r < ZS)
            def _():
                column_copies[r].start()

    def recurrence_out():
        for r in range(1, ZS):

            @pl.when(z >= r)
            def _():
                column_copies[r].wait_recv()

        def row_above(k, state):
            block = col_tiles[z - k]
            return block[0:1] * state + block[1:2]

        state = lax.fori_loop(0, z, row_above, zero)
        for k in range(XS):
            block = row_tiles[lax.rem(x + XS - k, XS)]
            state = jnp.where(k < x, block[0:1] * state + block[1:2], state)
        gate = gate_own[...].astype(jnp.float32)
        inner = 0.7978845608028654 * (gate + 0.044715 * gate * gate * gate)
        gelu = 0.5 * gate * (1.0 + jnp.tanh(inner))
        lru_out[...] = ((drives[...] + decays[...] * state) * gelu).astype(jnp.bfloat16)
        branch.begin()

    beside = {0: total_of_row, 2: recurrence_out, 4: branch.relay}
    for i in range(7):
        take_keys(i)
        if i in beside:
            beside[i]()
        if i < 4:
            receive(i + 2)
        elif i == 4:
            receive(6)
        elif i == 5:
            receive(7)

    right, left = along_x(1), along_x(3)
    out_copies = []
    for h in (0, 1):
        rows = pl.ds(h * HALF, HALF)
        quarters = [pl.ds(h * HALF + k * 128, 128) for k in (0, 1)]
        out_copies.append(
            {
                "relay": [
                    copy(o_send.at[2, part], o_relay.at[k, part], sp=to)
                    for k, (part, to) in enumerate(zip(quarters, (right, left)))
                ],
                "near": [copy(o_send.at[r, rows], o_recv.at[r, rows], sp=along_x(r)) for r in (1, 3)],
                "far": [
                    copy(o_relay.at[k, part], o_recv.at[2, part], sp=to)
                    for k, (part, to) in enumerate(zip(quarters, (right, left)))
                ],
            }
        )
    stat_copies = [copy(st_send.at[r], st_recv.at[r], sp=along_x(r)) for r in (1, 2, 3)]

    def stats(rows):
        total = jnp.broadcast_to(jnp.sum(l_ref[rows, :], axis=1, keepdims=True), (BLK, 128))
        return packed_rows(m_ref[rows, :]), packed_rows(total)

    def send_out(h, kind):
        for each in out_copies[h][kind]:
            each.start()

    def got_out(h, kind):
        for each in out_copies[h][kind]:
            each.wait_recv()

    def rows_of(r):
        return pl.ds(pl.multiple_of(lax.rem(x + r, XS) * BLK, BLK), BLK)

    o_send[2] = acc[rows_of(2), :].astype(jnp.bfloat16)
    send_out(0, "relay")
    for r in (1, 3):
        o_send[r] = acc[rows_of(r), :].astype(jnp.bfloat16)
    send_out(0, "near")
    send_out(1, "relay")
    for r in (1, 2, 3):
        st_send[r] = jnp.concatenate(stats(rows_of(r)), axis=0)
    for each in stat_copies:
        each.start()
    tops, sums = [None] * 4, [None] * 4
    tops[0], sums[0] = stats(own_rows)
    branch.relay_last()

    got_out(0, "relay")
    send_out(0, "far")
    send_out(1, "near")

    sources = [(0, c), (0, 1 - c), (3, c), (3, 1 - c), (1, c), (1, 1 - c), (2, c), (2, 1 - c)]

    def branch_product(k, own, slots, which, rows):
        lookup = [None, 0, 1, 4, 2, 5, 3, 6]
        blocks = [own[rows, :] if lookup[i] is None else slots[lookup[i], rows, :] for i in which]
        rights = [w_out[k, along_y(*sources[i])] for i in which]
        return dot(jnp.concatenate(blocks, axis=1), jnp.concatenate(rights, axis=0))

    for each in weight_copies:
        each.wait_recv()
    branch.arrived(0, 7, 8, 9, 10, 11, 12)
    got_out(1, "relay")
    send_out(1, "far")
    acc_out[...] = branch_product(0, lru_out, lru_g, range(8), pl.ds(0, BLK))

    for each in stat_copies:
        each.wait_recv()
    for r in (1, 2, 3):
        both = st_recv[r]
        tops[r], sums[r] = both[0:4], both[4:8]
    top = jnp.maximum(jnp.maximum(tops[0], tops[1]), jnp.maximum(tops[2], tops[3]))
    shares = [jnp.exp2(t - top) for t in tops]
    whole = shares[0] * sums[0] + shares[1] * sums[1] + shares[2] * sums[2] + shares[3] * sums[3]
    shares = [s / whole for s in shares]
    heads = [
        Gather(copy, fox_out, fox_g, along_y(1, c), along_y(3, c), partner, h * HALF, HALF) for h in (0, 1)
    ]

    def merge(h):
        got_out(h, "near")
        got_out(h, "far")
        for g in (2 * h, 2 * h + 1):
            part = pl.ds(g * 128, 128)
            mine = pl.ds(pl.multiple_of(x * BLK + g * 128, 128), 128)
            total = unpacked_row(shares[0][g : g + 1]) * acc[mine, :]
            for r in (1, 2, 3):
                total = total + unpacked_row(shares[r][g : g + 1]) * o_recv[r, part, :].astype(jnp.float32)
            fox_out[part, :] = total.astype(jnp.bfloat16)
        heads[h].begin()

    def head_product(h, which):
        rows = pl.ds(h * HALF, HALF)
        return branch_product(1, fox_out, fox_g, which, rows)

    halves = [pl.ds(h * HALF, HALF) for h in (0, 1)]
    out_loads = [
        pltpu.make_async_copy(out_rows.at[half], o_ref.at[half], load_sems.at[11 + h])
        for h, half in enumerate(halves)
    ]

    def write(h):
        heads[h].arrived(11, 12)
        out_rows[halves[h], :] = (acc_out[halves[h], :] + head_product(h, (6, 7))).astype(out_rows.dtype)
        out_loads[h].start()

    merge(0)
    merge(1)
    heads[0].relay()
    heads[0].arrived(0)
    acc_out[halves[0], :] += head_product(0, (0, 1))
    heads[1].relay_first()
    heads[0].relay_last()
    heads[1].relay_second()
    heads[1].arrived(0)
    acc_out[halves[1], :] += head_product(1, (0, 1))
    heads[0].arrived(7, 8, 9, 10)
    acc_out[halves[0], :] += head_product(0, (2, 3, 4, 5))
    write(0)
    heads[1].relay_last()
    heads[1].arrived(7, 8, 9, 10)
    acc_out[halves[1], :] += head_product(1, (2, 3, 4, 5))
    write(1)

    for i, each in enumerate(plus):

        @pl.when((z < ZS - 1) & (z >= i // 2))
        def _():
            each.wait_send()

    for i, each in enumerate(minus):

        @pl.when(wrapped(i // 2))
        def _():
            each.wait_send()

    @pl.when(sp < SP - 1)
    def _():
        tail.wait_send()

    for r in range(1, ZS):

        @pl.when(z + r < ZS)
        def _():
            column_copies[r].wait_send()

    for each in weight_copies + stat_copies:
        each.wait_send()
    for group in query_copies + [row_copies]:
        for each in group.values():
            each.wait_send()
    for group in out_copies:
        for kind in group.values():
            for each in kind:
                each.wait_send()
    for group in tokens + [branch] + heads:
        group.finish()
    for each in out_loads:
        each.wait()


def layer(
    tokens, lru_in, lru_gate_in, query_w, key_w, value_w, conv_weight, recur_gate_w, input_gate_w,
    rate_param, decay_extra, forget_cum, out_lru, out_fox,
):
    vmem = pl.BlockSpec(memory_space=pltpu.VMEM)
    hbm = pl.BlockSpec(memory_space=pl.ANY)
    bf16, f32 = jnp.bfloat16, jnp.float32
    return pl.pallas_call(
        layer_kernel,
        out_shape=jax.ShapeDtypeStruct((BLK, OUT), bf16),
        in_specs=[hbm] * 6 + [vmem, hbm, hbm, vmem, hbm, vmem, hbm, hbm],
        out_specs=hbm,
        scratch_shapes=[
            pltpu.VMEM((BLK, FEAT), bf16),
            pltpu.VMEM((2, 64, 64), bf16),
            pltpu.VMEM((2, 64, 64), bf16),
            pltpu.VMEM((BLK, 128), f32),
            pltpu.VMEM((5, D, 128), bf16),
            pltpu.VMEM((7, BLK, FEAT), bf16),
            pltpu.VMEM((BLK, 384), f32),
            pltpu.VMEM((BLK, 256), f32),
            pltpu.VMEM((BLK, BLK), f32),
            pltpu.VMEM((BLK, BLK), f32),
            pltpu.VMEM((BLK, 128), f32),
            pltpu.VMEM((2 * ZS, PIECE, 128), bf16),
            pltpu.VMEM((XS * BLK, 128), bf16),
            pltpu.VMEM((2 * ZS, HALF), f32),
            pltpu.VMEM((XS * BLK, 128), f32),
            pltpu.VMEM((XS * BLK, 128), f32),
            pltpu.VMEM((XS * BLK, 128), f32),
            pltpu.VMEM((XS, BLK, 128), bf16),
            pltpu.VMEM((XS, 8, 128), f32),
            pltpu.VMEM((2, BLK, 128), bf16),
            pltpu.VMEM((XS, BLK, 128), bf16),
            pltpu.VMEM((XS, 8, 128), f32),
            pltpu.VMEM((BLK, 128), bf16),
            pltpu.VMEM((16, 128), bf16),
            pltpu.VMEM((BLK, 128), bf16),
            pltpu.VMEM((BLK, 128), f32),
            pltpu.VMEM((BLK, 128), f32),
            pltpu.VMEM((XS, 8, 128), f32),
            pltpu.VMEM((ZS, 8, 128), f32),
            pltpu.VMEM((BLK, 128), bf16),
            pltpu.VMEM((7, BLK, 128), bf16),
            pltpu.VMEM((BLK, 128), bf16),
            pltpu.VMEM((7, BLK, 128), bf16),
            pltpu.VMEM((2, TP, 128, OUT), bf16),
            pltpu.VMEM((BLK, OUT), f32),
            pltpu.VMEM((BLK, OUT), bf16),
            pltpu.SemaphoreType.DMA((COPIES,)),
            pltpu.SemaphoreType.DMA((COPIES,)),
            pltpu.SemaphoreType.DMA((13,)),
            pltpu.SemaphoreType.REGULAR,
        ],
        compiler_params=pltpu.CompilerParams(collective_id=1, has_side_effects=True),
        cost_estimate=pl.CostEstimate(flops=5_000_000_000, bytes_accessed=8_000_000, transcendentals=9_000_000),
    )(
        tokens, lru_in, lru_gate_in, query_w, key_w, value_w, conv_weight, recur_gate_w, input_gate_w,
        rate_param.reshape(TP, 128), decay_extra, forget_cum.reshape(4, 128), out_lru, out_fox,
    )


def solution(mesh):
    placed = (
        P("sp", "tp"),
        P(None, "tp"),
        P(None, "tp"),
        P(None, "tp"),
        P(None, "tp"),
        P(None, "tp"),
        P(),
        P(),
        P(),
        P(),
        P("sp", "tp"),
        P("sp", "tp"),
        P("tp", None),
        P("tp", None),
    )
    return jax.shard_map(
        layer, mesh=mesh, in_specs=placed, out_specs=P("sp", "tp"), check_vma=False
    )
```

```python
import jax
import jax.numpy as jnp
from jax import lax
from jax.experimental import pallas as pl
from jax.experimental.pallas import tpu as pltpu
from jax.sharding import PartitionSpec as P

MESH = pl.DeviceIdType.MESH
D = 2048
HEAD_DIM = 128
SP, TP = 32, 8
ZS, XS, YS = 8, 4, 4
BLK = 512
HALF = BLK // 2
FEAT = D // TP
OUT = D // TP
HROWS = HALF + 16
PIECE = HROWS + HALF
LOG2E = 1.4426950408889634
NEG = -1e30
COPIES = 96

decay_sharpness = 8.0
epsilon_norm = 1e-06


def eye_mask():
    return lax.broadcasted_iota(jnp.int32, (128, 128), 0) == lax.broadcasted_iota(
        jnp.int32, (128, 128), 1
    )


def packed_rows(column):
    eye = eye_mask()
    return jnp.concatenate(
        [
            jnp.sum(jnp.where(eye, column[g * 128 : (g + 1) * 128], 0.0), axis=0, keepdims=True)
            for g in range(4)
        ],
        axis=0,
    )


def unpacked_row(row):
    return jnp.sum(
        jnp.where(eye_mask(), jnp.broadcast_to(row, (128, 128)), 0.0), axis=1, keepdims=True
    )


def dot(a, b):
    return jnp.dot(a, b, preferred_element_type=jnp.float32)


def log1p_unit(u):
    s = u / (2.0 + u)
    square = s * s
    total = jnp.full_like(s, 1.0 / 19.0)
    for k in range(17, 0, -2):
        total = total * square + 1.0 / k
    return 2.0 * s * total


def minus_expm1(x):
    near = jnp.full_like(x, 1.0 / 362880.0)
    for k in (40320.0, 5040.0, 720.0, 120.0, 24.0, 6.0, 2.0, 1.0):
        near = near * x + 1.0 / k
    return jnp.where(x > -0.5, -near * x, 1.0 - jnp.exp(x))


def await_bytes(ref, semaphore):
    pltpu.make_async_copy(ref, ref, semaphore).wait()


class Gather:
    def __init__(self, copy, sems, own, slots, up, down, partner, start=0, rows=BLK):
        half = rows // 2
        first, second = pl.ds(start, half), pl.ds(start + half, half)

        def send(a, b, part, to, k):
            source = own if a is None else slots.at[a]
            return copy(source.at[part], slots.at[b, part], send=sems[10], recv=sems[k], tp=to)

        plan = [
            (None, 0, pl.ds(start, rows), partner, 0),
            (None, 1, first, up, 1),
            (None, 1, second, up, 2),
            (None, 2, second, down, 3),
            (None, 2, first, down, 4),
            (1, 3, first, up, 5),
            (2, 3, second, down, 6),
            (1, 4, first, partner, 7),
            (1, 4, second, partner, 7),
            (2, 5, first, partner, 8),
            (2, 5, second, partner, 8),
            (3, 6, first, partner, 9),
            (3, 6, second, partner, 9),
        ]
        self.copies = [send(*each) for each in plan]
        self.sems, self.slots, self.rows = sems, slots, pl.ds(start, rows)

    def start(self, *which):
        for i in which:
            self.copies[i].start()

    def arrived(self, *which):
        for i in which:
            self.copies[i].wait_recv()

    def arrived_from_partner(self, *slots):
        for slot in slots:
            await_bytes(self.slots.at[slot, self.rows], self.sems[slot + 3])

    def finish(self):
        await_bytes(self.slots.at[:, self.rows], self.sems[10])

    def begin(self):
        self.start(1, 3, 0, 2, 4)

    def relay_first(self):
        self.arrived(1)
        self.start(5, 7)
        self.arrived(3)
        self.start(6, 10)

    def relay_second(self):
        self.arrived(2)
        self.start(8)
        self.arrived(4)
        self.start(9)

    def relay(self):
        self.relay_first()
        self.relay_second()

    def relay_last(self):
        self.arrived(5)
        self.start(11)
        self.arrived(6)
        self.start(12)


def layer_kernel(
    tok_hbm, lru_w_hbm, gate_w_hbm, query_w_hbm, key_w_hbm, value_w_hbm,
    conv_ref, recur_hbm, input_hbm, rate_ref, extra_hbm, f_ref, out_lru_ref, out_fox_ref,
    o_ref,
    tok_ref, recur_ref, input_ref, extra_ref, weights, tokg, acc_kv, acc_rest, scores_a, scores_b, squares,
    kv, qb, bias, m_ref, l_ref, acc, o_send, st_send, o_relay, o_recv, st_recv,
    lru_own, halo, gate_own, decays, drives, row_tiles, col_tiles,
    lru_out, lru_g, fox_out, fox_g, w_out, acc_out, out_rows,
    copy_sems, load_sems, alive,
):
    sp, tp = lax.axis_index("sp"), lax.axis_index("tp")
    z, x = lax.div(sp, XS), lax.rem(sp, XS)
    y, c = lax.div(tp, 2), lax.rem(tp, 2)
    above = lax.rem(z + 1, ZS) * XS + x
    below = lax.rem(z + ZS - 1, ZS) * XS + x
    partner = y * 2 + 1 - c

    def along_y(r, core):
        return lax.rem(y + r, YS) * 2 + core

    def along_x(r):
        return z * XS + lax.rem(x + r, XS)

    def along_z(r):
        return lax.rem(z + r, ZS) * XS + x

    following, preceding = lax.rem(sp + 1, SP), lax.rem(sp + SP - 1, SP)
    used = [0]

    def semaphore():
        used[0] += 1
        return copy_sems.at[used[0] - 1]

    def copy(src, dst, send=None, recv=None, **where):
        return pltpu.make_async_remote_copy(
            src_ref=src, dst_ref=dst, send_sem=send or semaphore(), recv_sem=recv or semaphore(),
            device_id=where, device_id_type=MESH,
        )

    gather_sems = [[semaphore() for k in range(11)] for group in range(3)]

    tok_load = pltpu.make_async_copy(tok_hbm, tok_ref, load_sems.at[1])
    tok_load.start()
    loads = [
        pltpu.make_async_copy(w, weights.at[i], load_sems.at[0])
        for i, w in enumerate((key_w_hbm, value_w_hbm, lru_w_hbm, query_w_hbm, gate_w_hbm))
    ]
    own_blocks = pl.ds(2 * tp, 2)
    own_columns = pl.ds(pl.multiple_of(tp * OUT, OUT), OUT)
    later_loads = [
        pltpu.make_async_copy(extra_hbm, extra_ref, load_sems.at[2]),
        pltpu.make_async_copy(recur_hbm.at[own_blocks], recur_ref, load_sems.at[3]),
        pltpu.make_async_copy(input_hbm.at[own_blocks], input_ref, load_sems.at[4]),
        pltpu.make_async_copy(out_lru_ref.at[:, own_columns], w_out.at[0, tp], load_sems.at[5]),
        pltpu.make_async_copy(out_fox_ref.at[:, own_columns], w_out.at[1, tp], load_sems.at[6]),
    ]
    for load in loads + later_loads:
        load.start()

    barrier = pltpu.get_barrier_semaphore()

    def tell(semaphore, **where):
        pl.semaphore_signal(semaphore, inc=1, device_id=where, device_id_type=MESH)

    for r in range(1, TP):
        tell(barrier, tp=lax.rem(tp + r, TP))
    for r in range(1, XS):
        tell(barrier, sp=along_x(r))
    for r in range(1, ZS):

        @pl.when(z + r < ZS)
        def _():
            tell(barrier, sp=along_z(r))

    last_of_row = (x == XS - 1) & (z < ZS - 1)
    first_of_row = (x == 0) & (z > 0)

    @pl.when(last_of_row)
    def _():
        tell(barrier, sp=following)

    pl.semaphore_wait(barrier, TP - 1 + XS - 1 + z + first_of_row.astype(jnp.int32))
    for r in range(1, ZS):

        @pl.when(z >= r)
        def _():
            tell(alive, sp=along_z(ZS - r))

    @pl.when(first_of_row)
    def _():
        tell(alive, sp=preceding)

    tokens = [
        Gather(copy, gather_sems[h], tok_ref, tokg, along_y(1, c), along_y(3, c), partner, h * HALF, HALF) for h in (0, 1)
    ]
    tok_load.wait()
    tokens[0].begin()
    forget = f_ref[...]
    high = forget.astype(jnp.bfloat16).astype(jnp.float32)
    middle = (forget - high).astype(jnp.bfloat16).astype(jnp.float32)
    low = forget - high - middle
    for h in (0, 1):
        lines = [part[2 * h : 2 * h + 2] for part in (high, middle, low)]
        kv[h, HALF:HROWS, :] = jnp.concatenate(
            lines + [jnp.zeros((10, 128), jnp.float32)], axis=0
        ).astype(jnp.bfloat16)

    def features(r, core):
        return pl.ds(pl.multiple_of(along_y(r, core) * FEAT, FEAT), FEAT)

    def pair(slot, h):
        rows = pl.ds(h * HALF, HALF)
        block = tok_ref if slot == 0 else tokg.at[slot]
        other = tokg.at[0] if slot == 0 else tokg.at[slot + 3]
        return block[rows, :], other[rows, :]

    distance = {0: 0, 1: 3, 2: 1, 3: 2}

    def project(slot, h, group, target):
        rows = [features(distance[slot], c), features(distance[slot], 1 - c)]
        right = jnp.concatenate(
            [jnp.concatenate([weights[i, part, :] for part in rows], axis=0) for i in group], axis=1
        )
        product = dot(jnp.concatenate(pair(slot, h), axis=1), right)
        half = pl.ds(h * HALF, HALF)
        target[half, :] = product if slot == 0 else target[half, :] + product

    def count_squares(slot, h):
        half = pl.ds(h * HALF, HALF)
        total = jnp.zeros((HALF, 128), jnp.float32) if slot == 0 else squares[half, :]
        for piece in pair(slot, h):
            for g in range(FEAT // 128):
                value = piece[:, g * 128 : (g + 1) * 128].astype(jnp.float32)
                total = total + value * value
        squares[half, :] = total

    def take(slot, h):
        project(slot, h, (0, 1, 2), acc_kv)
        project(slot, h, (3, 4), acc_rest)
        count_squares(slot, h)

    plus = [(0, 2), (1, 3), (2, 4), (3, 5), (4, 6), (5, 7)]
    minus = [(0, 8), (1, 9), (8, 10), (9, 11), (10, 12), (11, 13), (12, 14), (13, 15)]
    plus = [copy(kv.at[a], kv.at[b], sp=above) for a, b in plus]
    minus = [copy(kv.at[a], kv.at[b], sp=below) for a, b in minus]

    def wrapped(d):
        return lax.rem(z + d, ZS) < 4

    def send_plus(i):
        @pl.when((z < ZS - 1) & (z >= i // 2))
        def _():
            plus[i].start()

    def send_minus(i):
        @pl.when(wrapped(i // 2))
        def _():
            minus[i].start()

    tail = copy(lru_own.at[pl.ds(BLK - 16, 16)], halo, sp=following)
    query_rows = [pl.ds(pl.multiple_of(x * BLK + h * HALF, HALF), HALF) for h in (0, 1)]
    query_sems = semaphore(), semaphore()
    query_copies = [
        {r: copy(qb.at[rows], qb.at[rows], *query_sems, sp=along_x(r)) for r in (1, 2, 3)} for rows in query_rows
    ]
    others_queries = qb.at[pl.ds(0, (XS - 1) * BLK)]

    def conclude(h):
        half = pl.ds(h * HALF, HALF)
        count_squares(3, h)
        row_scale = lax.rsqrt(
            jnp.sum(squares[half, :], axis=1, keepdims=True) * (1.0 / D) + epsilon_norm
        )
        project(3, h, (0, 1, 2), acc_kv)
        ready = (acc_kv[half, :] * row_scale).astype(jnp.bfloat16)
        lru_own[half, :] = ready[:, 256:]
        if h == 0:
            later = (ZS - 1 - z) + last_of_row.astype(jnp.int32)

            @pl.when(later > 0)
            def _():
                pl.semaphore_wait(alive, later)

        else:

            @pl.when(sp < SP - 1)
            def _():
                tail.start()

        kv[h, :HALF, :] = ready[:, :128]
        kv[h, HROWS:, :] = ready[:, 128:256]
        send_plus(h)
        send_minus(h)
        project(3, h, (3, 4), acc_rest)
        rest = (acc_rest[half, :] * row_scale).astype(jnp.bfloat16)
        qb[query_rows[h], :] = rest[:, :128]
        gate_own[half, :] = rest[:, 128:]
        for r in (1, 3, 2):
            query_copies[h][r].start()

    await_bytes(weights, load_sems.at[0])
    early, late = tokens
    early.arrived(0)
    take(0, 0)
    early.relay_first()
    late.begin()
    early.relay_second()
    early.arrived_from_partner(4)
    take(1, 0)
    early.arrived_from_partner(5)
    take(2, 0)
    early.relay_last()
    late.arrived(0)
    take(0, 1)
    late.relay_first()
    early.arrived_from_partner(6)
    conclude(0)
    late.relay_second()
    late.arrived_from_partner(4)
    take(1, 1)
    late.arrived_from_partner(5)
    take(2, 1)
    late.relay_last()
    late.arrived_from_partner(6)
    conclude(1)

    for group in tokens:
        group.finish()

    weight_sems = semaphore(), semaphore()
    weight_copies = []
    for r in range(1, TP):
        to = lax.rem(tp + r, TP)
        columns = pl.ds(pl.multiple_of(to * OUT, OUT), OUT)
        for k, ref in enumerate((out_lru_ref, out_fox_ref)):
            weight_copies.append(copy(ref.at[:, columns], w_out.at[k, tp], *weight_sems, tp=to))
    for each in weight_copies:
        each.start()
    others_weights = w_out.at[:, pl.ds(0, TP - 1)]
    own_rows = pl.ds(pl.multiple_of(x * BLK, BLK), BLK)
    m_ref[...] = jnp.full_like(m_ref, NEG)
    l_ref[...] = jnp.zeros_like(l_ref)
    acc[...] = jnp.zeros_like(acc)

    def set_bias(slot):
        parts = kv[slot, HALF:HROWS, :].astype(jnp.float32)
        whole = parts[0:2] + parts[2:4] + parts[4:6]
        for g in range(2):
            bias[slot : slot + 1, g * 128 : (g + 1) * 128] = whole[g : g + 1] * -LOG2E

    scale = HEAD_DIM ** (-0.5) * LOG2E

    def joint(parts, axis):
        return parts[0] if len(parts) == 1 else jnp.concatenate(parts, axis=axis)

    def score(buffer, i, slots):
        rows = pl.ds(pl.multiple_of(i * BLK, BLK), BLK)
        buffer[:, : HALF * len(slots)] = lax.dot_general(
            qb[rows, :],
            joint([kv[slot, :HALF, :] for slot in slots], 0),
            (((1,), (1,)), ((), ())),
            preferred_element_type=jnp.float32,
        )

    def absorb(buffer, i, slots, masked=False):
        rows = pl.ds(pl.multiple_of(i * BLK, BLK), BLK)
        width = HALF * len(slots)
        offsets = joint([bias[slot : slot + 1, :] for slot in slots], 1)
        scores = buffer[:, :width] * scale + offsets
        if masked:
            earlier = lax.broadcasted_iota(jnp.int32, scores.shape, 0) >= lax.broadcasted_iota(
                jnp.int32, scores.shape, 1
            )
            scores = jnp.where(earlier, scores, NEG)
        old = m_ref[rows, :]
        new = jnp.maximum(old, jnp.max(scores, axis=1, keepdims=True))
        rescale = jnp.exp2(old - new)
        probs = jnp.exp2(scores - jnp.concatenate([new] * (width // 128), axis=1))
        total = l_ref[rows, :] * rescale
        for g in range(width // 128):
            total = total + probs[:, g * 128 : (g + 1) * 128]
        l_ref[rows, :] = total
        m_ref[rows, :] = new
        acc[rows, :] = acc[rows, :] * rescale + dot(
            probs.astype(jnp.bfloat16), joint([kv[slot, HROWS:, :] for slot in slots], 0)
        )

    def attend(i, slots, masked=False):
        score(scores_a, i, slots)
        absorb(scores_a, i, slots, masked)

    def visit_rest(slots, first):
        def body(i, carry):
            attend(i, slots)
            return carry

        lax.fori_loop(first, XS, body, 0)

    def visit(*slots):
        for slot in slots:
            set_bias(slot)
        score(scores_a, 0, slots)

        def body(k, carry):
            score(scores_b, 2 * k + 1, slots)
            absorb(scores_a, 2 * k, slots)
            score(scores_a, jnp.minimum(2 * k + 2, XS - 1), slots)
            absorb(scores_b, 2 * k + 1, slots)
            return carry

        lax.fori_loop(0, XS // 2, body, 0)

    def receive(i):
        d = i // 2 + 1
        if d < 4:

            @pl.when(z >= d)
            def _():
                plus[i].wait_recv()

            if d < 3:
                send_plus(i + 2)

        @pl.when(wrapped(d))
        def _():
            minus[i].wait_recv()
            if d < 4:
                minus[i + 2].start()

    def take_keys(i):
        d = i // 2 + 1
        @pl.when(z + d >= ZS)
        def _():
            visit(i + 2, i + 8)

        @pl.when((z >= d) & (z + d < ZS))
        def _():
            visit(i + 2)

    set_bias(0)
    set_bias(1)
    attend(x, (0, 1), masked=True)
    receive(0)

    @pl.when(sp > 0)
    def _():
        tail.wait_recv()

    @pl.when(sp == 0)
    def _():
        halo[...] = jnp.zeros_like(halo)

    for load in later_loads:
        load.wait()
    lru_input = lru_own[...].astype(jnp.float32)
    before = halo[8:16, :].astype(jnp.float32)
    joined = jnp.concatenate([before, lru_input], axis=0)
    channels = pl.ds(pl.multiple_of(tp * 128, 128), 128)
    taps = conv_ref[:, channels].astype(jnp.float32)
    conv = jnp.zeros((BLK, 128), jnp.float32)
    for j in range(4):
        shifted = joined if j == 3 else pltpu.roll(joined, 3 - j, 0)
        conv = conv + taps[j : j + 1, :] * shifted[8:, :]
    conv = conv.astype(jnp.bfloat16)
    column = lax.broadcasted_iota(jnp.int32, (64, 128), 1)
    row = lax.broadcasted_iota(jnp.int32, (64, 128), 0)
    left = jnp.where(column == row, 1.0, 0.0).astype(jnp.bfloat16)
    right = jnp.where(column == row + 64, 1.0, 0.0).astype(jnp.bfloat16)

    def block_diagonal(ref):
        return jnp.concatenate([dot(ref[0], left), dot(ref[1], right)], axis=0)

    gates_w = jnp.concatenate([block_diagonal(recur_ref), block_diagonal(input_ref)], axis=1)
    gates = dot(conv, gates_w.astype(jnp.bfloat16))
    gates = 1.0 / (1.0 + jnp.exp(-gates))
    rate = log1p_unit(jnp.exp(-rate_ref[pl.ds(tp, 1), :]))
    log_decay = (-decay_sharpness * rate) * gates[:, :128] + extra_ref[...]
    drive = jnp.sqrt(minus_expm1(2.0 * log_decay)) * gates[:, 128:] * conv.astype(jnp.float32)
    decay = jnp.exp(log_decay)
    place = lax.broadcasted_iota(jnp.int32, (BLK, 128), 0)
    step = 1
    while step < BLK:
        if step < 8:
            inside = place >= step
            decay_back = jnp.where(inside, pltpu.roll(decay, step, 0), 1.0)
            drive_back = jnp.where(inside, pltpu.roll(drive, step, 0), 0.0)
        else:
            decay_back = jnp.concatenate([jnp.ones((step, 128), jnp.float32), decay[:-step]], axis=0)
            drive_back = jnp.concatenate([jnp.zeros((step, 128), jnp.float32), drive[:-step]], axis=0)
        drive = decay * drive_back + drive
        decay = decay * decay_back
        step *= 2
    decays[...] = decay
    drives[...] = drive

    def tile_of(a, b):
        return jnp.concatenate([a, b, jnp.zeros((6, 128), jnp.float32)], axis=0)

    row_tiles[0] = tile_of(decays[BLK - 1 :, :], drives[BLK - 1 :, :])
    row_sems = semaphore(), semaphore()
    row_copies = {
        r: copy(row_tiles.at[0], row_tiles.at[r], *row_sems, sp=along_x(r)) for r in (1, 2, 3)
    }
    others_rows = row_tiles.at[pl.ds(1, XS - 1)]
    for r in (1, 3, 2):
        row_copies[r].start()

    receive(1)
    await_bytes(others_queries, query_sems[1])
    visit_rest((0, 1), x + 1)

    column_copies = {r: copy(col_tiles.at[0], col_tiles.at[r], sp=along_z(r)) for r in range(1, ZS)}
    branch = Gather(copy, gather_sems[0], lru_out, lru_g, along_y(1, c), along_y(3, c), partner)
    one, zero = jnp.ones((1, 128), jnp.float32), jnp.zeros((1, 128), jnp.float32)

    def total_of_row():
        await_bytes(others_rows, row_sems[1])
        whole_decay, whole_state, state = one, zero, zero
        for k in range(XS):
            block = row_tiles[lax.rem(x + XS - k, XS)]
            a, b = block[0:1], block[1:2]
            state = jnp.where(k < x, a * state + b, state)
            whole_state = a * whole_state + b
            whole_decay = whole_decay * a
        col_tiles[0] = tile_of(whole_decay, whole_state)
        for r in range(1, ZS):

            @pl.when(z + r < ZS)
            def _():
                column_copies[r].start()

    def recurrence_out():
        for r in range(1, ZS):

            @pl.when(z >= r)
            def _():
                column_copies[r].wait_recv()

        def row_above(k, state):
            block = col_tiles[z - k]
            return block[0:1] * state + block[1:2]

        state = lax.fori_loop(0, z, row_above, zero)
        for k in range(XS):
            block = row_tiles[lax.rem(x + XS - k, XS)]
            state = jnp.where(k < x, block[0:1] * state + block[1:2], state)
        gate = gate_own[...].astype(jnp.float32)
        inner = 0.7978845608028654 * (gate + 0.044715 * gate * gate * gate)
        gelu = 0.5 * gate * (1.0 + jnp.tanh(inner))
        lru_out[...] = ((drives[...] + decays[...] * state) * gelu).astype(jnp.bfloat16)
        branch.begin()

    beside = {0: total_of_row, 2: recurrence_out, 4: branch.relay}
    for i in range(6):
        take_keys(i)
        if i in beside:
            beside[i]()
        if i < 4:
            receive(i + 2)
        elif i == 4:
            receive(6)
        elif i == 5:
            receive(7)

    right, left = along_x(1), along_x(3)
    out_sent, out_sent_on = semaphore(), semaphore()
    relay_sems, out_sems = [semaphore(), semaphore()], [semaphore(), semaphore()]
    out_copies = []
    for h in (0, 1):
        rows = pl.ds(h * HALF, HALF)
        quarters = [pl.ds(h * HALF + k * 128, 128) for k in (0, 1)]
        out_copies.append(
            {
                "relay": [
                    copy(o_send.at[2, part], o_relay.at[k, part], out_sent, relay_sems[h], sp=to)
                    for k, (part, to) in enumerate(zip(quarters, (right, left)))
                ],
                "near": {
                    r: copy(o_send.at[r, rows], o_recv.at[r, rows], out_sent, out_sems[h], sp=along_x(r))
                    for r in (1, 3)
                },
                "far": [
                    copy(o_relay.at[k, part], o_recv.at[2, part], out_sent_on, out_sems[h], sp=to)
                    for k, (part, to) in enumerate(zip(quarters, (right, left)))
                ],
            }
        )
    stat_sems = semaphore(), semaphore()
    stat_copies = {r: copy(st_send.at[r], st_recv.at[r], *stat_sems, sp=along_x(r)) for r in (1, 2, 3)}
    others_stats = st_recv.at[pl.ds(1, XS - 1)]

    def stats(rows):
        total = jnp.broadcast_to(jnp.sum(l_ref[rows, :], axis=1, keepdims=True), (BLK, 128))
        return packed_rows(m_ref[rows, :]), packed_rows(total)

    def relay_on(h):
        await_bytes(o_relay.at[0, pl.ds(0, HALF)], relay_sems[h])
        for each in out_copies[h]["far"]:
            each.start()

    def block_of(r):
        return lax.rem(x + r, XS)

    @pl.when(z >= 4)
    def _():
        set_bias(14)
        set_bias(15)
        score(scores_a, block_of(2), (14, 15))

    buffers = (scores_a, scores_b)
    turns = (2, 1, 3, 0)
    for k, r in enumerate(turns):

        @pl.when(z >= 4)
        def _():
            if k + 1 < len(turns):
                score(buffers[(k + 1) % 2], block_of(turns[k + 1]), (14, 15))
            absorb(buffers[k % 2], block_of(r), (14, 15))

        if r > 0:
            rows = pl.ds(pl.multiple_of(block_of(r) * BLK, BLK), BLK)
            o_send[r] = acc[rows, :].astype(jnp.bfloat16)
            if r == 2:
                for h in (0, 1):
                    for each in out_copies[h]["relay"]:
                        each.start()
            else:
                for h in (0, 1):
                    out_copies[h]["near"][r].start()
            st_send[r] = jnp.concatenate(stats(rows), axis=0)
            stat_copies[r].start()
    tops, sums = [None] * 4, [None] * 4
    tops[0], sums[0] = stats(own_rows)
    branch.relay_last()

    relay_on(0)

    sources = [(0, c), (0, 1 - c), (3, c), (3, 1 - c), (1, c), (1, 1 - c), (2, c), (2, 1 - c)]

    def branch_product(k, own, slots, which, rows):
        lookup = [None, 0, 1, 4, 2, 5, 3, 6]
        blocks = [own[rows, :] if lookup[i] is None else slots[lookup[i], rows, :] for i in which]
        rights = [w_out[k, along_y(*sources[i])] for i in which]
        return dot(jnp.concatenate(blocks, axis=1), jnp.concatenate(rights, axis=0))

    await_bytes(others_weights, weight_sems[1])
    branch.arrived(0)
    branch.arrived_from_partner(4, 5, 6)
    relay_on(1)
    acc_out[...] = branch_product(0, lru_out, lru_g, range(8), pl.ds(0, BLK))

    await_bytes(others_stats, stat_sems[1])
    for r in (1, 2, 3):
        both = st_recv[r]
        tops[r], sums[r] = both[0:4], both[4:8]
    top = jnp.maximum(jnp.maximum(tops[0], tops[1]), jnp.maximum(tops[2], tops[3]))
    shares = [jnp.exp2(t - top) for t in tops]
    whole = shares[0] * sums[0] + shares[1] * sums[1] + shares[2] * sums[2] + shares[3] * sums[3]
    shares = [s / whole for s in shares]
    heads = [
        Gather(copy, gather_sems[1 + h], fox_out, fox_g, along_y(1, c), along_y(3, c), partner, h * HALF, HALF) for h in (0, 1)
    ]

    def merge(h):
        await_bytes(qb.at[pl.ds(0, (XS - 1) * HALF)], out_sems[h])
        for g in (2 * h, 2 * h + 1):
            part = pl.ds(g * 128, 128)
            mine = pl.ds(pl.multiple_of(x * BLK + g * 128, 128), 128)
            total = unpacked_row(shares[0][g : g + 1]) * acc[mine, :]
            for r in (1, 2, 3):
                total = total + unpacked_row(shares[r][g : g + 1]) * o_recv[r, part, :].astype(jnp.float32)
            fox_out[part, :] = total.astype(jnp.bfloat16)
        heads[h].begin()

    def head_product(h, which):
        rows = pl.ds(h * HALF, HALF)
        return branch_product(1, fox_out, fox_g, which, rows)

    halves = [pl.ds(h * HALF, HALF) for h in (0, 1)]
    out_loads = [
        pltpu.make_async_copy(out_rows.at[half], o_ref.at[half], load_sems.at[7 + h])
        for h, half in enumerate(halves)
    ]

    def write(h):
        heads[h].arrived_from_partner(6)
        out_rows[halves[h], :] = (acc_out[halves[h], :] + head_product(h, (6, 7))).astype(out_rows.dtype)
        out_loads[h].start()

    merge(0)
    merge(1)
    heads[0].relay()
    heads[0].arrived(0)
    acc_out[halves[0], :] += head_product(0, (0, 1))
    heads[1].relay_first()
    heads[0].relay_last()
    heads[1].relay_second()
    heads[1].arrived(0)
    acc_out[halves[1], :] += head_product(1, (0, 1))
    heads[0].arrived_from_partner(4, 5)
    acc_out[halves[0], :] += head_product(0, (2, 3, 4, 5))
    write(0)
    heads[1].relay_last()
    heads[1].arrived_from_partner(4, 5)
    acc_out[halves[1], :] += head_product(1, (2, 3, 4, 5))
    write(1)

    for i, each in enumerate(plus):

        @pl.when((z < ZS - 1) & (z >= i // 2))
        def _():
            each.wait_send()

    for i, each in enumerate(minus):

        @pl.when(wrapped(i // 2))
        def _():
            each.wait_send()

    @pl.when(sp < SP - 1)
    def _():
        tail.wait_send()

    for r in range(1, ZS):

        @pl.when(z + r < ZS)
        def _():
            column_copies[r].wait_send()

    await_bytes(others_weights, weight_sems[0])
    await_bytes(others_queries, query_sems[0])
    await_bytes(others_rows, row_sems[0])
    await_bytes(others_stats, stat_sems[0])
    await_bytes(o_recv.at[pl.ds(1, XS - 1)], out_sent)
    await_bytes(o_relay.at[0], out_sent_on)
    for group in [branch] + heads:
        group.finish()
    for each in out_loads:
        each.wait()


def layer(
    tokens, lru_in, lru_gate_in, query_w, key_w, value_w, conv_weight, recur_gate_w, input_gate_w,
    rate_param, decay_extra, forget_cum, out_lru, out_fox,
):
    vmem = pl.BlockSpec(memory_space=pltpu.VMEM)
    hbm = pl.BlockSpec(memory_space=pl.ANY)
    bf16, f32 = jnp.bfloat16, jnp.float32
    return pl.pallas_call(
        layer_kernel,
        out_shape=jax.ShapeDtypeStruct((BLK, OUT), f32),
        in_specs=[hbm] * 6 + [vmem, hbm, hbm, vmem, hbm, vmem, hbm, hbm],
        out_specs=hbm,
        scratch_shapes=[
            pltpu.VMEM((BLK, FEAT), bf16),
            pltpu.VMEM((2, 64, 64), bf16),
            pltpu.VMEM((2, 64, 64), bf16),
            pltpu.VMEM((BLK, 128), f32),
            pltpu.VMEM((5, D, 128), bf16),
            pltpu.VMEM((7, BLK, FEAT), bf16),
            pltpu.VMEM((BLK, 384), f32),
            pltpu.VMEM((BLK, 256), f32),
            pltpu.VMEM((BLK, BLK), f32),
            pltpu.VMEM((BLK, BLK), f32),
            pltpu.VMEM((BLK, 128), f32),
            pltpu.VMEM((2 * ZS, PIECE, 128), bf16),
            pltpu.VMEM((XS * BLK, 128), bf16),
            pltpu.VMEM((2 * ZS, HALF), f32),
            pltpu.VMEM((XS * BLK, 128), f32),
            pltpu.VMEM((XS * BLK, 128), f32),
            pltpu.VMEM((XS * BLK, 128), f32),
            pltpu.VMEM((XS, BLK, 128), bf16),
            pltpu.VMEM((XS, 8, 128), f32),
            pltpu.VMEM((2, BLK, 128), bf16),
            pltpu.VMEM((XS, BLK, 128), bf16),
            pltpu.VMEM((XS, 8, 128), f32),
            pltpu.VMEM((BLK, 128), bf16),
            pltpu.VMEM((16, 128), bf16),
            pltpu.VMEM((BLK, 128), bf16),
            pltpu.VMEM((BLK, 128), f32),
            pltpu.VMEM((BLK, 128), f32),
            pltpu.VMEM((XS, 8, 128), f32),
            pltpu.VMEM((ZS, 8, 128), f32),
            pltpu.VMEM((BLK, 128), bf16),
            pltpu.VMEM((7, BLK, 128), bf16),
            pltpu.VMEM((BLK, 128), bf16),
            pltpu.VMEM((7, BLK, 128), bf16),
            pltpu.VMEM((2, TP, 128, OUT), bf16),
            pltpu.VMEM((BLK, OUT), f32),
            pltpu.VMEM((BLK, OUT), f32),
            pltpu.SemaphoreType.DMA((COPIES,)),
            pltpu.SemaphoreType.DMA((9,)),
            pltpu.SemaphoreType.REGULAR,
        ],
        compiler_params=pltpu.CompilerParams(collective_id=1, has_side_effects=True),
        cost_estimate=pl.CostEstimate(flops=5_000_000_000, bytes_accessed=8_000_000, transcendentals=9_000_000),
    )(
        tokens, lru_in, lru_gate_in, query_w, key_w, value_w, conv_weight, recur_gate_w, input_gate_w,
        rate_param.reshape(TP, 128), decay_extra, forget_cum.reshape(4, 128), out_lru, out_fox,
    ).astype(bf16)


def solution(mesh):
    placed = (
        P("sp", "tp"),
        P(None, "tp"),
        P(None, "tp"),
        P(None, "tp"),
        P(None, "tp"),
        P(None, "tp"),
        P(),
        P(),
        P(),
        P(),
        P("sp", "tp"),
        P("sp", "tp"),
        P("tp", None),
        P("tp", None),
    )
    return jax.shard_map(
        layer, mesh=mesh, in_specs=placed, out_specs=P("sp", "tp"), check_vma=False
    )
```

```python
import jax
import jax.numpy as jnp
from jax import lax
from jax.experimental import pallas as pl
from jax.experimental.pallas import tpu as pltpu
from jax.sharding import PartitionSpec as P

MESH = pl.DeviceIdType.MESH
D = 2048
HEAD_DIM = 128
SP, TP = 32, 8
ZS, XS, YS = 8, 4, 4
BLK = 512
HALF = BLK // 2
FEAT = D // TP
OUT = D // TP
HROWS = HALF + 16
PIECE = HROWS + HALF
LOG2E = 1.4426950408889634
NEG = -1e30
COPIES = 96
ROWS = 256

decay_sharpness = 8.0
epsilon_norm = 1e-06


def eye_mask():
    return lax.broadcasted_iota(jnp.int32, (128, 128), 0) == lax.broadcasted_iota(
        jnp.int32, (128, 128), 1
    )


def packed_rows(column):
    eye = eye_mask()
    return jnp.concatenate(
        [
            jnp.sum(jnp.where(eye, column[g * 128 : (g + 1) * 128], 0.0), axis=0, keepdims=True)
            for g in range(4)
        ],
        axis=0,
    )


def unpacked_row(row):
    return jnp.sum(
        jnp.where(eye_mask(), jnp.broadcast_to(row, (128, 128)), 0.0), axis=1, keepdims=True
    )


def dot(a, b):
    return jnp.dot(a, b, preferred_element_type=jnp.float32)


def log1p_unit(u):
    s = u / (2.0 + u)
    square = s * s
    total = jnp.full_like(s, 1.0 / 19.0)
    for k in range(17, 0, -2):
        total = total * square + 1.0 / k
    return 2.0 * s * total


def minus_expm1(x):
    near = jnp.full_like(x, 1.0 / 362880.0)
    for k in (40320.0, 5040.0, 720.0, 120.0, 24.0, 6.0, 2.0, 1.0):
        near = near * x + 1.0 / k
    return jnp.where(x > -0.5, -near * x, 1.0 - jnp.exp(x))


def await_bytes(ref, semaphore):
    pltpu.make_async_copy(ref, ref, semaphore).wait()


class Gather:
    def __init__(self, copy, sems, own, slots, up, down, partner, start=0, rows=BLK):
        half = rows // 2
        first, second = pl.ds(start, half), pl.ds(start + half, half)

        def send(a, b, part, to, k):
            source = own if a is None else slots.at[a]
            return copy(source.at[part], slots.at[b, part], send=sems[10], recv=sems[k], tp=to)

        plan = [
            (None, 0, pl.ds(start, rows), partner, 0),
            (None, 1, first, up, 1),
            (None, 1, second, up, 2),
            (None, 2, second, down, 3),
            (None, 2, first, down, 4),
            (1, 3, first, up, 5),
            (2, 3, second, down, 6),
            (1, 4, first, partner, 7),
            (1, 4, second, partner, 7),
            (2, 5, first, partner, 8),
            (2, 5, second, partner, 8),
            (3, 6, first, partner, 9),
            (3, 6, second, partner, 9),
        ]
        self.copies = [send(*each) for each in plan]
        self.sems, self.slots, self.rows = sems, slots, pl.ds(start, rows)

    def start(self, *which):
        for i in which:
            self.copies[i].start()

    def arrived(self, *which):
        for i in which:
            self.copies[i].wait_recv()

    def arrived_from_partner(self, *slots):
        for slot in slots:
            await_bytes(self.slots.at[slot, self.rows], self.sems[slot + 3])

    def finish(self):
        await_bytes(self.slots.at[:, self.rows], self.sems[10])

    def begin(self):
        self.start(1, 3, 0, 2, 4)

    def relay_first(self):
        self.arrived(1)
        self.start(5, 7)
        self.arrived(3)
        self.start(6, 10)

    def relay_second(self):
        self.arrived(2)
        self.start(8)
        self.arrived(4)
        self.start(9)

    def relay(self):
        self.relay_first()
        self.relay_second()

    def relay_last(self):
        self.arrived(5)
        self.start(11)
        self.arrived(6)
        self.start(12)


def layer_kernel(
    tok_hbm, lru_w_hbm, gate_w_hbm, query_w_hbm, key_w_hbm, value_w_hbm,
    conv_ref, recur_hbm, input_hbm, rate_ref, extra_hbm, f_ref, out_lru_ref, out_fox_ref,
    o_ref,
    tok_ref, recur_ref, input_ref, extra_ref, weights, tokg, acc_kv, acc_rest, scores_a, scores_b, squares,
    kv, qb, bias, m_ref, acc, o_send, st_send, o_relay, o_recv, st_recv,
    lru_own, halo, gate_own, decays, drives, row_tiles, col_tiles,
    lru_out, lru_g, fox_out, fox_g, w_out, acc_out, out_rows,
    copy_sems, load_sems, alive,
):
    sp, tp = lax.axis_index("sp"), lax.axis_index("tp")
    z, x = lax.div(sp, XS), lax.rem(sp, XS)
    y, c = lax.div(tp, 2), lax.rem(tp, 2)
    above = lax.rem(z + 1, ZS) * XS + x
    below = lax.rem(z + ZS - 1, ZS) * XS + x
    partner = y * 2 + 1 - c

    def along_y(r, core):
        return lax.rem(y + r, YS) * 2 + core

    def along_x(r):
        return z * XS + lax.rem(x + r, XS)

    def along_z(r):
        return lax.rem(z + r, ZS) * XS + x

    following, preceding = lax.rem(sp + 1, SP), lax.rem(sp + SP - 1, SP)
    used = [0]

    def semaphore():
        used[0] += 1
        return copy_sems.at[used[0] - 1]

    def copy(src, dst, send=None, recv=None, **where):
        return pltpu.make_async_remote_copy(
            src_ref=src, dst_ref=dst, send_sem=send or semaphore(), recv_sem=recv or semaphore(),
            device_id=where, device_id_type=MESH,
        )

    gather_sems = [[semaphore() for k in range(11)] for group in range(3)]

    tok_load = pltpu.make_async_copy(tok_hbm, tok_ref, load_sems.at[1])
    tok_load.start()
    loads = [
        pltpu.make_async_copy(w, weights.at[i], load_sems.at[0])
        for i, w in enumerate((key_w_hbm, value_w_hbm, lru_w_hbm, query_w_hbm, gate_w_hbm))
    ]
    own_blocks = pl.ds(2 * tp, 2)
    own_columns = pl.ds(pl.multiple_of(tp * OUT, OUT), OUT)
    later_loads = [
        pltpu.make_async_copy(extra_hbm, extra_ref, load_sems.at[2]),
        pltpu.make_async_copy(recur_hbm.at[own_blocks], recur_ref, load_sems.at[3]),
        pltpu.make_async_copy(input_hbm.at[own_blocks], input_ref, load_sems.at[4]),
        pltpu.make_async_copy(out_lru_ref.at[:, own_columns], w_out.at[0, tp], load_sems.at[5]),
        pltpu.make_async_copy(out_fox_ref.at[:, own_columns], w_out.at[1, tp], load_sems.at[6]),
    ]
    for load in loads + later_loads:
        load.start()

    barrier = pltpu.get_barrier_semaphore()

    def tell(semaphore, **where):
        pl.semaphore_signal(semaphore, inc=1, device_id=where, device_id_type=MESH)

    for r in range(1, TP):
        tell(barrier, tp=lax.rem(tp + r, TP))
    for r in range(1, XS):
        tell(barrier, sp=along_x(r))
    for r in range(1, ZS):

        @pl.when(z + r < ZS)
        def _():
            tell(barrier, sp=along_z(r))

    last_of_row = (x == XS - 1) & (z < ZS - 1)
    first_of_row = (x == 0) & (z > 0)

    @pl.when(last_of_row)
    def _():
        tell(barrier, sp=following)

    pl.semaphore_wait(barrier, TP - 1 + XS - 1 + z + first_of_row.astype(jnp.int32))
    for r in range(1, ZS):

        @pl.when(z >= r)
        def _():
            tell(alive, sp=along_z(ZS - r))

    @pl.when(first_of_row)
    def _():
        tell(alive, sp=preceding)

    tokens = [
        Gather(copy, gather_sems[h], tok_ref, tokg, along_y(1, c), along_y(3, c), partner, h * HALF, HALF) for h in (0, 1)
    ]
    tok_load.wait()
    tokens[0].begin()
    forget = f_ref[...]
    high = forget.astype(jnp.bfloat16).astype(jnp.float32)
    middle = (forget - high).astype(jnp.bfloat16).astype(jnp.float32)
    low = forget - high - middle
    for h in (0, 1):
        lines = [part[2 * h : 2 * h + 2] for part in (high, middle, low)]
        kv[h, HALF:HROWS, :] = jnp.concatenate(
            lines + [jnp.zeros((10, 128), jnp.float32)], axis=0
        ).astype(jnp.bfloat16)

    def features(r, core):
        return pl.ds(pl.multiple_of(along_y(r, core) * FEAT, FEAT), FEAT)

    def pair(slot, h):
        rows = pl.ds(h * HALF, HALF)
        block = tok_ref if slot == 0 else tokg.at[slot]
        other = tokg.at[0] if slot == 0 else tokg.at[slot + 3]
        return block[rows, :], other[rows, :]

    distance = {0: 0, 1: 3, 2: 1, 3: 2}

    def project(slot, h, group, target):
        rows = [features(distance[slot], c), features(distance[slot], 1 - c)]
        right = jnp.concatenate(
            [jnp.concatenate([weights[i, part, :] for part in rows], axis=0) for i in group], axis=1
        )
        product = dot(jnp.concatenate(pair(slot, h), axis=1), right)
        half = pl.ds(h * HALF, HALF)
        target[half, :] = product if slot == 0 else target[half, :] + product

    def count_squares(slot, h):
        half = pl.ds(h * HALF, HALF)
        total = jnp.zeros((HALF, 128), jnp.float32) if slot == 0 else squares[half, :]
        for piece in pair(slot, h):
            for g in range(FEAT // 128):
                value = piece[:, g * 128 : (g + 1) * 128].astype(jnp.float32)
                total = total + value * value
        squares[half, :] = total

    def take(slot, h):
        project(slot, h, (0, 1, 2), acc_kv)
        project(slot, h, (3, 4), acc_rest)
        count_squares(slot, h)

    plus = [(0, 2), (1, 3), (2, 4), (3, 5), (4, 6), (5, 7)]
    minus = [(0, 8), (1, 9), (8, 10), (9, 11), (10, 12), (11, 13), (12, 14), (13, 15)]
    plus = [copy(kv.at[a], kv.at[b], sp=above) for a, b in plus]
    minus = [copy(kv.at[a], kv.at[b], sp=below) for a, b in minus]

    def wrapped(d):
        return lax.rem(z + d, ZS) < 4

    def send_plus(i):
        @pl.when((z < ZS - 1) & (z >= i // 2))
        def _():
            plus[i].start()

    def send_minus(i):
        @pl.when(wrapped(i // 2))
        def _():
            minus[i].start()

    last_row = z == ZS - 1

    def receive_plus(i, where=True):
        d = i // 2 + 1

        @pl.when((z >= d) & where)
        def _():
            plus[i].wait_recv()

        if d < 3:

            @pl.when((z < ZS - 1) & (z >= d) & where)
            def _():
                plus[i + 2].start()

    def receive_minus(i, where=True):
        d = i // 2 + 1

        @pl.when(wrapped(d) & where)
        def _():
            minus[i].wait_recv()
            if d < 4:
                minus[i + 2].start()

    tail = copy(lru_own.at[pl.ds(BLK - 16, 16)], halo, sp=following)
    query_rows = [pl.ds(pl.multiple_of(x * BLK + h * HALF, HALF), HALF) for h in (0, 1)]
    query_sems = semaphore(), semaphore()
    query_copies = [
        {r: copy(qb.at[rows], qb.at[rows], *query_sems, sp=along_x(r)) for r in (1, 2, 3)} for rows in query_rows
    ]
    others_queries = qb.at[pl.ds(0, (XS - 1) * BLK)]

    def conclude(h):
        half = pl.ds(h * HALF, HALF)
        count_squares(3, h)
        row_scale = lax.rsqrt(
            jnp.sum(squares[half, :], axis=1, keepdims=True) * (1.0 / D) + epsilon_norm
        )
        project(3, h, (0, 1, 2), acc_kv)
        ready = (acc_kv[half, :] * row_scale).astype(jnp.bfloat16)
        lru_own[half, :] = ready[:, 256:]
        if h == 0:
            later = (ZS - 1 - z) + last_of_row.astype(jnp.int32)

            @pl.when(later > 0)
            def _():
                pl.semaphore_wait(alive, later)

        else:

            @pl.when(sp < SP - 1)
            def _():
                tail.start()

        kv[h, :HALF, :] = ready[:, :128]
        kv[h, HROWS:, :] = ready[:, 128:256]
        send_plus(h)
        send_minus(h)
        project(3, h, (3, 4), acc_rest)
        rest = (acc_rest[half, :] * row_scale).astype(jnp.bfloat16)
        qb[query_rows[h], :] = rest[:, :128]
        gate_own[half, :] = rest[:, 128:]
        for r in (1, 3, 2):
            query_copies[h][r].start()

    await_bytes(weights, load_sems.at[0])
    early, late = tokens
    early.arrived(0)
    take(0, 0)
    early.relay_first()
    late.begin()
    early.relay_second()
    early.arrived_from_partner(4)
    take(1, 0)
    early.arrived_from_partner(5)
    take(2, 0)
    early.relay_last()
    late.arrived(0)
    take(0, 1)
    late.relay_first()
    early.arrived_from_partner(6)
    conclude(0)
    late.relay_second()
    late.arrived_from_partner(4)
    take(1, 1)
    late.arrived_from_partner(5)
    take(2, 1)
    receive_minus(0, last_row)
    late.relay_last()
    late.arrived_from_partner(6)
    conclude(1)

    for group in tokens:
        group.finish()

    weight_sems = semaphore(), semaphore()
    weight_copies = []
    for r in range(1, TP):
        to = lax.rem(tp + r, TP)
        columns = pl.ds(pl.multiple_of(to * OUT, OUT), OUT)
        for k, ref in enumerate((out_lru_ref, out_fox_ref)):
            weight_copies.append(copy(ref.at[:, columns], w_out.at[k, tp], *weight_sems, tp=to))
    for each in weight_copies:
        each.start()
    others_weights = w_out.at[:, pl.ds(0, TP - 1)]
    own_rows = pl.ds(pl.multiple_of(x * BLK, BLK), BLK)
    m_ref[...] = jnp.full_like(m_ref, NEG)
    acc[...] = jnp.zeros_like(acc)

    def set_bias(slot):
        parts = kv[slot, HALF:HROWS, :].astype(jnp.float32)
        whole = parts[0:2] + parts[2:4] + parts[4:6]
        for g in range(2):
            bias[slot : slot + 1, g * 128 : (g + 1) * 128] = whole[g : g + 1] * -LOG2E

    scale = HEAD_DIM ** (-0.5) * LOG2E

    def joint(parts, axis):
        return parts[0] if len(parts) == 1 else jnp.concatenate(parts, axis=axis)

    def score(buffer, i, slots):
        rows = pl.ds(i * BLK if isinstance(i, int) else pl.multiple_of(i * BLK, BLK), BLK)
        buffer[:, : HALF * len(slots)] = lax.dot_general(
            qb[rows, :],
            joint([kv[slot, :HALF, :] for slot in slots], 0),
            (((1,), (1,)), ((), ())),
            preferred_element_type=jnp.float32,
        )

    def absorb(buffer, i, slots, masked=False):
        width = HALF * len(slots)
        offsets = joint([bias[slot : slot + 1, :] for slot in slots], 1)
        values = joint([kv[slot, HROWS:, :] for slot in slots], 0)
        values = jnp.concatenate([values, jnp.ones_like(values)], axis=1)
        start = i * BLK if isinstance(i, int) else pl.multiple_of(i * BLK, BLK)
        for part in range(0, BLK, ROWS):
            rows = pl.ds(start + part, ROWS)
            scores = buffer[part : part + ROWS, :width] * scale + offsets
            if masked:
                earlier = lax.broadcasted_iota(jnp.int32, scores.shape, 0) + part >= (
                    lax.broadcasted_iota(jnp.int32, scores.shape, 1)
                )
                scores = jnp.where(earlier, scores, NEG)
            old = m_ref[rows, :]
            new = jnp.maximum(old, jnp.max(scores, axis=1, keepdims=True))
            rescale = jnp.exp2(old - new)
            probs = jnp.exp2(scores - jnp.concatenate([new] * (width // 128), axis=1))
            m_ref[rows, :] = new
            acc[rows, :] = acc[rows, :] * jnp.concatenate([rescale] * 2, axis=1) + dot(
                probs.astype(jnp.bfloat16), values
            )

    def attend(i, slots, masked=False):
        score(scores_a, i, slots)
        absorb(scores_a, i, slots, masked)

    def visit_rest(slots, first):
        def body(i, carry):
            attend(i, slots)
            return carry

        lax.fori_loop(first, XS, body, 0)

    def visit(*slots):
        for slot in slots:
            set_bias(slot)
        score(scores_a, 0, slots)
        pair = scores_a, scores_b
        for k in range(XS):
            if k + 1 < XS:
                score(pair[(k + 1) % 2], k + 1, slots)
            absorb(pair[k % 2], k, slots)

    def take_keys(i):
        d = i // 2 + 1
        @pl.when(z + d >= ZS)
        def _():
            visit(i + 2, i + 8)

        @pl.when((z >= d) & (z + d < ZS))
        def _():
            visit(i + 2)

    set_bias(0)
    set_bias(1)
    attend(x, (0, 1), masked=True)
    receive_plus(0)
    receive_minus(0, z < ZS - 1)
    receive_minus(1, last_row)

    @pl.when(sp > 0)
    def _():
        tail.wait_recv()

    @pl.when(sp == 0)
    def _():
        halo[...] = jnp.zeros_like(halo)

    for load in later_loads:
        load.wait()
    lru_input = lru_own[...].astype(jnp.float32)
    before = halo[8:16, :].astype(jnp.float32)
    joined = jnp.concatenate([before, lru_input], axis=0)
    channels = pl.ds(pl.multiple_of(tp * 128, 128), 128)
    taps = conv_ref[:, channels].astype(jnp.float32)
    conv = jnp.zeros((BLK, 128), jnp.float32)
    for j in range(4):
        shifted = joined if j == 3 else pltpu.roll(joined, 3 - j, 0)
        conv = conv + taps[j : j + 1, :] * shifted[8:, :]
    conv = conv.astype(jnp.bfloat16)
    column = lax.broadcasted_iota(jnp.int32, (64, 128), 1)
    row = lax.broadcasted_iota(jnp.int32, (64, 128), 0)
    left = jnp.where(column == row, 1.0, 0.0).astype(jnp.bfloat16)
    right = jnp.where(column == row + 64, 1.0, 0.0).astype(jnp.bfloat16)

    def block_diagonal(ref):
        return jnp.concatenate([dot(ref[0], left), dot(ref[1], right)], axis=0)

    gates_w = jnp.concatenate([block_diagonal(recur_ref), block_diagonal(input_ref)], axis=1)
    gates = dot(conv, gates_w.astype(jnp.bfloat16))
    gates = 1.0 / (1.0 + jnp.exp(-gates))
    rate = log1p_unit(jnp.exp(-rate_ref[pl.ds(tp, 1), :]))
    log_decay = (-decay_sharpness * rate) * gates[:, :128] + extra_ref[...]
    drive = jnp.sqrt(minus_expm1(2.0 * log_decay)) * gates[:, 128:] * conv.astype(jnp.float32)
    decay = jnp.exp(log_decay)
    place = lax.broadcasted_iota(jnp.int32, (BLK, 128), 0)
    step = 1
    while step < BLK:
        if step < 8:
            inside = place >= step
            decay_back = jnp.where(inside, pltpu.roll(decay, step, 0), 1.0)
            drive_back = jnp.where(inside, pltpu.roll(drive, step, 0), 0.0)
        else:
            decay_back = jnp.concatenate([jnp.ones((step, 128), jnp.float32), decay[:-step]], axis=0)
            drive_back = jnp.concatenate([jnp.zeros((step, 128), jnp.float32), drive[:-step]], axis=0)
        drive = decay * drive_back + drive
        decay = decay * decay_back
        step *= 2
    decays[...] = decay
    drives[...] = drive

    def tile_of(a, b):
        return jnp.concatenate([a, b, jnp.zeros((6, 128), jnp.float32)], axis=0)

    row_tiles[0] = tile_of(decays[BLK - 1 :, :], drives[BLK - 1 :, :])
    row_sems = semaphore(), semaphore()
    row_copies = {
        r: copy(row_tiles.at[0], row_tiles.at[r], *row_sems, sp=along_x(r)) for r in (1, 2, 3)
    }
    others_rows = row_tiles.at[pl.ds(1, XS - 1)]
    for r in (1, 3, 2):
        row_copies[r].start()

    receive_minus(1, z < ZS - 1)
    receive_plus(1, z < ZS - 1)
    receive_minus(2, z >= ZS - 2)
    await_bytes(others_queries, query_sems[1])
    visit_rest((0, 1), x + 1)

    column_copies = {r: copy(col_tiles.at[0], col_tiles.at[r], sp=along_z(r)) for r in range(1, ZS)}
    branch = Gather(copy, gather_sems[0], lru_out, lru_g, along_y(1, c), along_y(3, c), partner)
    one, zero = jnp.ones((1, 128), jnp.float32), jnp.zeros((1, 128), jnp.float32)

    def total_of_row():
        await_bytes(others_rows, row_sems[1])
        whole_decay, whole_state, state = one, zero, zero
        for k in range(XS):
            block = row_tiles[lax.rem(x + XS - k, XS)]
            a, b = block[0:1], block[1:2]
            state = jnp.where(k < x, a * state + b, state)
            whole_state = a * whole_state + b
            whole_decay = whole_decay * a
        col_tiles[0] = tile_of(whole_decay, whole_state)
        for r in range(1, ZS):

            @pl.when(z + r < ZS)
            def _():
                column_copies[r].start()

    def recurrence_out():
        for r in range(1, ZS):

            @pl.when(z >= r)
            def _():
                column_copies[r].wait_recv()

        def row_above(k, state):
            block = col_tiles[z - k]
            return block[0:1] * state + block[1:2]

        state = lax.fori_loop(0, z, row_above, zero)
        for k in range(XS):
            block = row_tiles[lax.rem(x + XS - k, XS)]
            state = jnp.where(k < x, block[0:1] * state + block[1:2], state)
        gate = gate_own[...].astype(jnp.float32)
        inner = 0.7978845608028654 * (gate + 0.044715 * gate * gate * gate)
        gelu = 0.5 * gate * (1.0 + jnp.tanh(inner))
        lru_out[...] = ((drives[...] + decays[...] * state) * gelu).astype(jnp.bfloat16)
        branch.begin()

    beside = {0: total_of_row, 2: recurrence_out, 4: branch.relay}
    receive_minus(2, z < ZS - 2)
    for i in range(6):
        take_keys(i)
        if i in beside:
            beside[i]()
        if i == 0:
            receive_plus(1, last_row)
        if i < 4:
            receive_plus(i + 2)
        if i < 5:
            receive_minus(i + 3)

    right, left = along_x(1), along_x(3)
    out_sent, out_sent_on = semaphore(), semaphore()
    relay_sems, out_sems = [semaphore(), semaphore()], [semaphore(), semaphore()]
    out_copies = []
    for h in (0, 1):
        rows = pl.ds(h * HALF, HALF)
        quarters = [pl.ds(h * HALF + k * 128, 128) for k in (0, 1)]
        out_copies.append(
            {
                "relay": [
                    copy(o_send.at[2, part], o_relay.at[k, part], out_sent, relay_sems[h], sp=to)
                    for k, (part, to) in enumerate(zip(quarters, (right, left)))
                ],
                "near": {
                    r: copy(o_send.at[r, rows], o_recv.at[r, rows], out_sent, out_sems[h], sp=along_x(r))
                    for r in (1, 3)
                },
                "far": [
                    copy(o_relay.at[k, part], o_recv.at[2, part], out_sent_on, out_sems[h], sp=to)
                    for k, (part, to) in enumerate(zip(quarters, (right, left)))
                ],
            }
        )
    stat_sems = semaphore(), semaphore()
    stat_copies = {r: copy(st_send.at[r], st_recv.at[r], *stat_sems, sp=along_x(r)) for r in (1, 2, 3)}
    others_stats = st_recv.at[pl.ds(1, XS - 1)]

    def stats(rows):
        return packed_rows(m_ref[rows, :]), packed_rows(acc[rows, 128:])

    def relay_on(h):
        await_bytes(o_relay.at[0, pl.ds(0, HALF)], relay_sems[h])
        for each in out_copies[h]["far"]:
            each.start()

    def block_of(r):
        return lax.rem(x + r, XS)

    @pl.when(z >= 4)
    def _():
        set_bias(14)
        set_bias(15)
        score(scores_a, block_of(2), (14, 15))

    buffers = (scores_a, scores_b)
    turns = (2, 1, 3, 0)
    for k, r in enumerate(turns):

        @pl.when(z >= 4)
        def _():
            if k + 1 < len(turns):
                score(buffers[(k + 1) % 2], block_of(turns[k + 1]), (14, 15))
            absorb(buffers[k % 2], block_of(r), (14, 15))

        if r > 0:
            rows = pl.ds(pl.multiple_of(block_of(r) * BLK, BLK), BLK)
            st_send[r] = jnp.concatenate(stats(rows), axis=0)
            stat_copies[r].start()
            o_send[r] = acc[rows, :128].astype(jnp.bfloat16)
            if r == 2:
                for h in (0, 1):
                    for each in out_copies[h]["relay"]:
                        each.start()
            else:
                for h in (0, 1):
                    out_copies[h]["near"][r].start()
    tops, sums = [None] * 4, [None] * 4
    tops[0], sums[0] = stats(own_rows)
    branch.relay_last()

    relay_on(0)

    sources = [(0, c), (0, 1 - c), (3, c), (3, 1 - c), (1, c), (1, 1 - c), (2, c), (2, 1 - c)]

    def branch_product(k, own, slots, which, rows):
        lookup = [None, 0, 1, 4, 2, 5, 3, 6]
        blocks = [own[rows, :] if lookup[i] is None else slots[lookup[i], rows, :] for i in which]
        rights = [w_out[k, along_y(*sources[i])] for i in which]
        return dot(jnp.concatenate(blocks, axis=1), jnp.concatenate(rights, axis=0))

    await_bytes(others_weights, weight_sems[1])
    branch.arrived(0)
    branch.arrived_from_partner(4, 5, 6)
    relay_on(1)
    acc_out[...] = branch_product(0, lru_out, lru_g, range(8), pl.ds(0, BLK))

    await_bytes(others_stats, stat_sems[1])
    for r in (1, 2, 3):
        both = st_recv[r]
        tops[r], sums[r] = both[0:4], both[4:8]
    top = jnp.maximum(jnp.maximum(tops[0], tops[1]), jnp.maximum(tops[2], tops[3]))
    shares = [jnp.exp2(t - top) for t in tops]
    whole = shares[0] * sums[0] + shares[1] * sums[1] + shares[2] * sums[2] + shares[3] * sums[3]
    shares = [s / whole for s in shares]
    heads = [
        Gather(copy, gather_sems[1 + h], fox_out, fox_g, along_y(1, c), along_y(3, c), partner, h * HALF, HALF) for h in (0, 1)
    ]

    def merge(h):
        await_bytes(qb.at[pl.ds(0, (XS - 1) * HALF)], out_sems[h])
        for g in (2 * h, 2 * h + 1):
            part = pl.ds(g * 128, 128)
            mine = pl.ds(pl.multiple_of(x * BLK + g * 128, 128), 128)
            total = unpacked_row(shares[0][g : g + 1]) * acc[mine, :128]
            for r in (1, 2, 3):
                total = total + unpacked_row(shares[r][g : g + 1]) * o_recv[r, part, :].astype(jnp.float32)
            fox_out[part, :] = total.astype(jnp.bfloat16)
        heads[h].begin()

    def head_product(h, which):
        rows = pl.ds(h * HALF, HALF)
        return branch_product(1, fox_out, fox_g, which, rows)

    halves = [pl.ds(h * HALF, HALF) for h in (0, 1)]
    out_loads = [
        pltpu.make_async_copy(out_rows.at[half], o_ref.at[half], load_sems.at[7 + h])
        for h, half in enumerate(halves)
    ]

    def write(h):
        heads[h].arrived_from_partner(6)
        out_rows[halves[h], :] = (acc_out[halves[h], :] + head_product(h, (6, 7))).astype(out_rows.dtype)
        out_loads[h].start()

    merge(0)
    merge(1)
    heads[0].relay()
    heads[0].arrived(0)
    acc_out[halves[0], :] += head_product(0, (0, 1))
    heads[1].relay_first()
    heads[0].relay_last()
    heads[1].relay_second()
    heads[1].arrived(0)
    acc_out[halves[1], :] += head_product(1, (0, 1))
    heads[0].arrived_from_partner(4, 5)
    acc_out[halves[0], :] += head_product(0, (2, 3, 4, 5))
    write(0)
    heads[1].relay_last()
    heads[1].arrived_from_partner(4, 5)
    acc_out[halves[1], :] += head_product(1, (2, 3, 4, 5))
    write(1)

    for i, each in enumerate(plus):

        @pl.when((z < ZS - 1) & (z >= i // 2))
        def _():
            each.wait_send()

    for i, each in enumerate(minus):

        @pl.when(wrapped(i // 2))
        def _():
            each.wait_send()

    @pl.when(sp < SP - 1)
    def _():
        tail.wait_send()

    for r in range(1, ZS):

        @pl.when(z + r < ZS)
        def _():
            column_copies[r].wait_send()

    await_bytes(others_weights, weight_sems[0])
    await_bytes(others_queries, query_sems[0])
    await_bytes(others_rows, row_sems[0])
    await_bytes(others_stats, stat_sems[0])
    await_bytes(o_recv.at[pl.ds(1, XS - 1)], out_sent)
    await_bytes(o_relay.at[0], out_sent_on)
    for group in [branch] + heads:
        group.finish()
    for each in out_loads:
        each.wait()


def layer(
    tokens, lru_in, lru_gate_in, query_w, key_w, value_w, conv_weight, recur_gate_w, input_gate_w,
    rate_param, decay_extra, forget_cum, out_lru, out_fox,
):
    vmem = pl.BlockSpec(memory_space=pltpu.VMEM)
    hbm = pl.BlockSpec(memory_space=pl.ANY)
    bf16, f32 = jnp.bfloat16, jnp.float32
    return pl.pallas_call(
        layer_kernel,
        out_shape=jax.ShapeDtypeStruct((BLK, OUT), f32),
        in_specs=[hbm] * 6 + [vmem, hbm, hbm, vmem, hbm, vmem, hbm, hbm],
        out_specs=hbm,
        scratch_shapes=[
            pltpu.VMEM((BLK, FEAT), bf16),
            pltpu.VMEM((2, 64, 64), bf16),
            pltpu.VMEM((2, 64, 64), bf16),
            pltpu.VMEM((BLK, 128), f32),
            pltpu.VMEM((5, D, 128), bf16),
            pltpu.VMEM((7, BLK, FEAT), bf16),
            pltpu.VMEM((BLK, 384), f32),
            pltpu.VMEM((BLK, 256), f32),
            pltpu.VMEM((BLK, BLK), f32),
            pltpu.VMEM((BLK, BLK), f32),
            pltpu.VMEM((BLK, 128), f32),
            pltpu.VMEM((2 * ZS, PIECE, 128), bf16),
            pltpu.VMEM((XS * BLK, 128), bf16),
            pltpu.VMEM((2 * ZS, HALF), f32),
            pltpu.VMEM((XS * BLK, 128), f32),
            pltpu.VMEM((XS * BLK, 256), f32),
            pltpu.VMEM((XS, BLK, 128), bf16),
            pltpu.VMEM((XS, 8, 128), f32),
            pltpu.VMEM((2, BLK, 128), bf16),
            pltpu.VMEM((XS, BLK, 128), bf16),
            pltpu.VMEM((XS, 8, 128), f32),
            pltpu.VMEM((BLK, 128), bf16),
            pltpu.VMEM((16, 128), bf16),
            pltpu.VMEM((BLK, 128), bf16),
            pltpu.VMEM((BLK, 128), f32),
            pltpu.VMEM((BLK, 128), f32),
            pltpu.VMEM((XS, 8, 128), f32),
            pltpu.VMEM((ZS, 8, 128), f32),
            pltpu.VMEM((BLK, 128), bf16),
            pltpu.VMEM((7, BLK, 128), bf16),
            pltpu.VMEM((BLK, 128), bf16),
            pltpu.VMEM((7, BLK, 128), bf16),
            pltpu.VMEM((2, TP, 128, OUT), bf16),
            pltpu.VMEM((BLK, OUT), f32),
            pltpu.VMEM((BLK, OUT), f32),
            pltpu.SemaphoreType.DMA((COPIES,)),
            pltpu.SemaphoreType.DMA((9,)),
            pltpu.SemaphoreType.REGULAR,
        ],
        compiler_params=pltpu.CompilerParams(collective_id=1, has_side_effects=True),
        cost_estimate=pl.CostEstimate(flops=5_000_000_000, bytes_accessed=8_000_000, transcendentals=9_000_000),
    )(
        tokens, lru_in, lru_gate_in, query_w, key_w, value_w, conv_weight, recur_gate_w, input_gate_w,
        rate_param.reshape(TP, 128), decay_extra, forget_cum.reshape(4, 128), out_lru, out_fox,
    ).astype(bf16)


def solution(mesh):
    placed = (
        P("sp", "tp"),
        P(None, "tp"),
        P(None, "tp"),
        P(None, "tp"),
        P(None, "tp"),
        P(None, "tp"),
        P(),
        P(),
        P(),
        P(),
        P("sp", "tp"),
        P("sp", "tp"),
        P("tp", None),
        P("tp", None),
    )
    return jax.shard_map(
        layer, mesh=mesh, in_specs=placed, out_specs=P("sp", "tp"), check_vma=False
    )
```

```python
import jax
import jax.numpy as jnp
from jax import lax
from jax.experimental import pallas as pl
from jax.experimental.pallas import tpu as pltpu
from jax.sharding import PartitionSpec as P

MESH = pl.DeviceIdType.MESH
D = 2048
HEAD_DIM = 128
SP, TP = 32, 8
ZS, XS, YS = 8, 4, 4
BLK = 512
HALF = BLK // 2
FEAT = D // TP
OUT = D // TP
HROWS = HALF + 16
PIECE = HROWS + HALF
LOG2E = 1.4426950408889634
NEG = -1e30
COPIES = 96
ROWS = 256

decay_sharpness = 8.0
epsilon_norm = 1e-06


def eye_mask():
    return lax.broadcasted_iota(jnp.int32, (128, 128), 0) == lax.broadcasted_iota(
        jnp.int32, (128, 128), 1
    )


def packed_rows(column):
    eye = eye_mask()
    return jnp.concatenate(
        [
            jnp.sum(jnp.where(eye, column[g * 128 : (g + 1) * 128], 0.0), axis=0, keepdims=True)
            for g in range(4)
        ],
        axis=0,
    )


def unpacked_row(row):
    return jnp.sum(
        jnp.where(eye_mask(), jnp.broadcast_to(row, (128, 128)), 0.0), axis=1, keepdims=True
    )


def dot(a, b):
    return jnp.dot(a, b, preferred_element_type=jnp.float32)


def log1p_unit(u):
    s = u / (2.0 + u)
    square = s * s
    total = jnp.full_like(s, 1.0 / 19.0)
    for k in range(17, 0, -2):
        total = total * square + 1.0 / k
    return 2.0 * s * total


def minus_expm1(x):
    near = jnp.full_like(x, 1.0 / 362880.0)
    for k in (40320.0, 5040.0, 720.0, 120.0, 24.0, 6.0, 2.0, 1.0):
        near = near * x + 1.0 / k
    return jnp.where(x > -0.5, -near * x, 1.0 - jnp.exp(x))


def await_bytes(ref, semaphore):
    pltpu.make_async_copy(ref, ref, semaphore).wait()


class Gather:
    def __init__(self, copy, sems, own, slots, up, down, partner, start=0, rows=BLK, last=None):
        half = rows // 2
        first, second = pl.ds(start, half), pl.ds(start + half, half)

        def send(a, b, part, to, k):
            source = own if a is None else slots.at[a]
            return copy(source.at[part], slots.at[b, part], send=sems[10], recv=sems[k], tp=to)

        plan = [
            (None, 0, pl.ds(start, rows), partner, 0),
            (None, 1, first, up, 1),
            (None, 1, second, up, 2),
            (None, 2, second, down, 3),
            (None, 2, first, down, 4),
            (1, 3, first, up, 5),
            (2, 3, second, down, 6),
            (1, 4, first, partner, 7),
            (1, 4, second, partner, 7),
            (2, 5, first, partner, 8),
            (2, 5, second, partner, 8),
            (3, 6, first, partner, 9) if last is None else (1, 6, first, last[0], 9),
            (3, 6, second, partner, 9) if last is None else (2, 6, second, last[1], 9),
        ]
        self.direct = last is not None
        self.copies = [send(*each) for each in plan]
        self.sems, self.slots, self.rows = sems, slots, pl.ds(start, rows)

    def start(self, *which):
        for i in which:
            self.copies[i].start()

    def arrived(self, *which):
        for i in which:
            self.copies[i].wait_recv()

    def arrived_from_partner(self, *slots):
        for slot in slots:
            await_bytes(self.slots.at[slot, self.rows], self.sems[slot + 3])

    def finish(self):
        await_bytes(self.slots.at[:, self.rows], self.sems[10])

    def begin(self):
        self.start(1, 3, 0, 2, 4)

    def relay_first(self):
        self.arrived(1)
        self.start(5, 7)
        if self.direct:
            self.start(11)
        self.arrived(3)
        self.start(6, 10)
        if self.direct:
            self.start(12)

    def relay_second(self):
        self.arrived(2)
        self.start(8)
        self.arrived(4)
        self.start(9)

    def relay(self):
        self.relay_first()
        self.relay_second()

    def relay_last(self):
        self.arrived(5)
        if not self.direct:
            self.start(11)
        self.arrived(6)
        if not self.direct:
            self.start(12)


def layer_kernel(
    tok_hbm, lru_w_hbm, gate_w_hbm, query_w_hbm, key_w_hbm, value_w_hbm,
    conv_ref, recur_hbm, input_hbm, rate_ref, extra_hbm, f_ref, out_lru_ref, out_fox_ref,
    o_ref,
    tok_ref, recur_ref, input_ref, extra_ref, weights, tokg, acc_kv, acc_rest, scores_a, scores_b, squares,
    kv, qb, bias, m_ref, acc, o_send, st_send, o_relay, o_recv, st_recv,
    lru_own, halo, gate_own, decays, drives, row_tiles, col_tiles,
    lru_out, lru_g, fox_out, fox_g, w_out, acc_out, out_rows,
    copy_sems, load_sems, alive,
):
    sp, tp = lax.axis_index("sp"), lax.axis_index("tp")
    z, x = lax.div(sp, XS), lax.rem(sp, XS)
    y, c = lax.div(tp, 2), lax.rem(tp, 2)
    above = lax.rem(z + 1, ZS) * XS + x
    below = lax.rem(z + ZS - 1, ZS) * XS + x
    partner = y * 2 + 1 - c

    def along_y(r, core):
        return lax.rem(y + r, YS) * 2 + core

    def along_x(r):
        return z * XS + lax.rem(x + r, XS)

    def along_z(r):
        return lax.rem(z + r, ZS) * XS + x

    following, preceding = lax.rem(sp + 1, SP), lax.rem(sp + SP - 1, SP)
    used = [0]

    def semaphore():
        used[0] += 1
        return copy_sems.at[used[0] - 1]

    def copy(src, dst, send=None, recv=None, **where):
        return pltpu.make_async_remote_copy(
            src_ref=src, dst_ref=dst, send_sem=send or semaphore(), recv_sem=recv or semaphore(),
            device_id=where, device_id_type=MESH,
        )

    gather_sems = [[semaphore() for k in range(11)] for group in range(3)]

    tok_load = pltpu.make_async_copy(tok_hbm, tok_ref, load_sems.at[1])
    tok_load.start()
    loads = [
        pltpu.make_async_copy(w, weights.at[i], load_sems.at[0])
        for i, w in enumerate((key_w_hbm, value_w_hbm, lru_w_hbm, query_w_hbm, gate_w_hbm))
    ]
    own_blocks = pl.ds(2 * tp, 2)
    own_columns = pl.ds(pl.multiple_of(tp * OUT, OUT), OUT)
    later_loads = [
        pltpu.make_async_copy(extra_hbm, extra_ref, load_sems.at[2]),
        pltpu.make_async_copy(recur_hbm.at[own_blocks], recur_ref, load_sems.at[3]),
        pltpu.make_async_copy(input_hbm.at[own_blocks], input_ref, load_sems.at[4]),
        pltpu.make_async_copy(out_lru_ref.at[:, own_columns], w_out.at[0, tp], load_sems.at[5]),
        pltpu.make_async_copy(out_fox_ref.at[:, own_columns], w_out.at[1, tp], load_sems.at[6]),
    ]
    for load in loads + later_loads:
        load.start()

    barrier = pltpu.get_barrier_semaphore()

    def tell(semaphore, **where):
        pl.semaphore_signal(semaphore, inc=1, device_id=where, device_id_type=MESH)

    for r in range(1, TP):
        tell(barrier, tp=lax.rem(tp + r, TP))
    for r in range(1, XS):
        tell(barrier, sp=along_x(r))
    for r in range(1, ZS):

        @pl.when(z + r < ZS)
        def _():
            tell(barrier, sp=along_z(r))

    last_of_row = (x == XS - 1) & (z < ZS - 1)
    first_of_row = (x == 0) & (z > 0)

    @pl.when(last_of_row)
    def _():
        tell(barrier, sp=following)

    pl.semaphore_wait(barrier, TP - 1 + XS - 1 + z + first_of_row.astype(jnp.int32))
    for r in range(1, ZS):

        @pl.when(z >= r)
        def _():
            tell(alive, sp=along_z(ZS - r))

    @pl.when(first_of_row)
    def _():
        tell(alive, sp=preceding)

    tokens = [
        Gather(copy, gather_sems[h], tok_ref, tokg, along_y(1, c), along_y(3, c), partner, h * HALF, HALF) for h in (0, 1)
    ]
    tok_load.wait()
    tokens[0].begin()
    forget = f_ref[...]
    high = forget.astype(jnp.bfloat16).astype(jnp.float32)
    middle = (forget - high).astype(jnp.bfloat16).astype(jnp.float32)
    low = forget - high - middle
    for h in (0, 1):
        lines = [part[2 * h : 2 * h + 2] for part in (high, middle, low)]
        kv[h, HALF:HROWS, :] = jnp.concatenate(
            lines + [jnp.zeros((10, 128), jnp.float32)], axis=0
        ).astype(jnp.bfloat16)

    def features(r, core):
        return pl.ds(pl.multiple_of(along_y(r, core) * FEAT, FEAT), FEAT)

    def pair(slot, h):
        rows = pl.ds(h * HALF, HALF)
        block = tok_ref if slot == 0 else tokg.at[slot]
        other = tokg.at[0] if slot == 0 else tokg.at[slot + 3]
        return block[rows, :], other[rows, :]

    distance = {0: 0, 1: 3, 2: 1, 3: 2}

    def project(slot, h, group, target):
        rows = [features(distance[slot], c), features(distance[slot], 1 - c)]
        right = jnp.concatenate(
            [jnp.concatenate([weights[i, part, :] for part in rows], axis=0) for i in group], axis=1
        )
        product = dot(jnp.concatenate(pair(slot, h), axis=1), right)
        half = pl.ds(h * HALF, HALF)
        target[half, :] = product if slot == 0 else target[half, :] + product

    def count_squares(slot, h):
        half = pl.ds(h * HALF, HALF)
        total = jnp.zeros((HALF, 128), jnp.float32) if slot == 0 else squares[half, :]
        for piece in pair(slot, h):
            for g in range(FEAT // 128):
                value = piece[:, g * 128 : (g + 1) * 128].astype(jnp.float32)
                total = total + value * value
        squares[half, :] = total

    def take(slot, h):
        project(slot, h, (0, 1, 2), acc_kv)
        project(slot, h, (3, 4), acc_rest)
        count_squares(slot, h)

    plus = [(0, 2), (1, 3), (2, 4), (3, 5), (4, 6), (5, 7)]
    minus = [(0, 8), (1, 9), (8, 10), (9, 11), (10, 12), (11, 13), (12, 14), (13, 15)]
    plus = [copy(kv.at[a], kv.at[b], sp=above) for a, b in plus]
    minus = [copy(kv.at[a], kv.at[b], sp=below) for a, b in minus]

    def wrapped(d):
        return lax.rem(z + d, ZS) < 4

    def send_plus(i):
        @pl.when((z < ZS - 1) & (z >= i // 2))
        def _():
            plus[i].start()

    def send_minus(i):
        @pl.when(wrapped(i // 2))
        def _():
            minus[i].start()

    last_row = z == ZS - 1

    def receive_plus(i, where=True):
        d = i // 2 + 1

        @pl.when((z >= d) & where)
        def _():
            plus[i].wait_recv()

        if d < 3:

            @pl.when((z < ZS - 1) & (z >= d) & where)
            def _():
                plus[i + 2].start()

    def receive_minus(i, where=True):
        d = i // 2 + 1

        @pl.when(wrapped(d) & where)
        def _():
            minus[i].wait_recv()
            if d < 4:
                minus[i + 2].start()

    tail = copy(lru_own.at[pl.ds(BLK - 16, 16)], halo, sp=following)
    query_rows = [pl.ds(pl.multiple_of(x * BLK + h * HALF, HALF), HALF) for h in (0, 1)]
    query_sems = semaphore(), semaphore()
    query_copies = [
        {r: copy(qb.at[rows], qb.at[rows], *query_sems, sp=along_x(r)) for r in (1, 2, 3)} for rows in query_rows
    ]
    others_queries = qb.at[pl.ds(0, (XS - 1) * BLK)]

    def conclude(h):
        half = pl.ds(h * HALF, HALF)
        count_squares(3, h)
        row_scale = lax.rsqrt(
            jnp.sum(squares[half, :], axis=1, keepdims=True) * (1.0 / D) + epsilon_norm
        )
        project(3, h, (0, 1, 2), acc_kv)
        ready = (acc_kv[half, :] * row_scale).astype(jnp.bfloat16)
        lru_own[half, :] = ready[:, 256:]
        if h == 0:
            later = (ZS - 1 - z) + last_of_row.astype(jnp.int32)

            @pl.when(later > 0)
            def _():
                pl.semaphore_wait(alive, later)

        else:

            @pl.when(sp < SP - 1)
            def _():
                tail.start()

        kv[h, :HALF, :] = ready[:, :128]
        kv[h, HROWS:, :] = ready[:, 128:256]
        send_plus(h)
        send_minus(h)
        project(3, h, (3, 4), acc_rest)
        rest = (acc_rest[half, :] * row_scale).astype(jnp.bfloat16)
        qb[query_rows[h], :] = rest[:, :128]
        gate_own[half, :] = rest[:, 128:]
        for r in (1, 3, 2):
            query_copies[h][r].start()

    await_bytes(weights, load_sems.at[0])
    early, late = tokens
    early.arrived(0)
    take(0, 0)
    early.relay_first()
    late.begin()
    early.relay_second()
    early.arrived_from_partner(4)
    take(1, 0)
    early.arrived_from_partner(5)
    take(2, 0)
    early.relay_last()
    late.arrived(0)
    take(0, 1)
    late.relay_first()
    early.arrived_from_partner(6)
    conclude(0)
    late.relay_second()
    late.arrived_from_partner(4)
    take(1, 1)
    late.arrived_from_partner(5)
    take(2, 1)
    receive_minus(0, last_row)
    late.relay_last()
    late.arrived_from_partner(6)
    conclude(1)

    for group in tokens:
        group.finish()

    weight_sems = semaphore(), semaphore()
    weight_copies = []
    for r in range(1, TP):
        to = lax.rem(tp + r, TP)
        columns = pl.ds(pl.multiple_of(to * OUT, OUT), OUT)
        for k, ref in enumerate((out_lru_ref, out_fox_ref)):
            weight_copies.append(copy(ref.at[:, columns], w_out.at[k, tp], *weight_sems, tp=to))
    for each in weight_copies:
        each.start()
    others_weights = w_out.at[:, pl.ds(0, TP - 1)]
    own_rows = pl.ds(pl.multiple_of(x * BLK, BLK), BLK)
    m_ref[...] = jnp.full_like(m_ref, NEG)
    acc[...] = jnp.zeros_like(acc)

    def set_bias(slot):
        parts = kv[slot, HALF:HROWS, :].astype(jnp.float32)
        whole = parts[0:2] + parts[2:4] + parts[4:6]
        for g in range(2):
            bias[slot : slot + 1, g * 128 : (g + 1) * 128] = whole[g : g + 1] * -LOG2E

    scale = HEAD_DIM ** (-0.5) * LOG2E

    def joint(parts, axis):
        return parts[0] if len(parts) == 1 else jnp.concatenate(parts, axis=axis)

    def score(buffer, i, slots):
        rows = pl.ds(i * BLK if isinstance(i, int) else pl.multiple_of(i * BLK, BLK), BLK)
        buffer[:, : HALF * len(slots)] = lax.dot_general(
            qb[rows, :],
            joint([kv[slot, :HALF, :] for slot in slots], 0),
            (((1,), (1,)), ((), ())),
            preferred_element_type=jnp.float32,
        )

    def absorb(buffer, i, slots, masked=False):
        width = HALF * len(slots)
        offsets = joint([bias[slot : slot + 1, :] for slot in slots], 1)
        values = joint([kv[slot, HROWS:, :] for slot in slots], 0)
        values = jnp.concatenate([values, jnp.ones_like(values)], axis=1)
        start = i * BLK if isinstance(i, int) else pl.multiple_of(i * BLK, BLK)
        for part in range(0, BLK, ROWS):
            rows = pl.ds(start + part, ROWS)
            scores = buffer[part : part + ROWS, :width] * scale + offsets
            if masked:
                earlier = lax.broadcasted_iota(jnp.int32, scores.shape, 0) + part >= (
                    lax.broadcasted_iota(jnp.int32, scores.shape, 1)
                )
                scores = jnp.where(earlier, scores, NEG)
            old = m_ref[rows, :]
            new = jnp.maximum(old, jnp.max(scores, axis=1, keepdims=True))
            rescale = jnp.exp2(old - new)
            probs = jnp.exp2(scores - jnp.concatenate([new] * (width // 128), axis=1))
            m_ref[rows, :] = new
            acc[rows, :] = acc[rows, :] * jnp.concatenate([rescale] * 2, axis=1) + dot(
                probs.astype(jnp.bfloat16), values
            )

    def attend(i, slots, masked=False):
        score(scores_a, i, slots)
        absorb(scores_a, i, slots, masked)

    def visit_rest(slots, first):
        def body(i, carry):
            attend(i, slots)
            return carry

        lax.fori_loop(first, XS, body, 0)

    def visit(*slots):
        for slot in slots:
            set_bias(slot)
        score(scores_a, 0, slots)
        pair = scores_a, scores_b
        for k in range(XS):
            if k + 1 < XS:
                score(pair[(k + 1) % 2], k + 1, slots)
            absorb(pair[k % 2], k, slots)

    def take_keys(i):
        d = i // 2 + 1
        @pl.when(z + d >= ZS)
        def _():
            visit(i + 2, i + 8)

        @pl.when((z >= d) & (z + d < ZS))
        def _():
            visit(i + 2)

    set_bias(0)
    set_bias(1)
    attend(x, (0, 1), masked=True)
    receive_plus(0)
    receive_minus(0, z < ZS - 1)
    receive_minus(1, last_row)

    @pl.when(sp > 0)
    def _():
        tail.wait_recv()

    @pl.when(sp == 0)
    def _():
        halo[...] = jnp.zeros_like(halo)

    for load in later_loads:
        load.wait()
    lru_input = lru_own[...].astype(jnp.float32)
    before = halo[8:16, :].astype(jnp.float32)
    joined = jnp.concatenate([before, lru_input], axis=0)
    channels = pl.ds(pl.multiple_of(tp * 128, 128), 128)
    taps = conv_ref[:, channels].astype(jnp.float32)
    conv = jnp.zeros((BLK, 128), jnp.float32)
    for j in range(4):
        shifted = joined if j == 3 else pltpu.roll(joined, 3 - j, 0)
        conv = conv + taps[j : j + 1, :] * shifted[8:, :]
    conv = conv.astype(jnp.bfloat16)
    column = lax.broadcasted_iota(jnp.int32, (64, 128), 1)
    row = lax.broadcasted_iota(jnp.int32, (64, 128), 0)
    left = jnp.where(column == row, 1.0, 0.0).astype(jnp.bfloat16)
    right = jnp.where(column == row + 64, 1.0, 0.0).astype(jnp.bfloat16)

    def block_diagonal(ref):
        return jnp.concatenate([dot(ref[0], left), dot(ref[1], right)], axis=0)

    gates_w = jnp.concatenate([block_diagonal(recur_ref), block_diagonal(input_ref)], axis=1)
    gates = dot(conv, gates_w.astype(jnp.bfloat16))
    gates = 1.0 / (1.0 + jnp.exp(-gates))
    rate = log1p_unit(jnp.exp(-rate_ref[pl.ds(tp, 1), :]))
    log_decay = (-decay_sharpness * rate) * gates[:, :128] + extra_ref[...]
    drive = jnp.sqrt(minus_expm1(2.0 * log_decay)) * gates[:, 128:] * conv.astype(jnp.float32)
    decay = jnp.exp(log_decay)
    place = lax.broadcasted_iota(jnp.int32, (BLK, 128), 0)
    step = 1
    while step < BLK:
        if step < 8:
            inside = place >= step
            decay_back = jnp.where(inside, pltpu.roll(decay, step, 0), 1.0)
            drive_back = jnp.where(inside, pltpu.roll(drive, step, 0), 0.0)
        else:
            decay_back = jnp.concatenate([jnp.ones((step, 128), jnp.float32), decay[:-step]], axis=0)
            drive_back = jnp.concatenate([jnp.zeros((step, 128), jnp.float32), drive[:-step]], axis=0)
        drive = decay * drive_back + drive
        decay = decay * decay_back
        step *= 2
    decays[...] = decay
    drives[...] = drive

    def tile_of(a, b):
        return jnp.concatenate([a, b, jnp.zeros((6, 128), jnp.float32)], axis=0)

    row_tiles[0] = tile_of(decays[BLK - 1 :, :], drives[BLK - 1 :, :])
    row_sems = semaphore(), semaphore()
    row_copies = {
        r: copy(row_tiles.at[0], row_tiles.at[r], *row_sems, sp=along_x(r)) for r in (1, 2, 3)
    }
    others_rows = row_tiles.at[pl.ds(1, XS - 1)]
    for r in (1, 3, 2):
        row_copies[r].start()

    receive_minus(1, z < ZS - 1)
    receive_plus(1, z < ZS - 1)
    receive_minus(2, z >= ZS - 2)
    await_bytes(others_queries, query_sems[1])
    visit_rest((0, 1), x + 1)

    column_copies = {r: copy(col_tiles.at[0], col_tiles.at[r], sp=along_z(r)) for r in range(1, ZS)}
    branch = Gather(copy, gather_sems[0], lru_out, lru_g, along_y(1, c), along_y(3, c), partner)
    one, zero = jnp.ones((1, 128), jnp.float32), jnp.zeros((1, 128), jnp.float32)

    def total_of_row():
        await_bytes(others_rows, row_sems[1])
        whole_decay, whole_state, state = one, zero, zero
        for k in range(XS):
            block = row_tiles[lax.rem(x + XS - k, XS)]
            a, b = block[0:1], block[1:2]
            state = jnp.where(k < x, a * state + b, state)
            whole_state = a * whole_state + b
            whole_decay = whole_decay * a
        col_tiles[0] = tile_of(whole_decay, whole_state)
        for r in range(1, ZS):

            @pl.when(z + r < ZS)
            def _():
                column_copies[r].start()

    def recurrence_out():
        for r in range(1, ZS):

            @pl.when(z >= r)
            def _():
                column_copies[r].wait_recv()

        def row_above(k, state):
            block = col_tiles[z - k]
            return block[0:1] * state + block[1:2]

        state = lax.fori_loop(0, z, row_above, zero)
        for k in range(XS):
            block = row_tiles[lax.rem(x + XS - k, XS)]
            state = jnp.where(k < x, block[0:1] * state + block[1:2], state)
        gate = gate_own[...].astype(jnp.float32)
        inner = 0.7978845608028654 * (gate + 0.044715 * gate * gate * gate)
        gelu = 0.5 * gate * (1.0 + jnp.tanh(inner))
        lru_out[...] = ((drives[...] + decays[...] * state) * gelu).astype(jnp.bfloat16)
        branch.begin()

    beside = {0: total_of_row, 2: recurrence_out, 4: branch.relay}
    receive_minus(2, z < ZS - 2)
    for i in range(6):
        take_keys(i)
        if i in beside:
            beside[i]()
        if i == 0:
            receive_plus(1, last_row)
        if i < 4:
            receive_plus(i + 2)
        if i < 5:
            receive_minus(i + 3)

    right, left = along_x(1), along_x(3)
    out_sent, out_sent_on = semaphore(), semaphore()
    relay_sems, out_sems = [semaphore(), semaphore()], [semaphore(), semaphore()]
    out_copies = []
    for h in (0, 1):
        rows = pl.ds(h * HALF, HALF)
        quarters = [pl.ds(h * HALF + k * 128, 128) for k in (0, 1)]
        out_copies.append(
            {
                "relay": [
                    copy(o_send.at[2, part], o_relay.at[k, part], out_sent, relay_sems[h], sp=to)
                    for k, (part, to) in enumerate(zip(quarters, (right, left)))
                ],
                "near": {
                    r: copy(o_send.at[r, rows], o_recv.at[r, rows], out_sent, out_sems[h], sp=along_x(r))
                    for r in (1, 3)
                },
                "far": [
                    copy(o_relay.at[k, part], o_recv.at[2, part], out_sent_on, out_sems[h], sp=to)
                    for k, (part, to) in enumerate(zip(quarters, (right, left)))
                ],
            }
        )
    stat_sems = semaphore(), semaphore()
    stat_copies = {r: copy(st_send.at[r], st_recv.at[r], *stat_sems, sp=along_x(r)) for r in (1, 2, 3)}
    others_stats = st_recv.at[pl.ds(1, XS - 1)]

    def stats(rows):
        return packed_rows(m_ref[rows, :]), packed_rows(acc[rows, 128:])

    def relay_on(h):
        await_bytes(o_relay.at[0, pl.ds(0, HALF)], relay_sems[h])
        for each in out_copies[h]["far"]:
            each.start()

    def block_of(r):
        return lax.rem(x + r, XS)

    @pl.when(z >= 4)
    def _():
        set_bias(14)
        set_bias(15)
        score(scores_a, block_of(2), (14, 15))

    buffers = (scores_a, scores_b)
    turns = (2, 1, 3, 0)
    for k, r in enumerate(turns):

        @pl.when(z >= 4)
        def _():
            if k + 1 < len(turns):
                score(buffers[(k + 1) % 2], block_of(turns[k + 1]), (14, 15))
            absorb(buffers[k % 2], block_of(r), (14, 15))

        if r > 0:
            rows = pl.ds(pl.multiple_of(block_of(r) * BLK, BLK), BLK)
            st_send[r] = jnp.concatenate(stats(rows), axis=0)
            stat_copies[r].start()
            o_send[r] = acc[rows, :128].astype(jnp.bfloat16)
            if r == 2:
                for h in (0, 1):
                    for each in out_copies[h]["relay"]:
                        each.start()
            else:
                for h in (0, 1):
                    out_copies[h]["near"][r].start()
    tops, sums = [None] * 4, [None] * 4
    tops[0], sums[0] = stats(own_rows)
    branch.relay_last()

    relay_on(0)

    sources = [(0, c), (0, 1 - c), (3, c), (3, 1 - c), (1, c), (1, 1 - c), (2, c), (2, 1 - c)]

    def branch_product(k, own, slots, which, rows):
        lookup = [None, 0, 1, 4, 2, 5, 3, 6]
        blocks = [own[rows, :] if lookup[i] is None else slots[lookup[i], rows, :] for i in which]
        rights = [w_out[k, along_y(*sources[i])] for i in which]
        return dot(jnp.concatenate(blocks, axis=1), jnp.concatenate(rights, axis=0))

    await_bytes(others_weights, weight_sems[1])
    branch.arrived(0)
    branch.arrived_from_partner(4, 5, 6)
    relay_on(1)
    acc_out[...] = branch_product(0, lru_out, lru_g, range(8), pl.ds(0, BLK))

    await_bytes(others_stats, stat_sems[1])
    for r in (1, 2, 3):
        both = st_recv[r]
        tops[r], sums[r] = both[0:4], both[4:8]
    top = jnp.maximum(jnp.maximum(tops[0], tops[1]), jnp.maximum(tops[2], tops[3]))
    shares = [jnp.exp2(t - top) for t in tops]
    whole = shares[0] * sums[0] + shares[1] * sums[1] + shares[2] * sums[2] + shares[3] * sums[3]
    shares = [s / whole for s in shares]
    heads = [
        Gather(
            copy, gather_sems[1 + h], fox_out, fox_g, along_y(1, c), along_y(3, c), partner, h * HALF, HALF,
            last=(along_y(1, 1 - c), along_y(3, 1 - c)),
        )
        for h in (0, 1)
    ]

    def merge(h):
        await_bytes(qb.at[pl.ds(0, (XS - 1) * HALF)], out_sems[h])
        for g in (2 * h, 2 * h + 1):
            part = pl.ds(g * 128, 128)
            mine = pl.ds(pl.multiple_of(x * BLK + g * 128, 128), 128)
            total = unpacked_row(shares[0][g : g + 1]) * acc[mine, :128]
            for r in (1, 2, 3):
                total = total + unpacked_row(shares[r][g : g + 1]) * o_recv[r, part, :].astype(jnp.float32)
            fox_out[part, :] = total.astype(jnp.bfloat16)
        heads[h].begin()

    def head_product(h, which):
        rows = pl.ds(h * HALF, HALF)
        return branch_product(1, fox_out, fox_g, which, rows)

    halves = [pl.ds(h * HALF, HALF) for h in (0, 1)]
    out_loads = [
        pltpu.make_async_copy(out_rows.at[half], o_ref.at[half], load_sems.at[7 + h])
        for h, half in enumerate(halves)
    ]

    def write(h):
        heads[h].arrived_from_partner(6)
        out_rows[halves[h], :] = (acc_out[halves[h], :] + head_product(h, (6, 7))).astype(out_rows.dtype)
        out_loads[h].start()

    merge(0)
    merge(1)
    heads[0].relay()
    heads[0].arrived(0)
    acc_out[halves[0], :] += head_product(0, (0, 1))
    heads[1].relay_first()
    heads[0].relay_last()
    heads[1].relay_second()
    heads[1].arrived(0)
    acc_out[halves[1], :] += head_product(1, (0, 1))
    heads[0].arrived_from_partner(4, 5)
    acc_out[halves[0], :] += head_product(0, (2, 3, 4, 5))
    write(0)
    heads[1].relay_last()
    heads[1].arrived_from_partner(4, 5)
    acc_out[halves[1], :] += head_product(1, (2, 3, 4, 5))
    write(1)

    for i, each in enumerate(plus):

        @pl.when((z < ZS - 1) & (z >= i // 2))
        def _():
            each.wait_send()

    for i, each in enumerate(minus):

        @pl.when(wrapped(i // 2))
        def _():
            each.wait_send()

    @pl.when(sp < SP - 1)
    def _():
        tail.wait_send()

    for r in range(1, ZS):

        @pl.when(z + r < ZS)
        def _():
            column_copies[r].wait_send()

    await_bytes(others_weights, weight_sems[0])
    await_bytes(others_queries, query_sems[0])
    await_bytes(others_rows, row_sems[0])
    await_bytes(others_stats, stat_sems[0])
    await_bytes(o_recv.at[pl.ds(1, XS - 1)], out_sent)
    await_bytes(o_relay.at[0], out_sent_on)
    for group in [branch] + heads:
        group.finish()
    for each in out_loads:
        each.wait()


def layer(
    tokens, lru_in, lru_gate_in, query_w, key_w, value_w, conv_weight, recur_gate_w, input_gate_w,
    rate_param, decay_extra, forget_cum, out_lru, out_fox,
):
    vmem = pl.BlockSpec(memory_space=pltpu.VMEM)
    hbm = pl.BlockSpec(memory_space=pl.ANY)
    bf16, f32 = jnp.bfloat16, jnp.float32
    return pl.pallas_call(
        layer_kernel,
        out_shape=pltpu.VMEM((BLK, OUT), f32),
        in_specs=[hbm] * 6 + [vmem, hbm, hbm, vmem, hbm, vmem, hbm, hbm],
        out_specs=hbm,
        scratch_shapes=[
            pltpu.VMEM((BLK, FEAT), bf16),
            pltpu.VMEM((2, 64, 64), bf16),
            pltpu.VMEM((2, 64, 64), bf16),
            pltpu.VMEM((BLK, 128), f32),
            pltpu.VMEM((5, D, 128), bf16),
            pltpu.VMEM((7, BLK, FEAT), bf16),
            pltpu.VMEM((BLK, 384), f32),
            pltpu.VMEM((BLK, 256), f32),
            pltpu.VMEM((BLK, BLK), f32),
            pltpu.VMEM((BLK, BLK), f32),
            pltpu.VMEM((BLK, 128), f32),
            pltpu.VMEM((2 * ZS, PIECE, 128), bf16),
            pltpu.VMEM((XS * BLK, 128), bf16),
            pltpu.VMEM((2 * ZS, HALF), f32),
            pltpu.VMEM((XS * BLK, 128), f32),
            pltpu.VMEM((XS * BLK, 256), f32),
            pltpu.VMEM((XS, BLK, 128), bf16),
            pltpu.VMEM((XS, 8, 128), f32),
            pltpu.VMEM((2, BLK, 128), bf16),
            pltpu.VMEM((XS, BLK, 128), bf16),
            pltpu.VMEM((XS, 8, 128), f32),
            pltpu.VMEM((BLK, 128), bf16),
            pltpu.VMEM((16, 128), bf16),
            pltpu.VMEM((BLK, 128), bf16),
            pltpu.VMEM((BLK, 128), f32),
            pltpu.VMEM((BLK, 128), f32),
            pltpu.VMEM((XS, 8, 128), f32),
            pltpu.VMEM((ZS, 8, 128), f32),
            pltpu.VMEM((BLK, 128), bf16),
            pltpu.VMEM((7, BLK, 128), bf16),
            pltpu.VMEM((BLK, 128), bf16),
            pltpu.VMEM((7, BLK, 128), bf16),
            pltpu.VMEM((2, TP, 128, OUT), bf16),
            pltpu.VMEM((BLK, OUT), f32),
            pltpu.VMEM((BLK, OUT), f32),
            pltpu.SemaphoreType.DMA((COPIES,)),
            pltpu.SemaphoreType.DMA((9,)),
            pltpu.SemaphoreType.REGULAR,
        ],
        compiler_params=pltpu.CompilerParams(collective_id=1, has_side_effects=True),
        cost_estimate=pl.CostEstimate(flops=5_000_000_000, bytes_accessed=8_000_000, transcendentals=9_000_000),
    )(
        tokens, lru_in, lru_gate_in, query_w, key_w, value_w, conv_weight, recur_gate_w, input_gate_w,
        rate_param.reshape(TP, 128), decay_extra, forget_cum.reshape(4, 128), out_lru, out_fox,
    ).astype(bf16)


def solution(mesh):
    placed = (
        P("sp", "tp"),
        P(None, "tp"),
        P(None, "tp"),
        P(None, "tp"),
        P(None, "tp"),
        P(None, "tp"),
        P(),
        P(),
        P(),
        P(),
        P("sp", "tp"),
        P("sp", "tp"),
        P("tp", None),
        P("tp", None),
    )
    return jax.shard_map(
        layer, mesh=mesh, in_specs=placed, out_specs=P("sp", "tp"), check_vma=False
    )
```

```python
import jax
import jax.numpy as jnp
from jax import lax
from jax.experimental import pallas as pl
from jax.experimental.pallas import tpu as pltpu
from jax.sharding import PartitionSpec as P

MESH = pl.DeviceIdType.MESH
D = 2048
HEAD_DIM = 128
SP, TP = 32, 8
ZS, XS, YS = 8, 4, 4
BLK = 512
HALF = BLK // 2
FEAT = D // TP
OUT = D // TP
HROWS = HALF + 16
PIECE = HROWS + HALF
LOG2E = 1.4426950408889634
NEG = -1e30
COPIES = 73
ROWS = 256

decay_sharpness = 8.0
epsilon_norm = 1e-06


def eye_mask():
    return lax.broadcasted_iota(jnp.int32, (128, 128), 0) == lax.broadcasted_iota(
        jnp.int32, (128, 128), 1
    )


def packed_rows(column):
    eye = eye_mask()
    return jnp.concatenate(
        [
            jnp.sum(jnp.where(eye, column[g * 128 : (g + 1) * 128], 0.0), axis=0, keepdims=True)
            for g in range(4)
        ],
        axis=0,
    )


def unpacked_row(row):
    return jnp.sum(
        jnp.where(eye_mask(), jnp.broadcast_to(row, (128, 128)), 0.0), axis=1, keepdims=True
    )


def dot(a, b):
    return jnp.dot(a, b, preferred_element_type=jnp.float32)


def log1p_unit(u):
    s = u / (2.0 + u)
    square = s * s
    total = jnp.full_like(s, 1.0 / 19.0)
    for k in range(17, 0, -2):
        total = total * square + 1.0 / k
    return 2.0 * s * total


def minus_expm1(x):
    near = jnp.full_like(x, 1.0 / 362880.0)
    for k in (40320.0, 5040.0, 720.0, 120.0, 24.0, 6.0, 2.0, 1.0):
        near = near * x + 1.0 / k
    return jnp.where(x > -0.5, -near * x, 1.0 - jnp.exp(x))


def await_bytes(ref, semaphore):
    pltpu.make_async_copy(ref, ref, semaphore).wait()


class Gather:
    def __init__(self, copy, sems, own, slots, up, down, partner, start=0, rows=BLK, last=None):
        half = rows // 2
        first, second = pl.ds(start, half), pl.ds(start + half, half)

        def send(a, b, part, to, k):
            source = own if a is None else slots.at[a]
            return copy(source.at[part], slots.at[b, part], send=sems[10], recv=sems[k], tp=to)

        plan = [
            (None, 0, pl.ds(start, rows), partner, 0),
            (None, 1, first, up, 1),
            (None, 1, second, up, 2),
            (None, 2, second, down, 3),
            (None, 2, first, down, 4),
            (1, 3, first, up, 5),
            (2, 3, second, down, 6),
            (1, 4, first, partner, 7),
            (1, 4, second, partner, 7),
            (2, 5, first, partner, 8),
            (2, 5, second, partner, 8),
            (3, 6, first, partner, 9) if last is None else (1, 6, first, last[0], 9),
            (3, 6, second, partner, 9) if last is None else (2, 6, second, last[1], 9),
        ]
        self.direct = last is not None
        self.copies = [send(*each) for each in plan]
        self.sems, self.slots, self.rows = sems, slots, pl.ds(start, rows)

    def start(self, *which):
        for i in which:
            self.copies[i].start()

    def arrived(self, *which):
        for i in which:
            self.copies[i].wait_recv()

    def arrived_from_partner(self, *slots):
        for slot in slots:
            await_bytes(self.slots.at[slot, self.rows], self.sems[slot + 3])

    def finish(self):
        await_bytes(self.slots.at[:, self.rows], self.sems[10])

    def begin(self):
        self.start(1, 3, 0, 2, 4)

    def relay_first(self):
        self.arrived(1)
        self.start(5, 7)
        if self.direct:
            self.start(11)
        self.arrived(3)
        self.start(6, 10)
        if self.direct:
            self.start(12)

    def relay_second(self):
        self.arrived(2)
        self.start(8)
        self.arrived(4)
        self.start(9)

    def relay(self):
        self.relay_first()
        self.relay_second()

    def relay_last(self):
        self.arrived(5)
        if not self.direct:
            self.start(11)
        self.arrived(6)
        if not self.direct:
            self.start(12)


def layer_kernel(
    tok_hbm, lru_w_hbm, gate_w_hbm, query_w_hbm, key_w_hbm, value_w_hbm,
    conv_ref, recur_hbm, input_hbm, rate_ref, extra_hbm, f_ref, out_lru_ref, out_fox_ref,
    o_ref,
    tok_ref, recur_ref, input_ref, extra_ref, weights, tokg, acc_kv, acc_rest, scores_a, scores_b, squares,
    kv, qb, bias, m_ref, acc, o_send, st_send, o_relay, o_recv, st_recv,
    lru_own, halo, gate_own, decays, drives, row_tiles, col_tiles,
    lru_out, lru_g, fox_out, fox_g, w_out, acc_out, out_rows,
    copy_sems, load_sems, alive,
):
    sp, tp = lax.axis_index("sp"), lax.axis_index("tp")
    z, x = lax.div(sp, XS), lax.rem(sp, XS)
    y, c = lax.div(tp, 2), lax.rem(tp, 2)
    above = lax.rem(z + 1, ZS) * XS + x
    below = lax.rem(z + ZS - 1, ZS) * XS + x
    partner = y * 2 + 1 - c

    def along_y(r, core):
        return lax.rem(y + r, YS) * 2 + core

    def along_x(r):
        return z * XS + lax.rem(x + r, XS)

    def along_z(r):
        return lax.rem(z + r, ZS) * XS + x

    following, preceding = lax.rem(sp + 1, SP), lax.rem(sp + SP - 1, SP)
    used = [0]

    def semaphore():
        used[0] += 1
        return copy_sems.at[used[0] - 1]

    def copy(src, dst, send=None, recv=None, **where):
        return pltpu.make_async_remote_copy(
            src_ref=src, dst_ref=dst, send_sem=send or semaphore(), recv_sem=recv or semaphore(),
            device_id=where, device_id_type=MESH,
        )

    gather_sems = [[semaphore() for k in range(11)] for group in range(3)]

    tok_load = pltpu.make_async_copy(tok_hbm, tok_ref, load_sems.at[1])
    tok_load.start()
    loads = [
        pltpu.make_async_copy(w, weights.at[i], load_sems.at[0])
        for i, w in enumerate((key_w_hbm, value_w_hbm, lru_w_hbm, query_w_hbm, gate_w_hbm))
    ]
    own_blocks = pl.ds(2 * tp, 2)
    own_columns = pl.ds(pl.multiple_of(tp * OUT, OUT), OUT)
    later_loads = [
        pltpu.make_async_copy(extra_hbm, extra_ref, load_sems.at[2]),
        pltpu.make_async_copy(recur_hbm.at[own_blocks], recur_ref, load_sems.at[3]),
        pltpu.make_async_copy(input_hbm.at[own_blocks], input_ref, load_sems.at[4]),
        pltpu.make_async_copy(out_lru_ref.at[:, own_columns], w_out.at[0, tp], load_sems.at[5]),
        pltpu.make_async_copy(out_fox_ref.at[:, own_columns], w_out.at[1, tp], load_sems.at[6]),
    ]
    for load in loads + later_loads:
        load.start()

    barrier = pltpu.get_barrier_semaphore()

    def tell(semaphore, **where):
        pl.semaphore_signal(semaphore, inc=1, device_id=where, device_id_type=MESH)

    for r in range(1, TP):
        tell(barrier, tp=lax.rem(tp + r, TP))
    for r in range(1, XS):
        tell(barrier, sp=along_x(r))
    for r in range(1, ZS):

        @pl.when(z + r < ZS)
        def _():
            tell(barrier, sp=along_z(r))

    last_of_row = (x == XS - 1) & (z < ZS - 1)
    first_of_row = (x == 0) & (z > 0)

    @pl.when(last_of_row)
    def _():
        tell(barrier, sp=following)

    pl.semaphore_wait(barrier, TP - 1 + XS - 1 + z + first_of_row.astype(jnp.int32))
    for r in range(1, ZS):

        @pl.when(z >= r)
        def _():
            tell(alive, sp=along_z(ZS - r))

    @pl.when(first_of_row)
    def _():
        tell(alive, sp=preceding)

    tokens = [
        Gather(copy, gather_sems[h], tok_ref, tokg, along_y(1, c), along_y(3, c), partner, h * HALF, HALF) for h in (0, 1)
    ]
    tok_load.wait()
    tokens[0].begin()
    forget = f_ref[...]
    high = forget.astype(jnp.bfloat16).astype(jnp.float32)
    middle = (forget - high).astype(jnp.bfloat16).astype(jnp.float32)
    low = forget - high - middle
    for h in (0, 1):
        lines = [part[2 * h : 2 * h + 2] for part in (high, middle, low)]
        kv[h, HALF:HROWS, :] = jnp.concatenate(
            lines + [jnp.zeros((10, 128), jnp.float32)], axis=0
        ).astype(jnp.bfloat16)

    def features(r, core):
        return pl.ds(pl.multiple_of(along_y(r, core) * FEAT, FEAT), FEAT)

    def pair(slot, h):
        rows = pl.ds(h * HALF, HALF)
        block = tok_ref if slot == 0 else tokg.at[slot]
        other = tokg.at[0] if slot == 0 else tokg.at[slot + 3]
        return block[rows, :], other[rows, :]

    distance = {0: 0, 1: 3, 2: 1, 3: 2}

    def project(slot, h, group, target):
        rows = [features(distance[slot], c), features(distance[slot], 1 - c)]
        right = jnp.concatenate(
            [jnp.concatenate([weights[i, part, :] for part in rows], axis=0) for i in group], axis=1
        )
        product = dot(jnp.concatenate(pair(slot, h), axis=1), right)
        half = pl.ds(h * HALF, HALF)
        target[half, :] = product if slot == 0 else target[half, :] + product

    def count_squares(slot, h):
        half = pl.ds(h * HALF, HALF)
        total = jnp.zeros((HALF, 128), jnp.float32) if slot == 0 else squares[half, :]
        for piece in pair(slot, h):
            for g in range(FEAT // 128):
                value = piece[:, g * 128 : (g + 1) * 128].astype(jnp.float32)
                total = total + value * value
        squares[half, :] = total

    def take(slot, h):
        project(slot, h, (0, 1, 2), acc_kv)
        project(slot, h, (3, 4), acc_rest)
        count_squares(slot, h)

    plus = [(0, 2), (1, 3), (2, 4), (3, 5), (4, 6), (5, 7)]
    minus = [(0, 8), (1, 9), (8, 10), (9, 11), (10, 12), (11, 13), (12, 14), (13, 15)]
    plus_sent, minus_sent = semaphore(), semaphore()
    plus = [copy(kv.at[a], kv.at[b], plus_sent, sp=above) for a, b in plus]
    minus = [copy(kv.at[a], kv.at[b], minus_sent, sp=below) for a, b in minus]

    def wrapped(d):
        return lax.rem(z + d, ZS) < 4

    def send_plus(i):
        @pl.when((z < ZS - 1) & (z >= i // 2))
        def _():
            plus[i].start()

    def send_minus(i):
        @pl.when(wrapped(i // 2))
        def _():
            minus[i].start()

    last_row = z == ZS - 1

    def receive_plus(i, where=True):
        d = i // 2 + 1

        @pl.when((z >= d) & where)
        def _():
            plus[i].wait_recv()

        if d < 3:

            @pl.when((z < ZS - 1) & (z >= d) & where)
            def _():
                plus[i + 2].start()

    def receive_minus(i, where=True):
        d = i // 2 + 1

        @pl.when(wrapped(d) & where)
        def _():
            minus[i].wait_recv()
            if d < 4:
                minus[i + 2].start()

    tail = copy(lru_own.at[pl.ds(BLK - 16, 16)], halo, sp=following)
    query_rows = [pl.ds(pl.multiple_of(x * BLK + h * HALF, HALF), HALF) for h in (0, 1)]
    query_sems = semaphore(), semaphore()
    query_copies = [
        {r: copy(qb.at[rows], qb.at[rows], *query_sems, sp=along_x(r)) for r in (1, 2, 3)} for rows in query_rows
    ]
    others_queries = qb.at[pl.ds(0, (XS - 1) * BLK)]

    def conclude(h):
        half = pl.ds(h * HALF, HALF)
        count_squares(3, h)
        row_scale = lax.rsqrt(
            jnp.sum(squares[half, :], axis=1, keepdims=True) * (1.0 / D) + epsilon_norm
        )
        project(3, h, (0, 1, 2), acc_kv)
        ready = (acc_kv[half, :] * row_scale).astype(jnp.bfloat16)
        lru_own[half, :] = ready[:, 256:]
        if h == 0:
            later = (ZS - 1 - z) + last_of_row.astype(jnp.int32)

            @pl.when(later > 0)
            def _():
                pl.semaphore_wait(alive, later)

        else:

            @pl.when(sp < SP - 1)
            def _():
                tail.start()

        kv[h, :HALF, :] = ready[:, :128]
        kv[h, HROWS:, :] = ready[:, 128:256]
        send_plus(h)
        send_minus(h)
        project(3, h, (3, 4), acc_rest)
        rest = (acc_rest[half, :] * row_scale).astype(jnp.bfloat16)
        qb[query_rows[h], :] = rest[:, :128]
        gate_own[half, :] = rest[:, 128:]
        for r in (1, 3, 2):
            query_copies[h][r].start()

    await_bytes(weights, load_sems.at[0])
    early, late = tokens
    early.arrived(0)
    take(0, 0)
    early.relay_first()
    late.begin()
    early.relay_second()
    early.arrived_from_partner(4)
    take(1, 0)
    early.arrived_from_partner(5)
    take(2, 0)
    early.relay_last()
    late.arrived(0)
    take(0, 1)
    late.relay_first()
    early.arrived_from_partner(6)
    conclude(0)
    late.relay_second()
    late.arrived_from_partner(4)
    take(1, 1)
    late.arrived_from_partner(5)
    take(2, 1)
    receive_minus(0, last_row)
    late.relay_last()
    late.arrived_from_partner(6)
    conclude(1)

    for group in tokens:
        group.finish()

    weight_sems = semaphore(), semaphore()
    weight_copies = []
    for r in range(1, TP):
        to = lax.rem(tp + r, TP)
        columns = pl.ds(pl.multiple_of(to * OUT, OUT), OUT)
        for k, ref in enumerate((out_lru_ref, out_fox_ref)):
            weight_copies.append(copy(ref.at[:, columns], w_out.at[k, tp], *weight_sems, tp=to))
    for each in weight_copies:
        each.start()
    others_weights = w_out.at[:, pl.ds(0, TP - 1)]
    own_rows = pl.ds(pl.multiple_of(x * BLK, BLK), BLK)
    m_ref[...] = jnp.full_like(m_ref, NEG)
    acc[...] = jnp.zeros_like(acc)

    def set_bias(slot):
        parts = kv[slot, HALF:HROWS, :].astype(jnp.float32)
        whole = parts[0:2] + parts[2:4] + parts[4:6]
        for g in range(2):
            bias[slot : slot + 1, g * 128 : (g + 1) * 128] = whole[g : g + 1] * -LOG2E

    scale = HEAD_DIM ** (-0.5) * LOG2E

    def joint(parts, axis):
        return parts[0] if len(parts) == 1 else jnp.concatenate(parts, axis=axis)

    def score(buffer, i, slots):
        rows = pl.ds(i * BLK if isinstance(i, int) else pl.multiple_of(i * BLK, BLK), BLK)
        buffer[:, : HALF * len(slots)] = lax.dot_general(
            qb[rows, :],
            joint([kv[slot, :HALF, :] for slot in slots], 0),
            (((1,), (1,)), ((), ())),
            preferred_element_type=jnp.float32,
        )

    def absorb(buffer, i, slots, masked=False):
        width = HALF * len(slots)
        offsets = joint([bias[slot : slot + 1, :] for slot in slots], 1)
        values = joint([kv[slot, HROWS:, :] for slot in slots], 0)
        values = jnp.concatenate([values, jnp.ones_like(values)], axis=1)
        start = i * BLK if isinstance(i, int) else pl.multiple_of(i * BLK, BLK)
        for part in range(0, BLK, ROWS):
            rows = pl.ds(start + part, ROWS)
            scores = buffer[part : part + ROWS, :width] * scale + offsets
            if masked:
                earlier = lax.broadcasted_iota(jnp.int32, scores.shape, 0) + part >= (
                    lax.broadcasted_iota(jnp.int32, scores.shape, 1)
                )
                scores = jnp.where(earlier, scores, NEG)
            old = m_ref[rows, :]
            new = jnp.maximum(old, jnp.max(scores, axis=1, keepdims=True))
            rescale = jnp.exp2(old - new)
            probs = jnp.exp2(scores - jnp.concatenate([new] * (width // 128), axis=1))
            m_ref[rows, :] = new
            acc[rows, :] = acc[rows, :] * jnp.concatenate([rescale] * 2, axis=1) + dot(
                probs.astype(jnp.bfloat16), values
            )

    def attend(i, slots, masked=False):
        score(scores_a, i, slots)
        absorb(scores_a, i, slots, masked)

    def visit_rest(slots, first):
        def body(i, carry):
            attend(i, slots)
            return carry

        lax.fori_loop(first, XS, body, 0)

    def visit(*slots):
        for slot in slots:
            set_bias(slot)
        score(scores_a, 0, slots)
        pair = scores_a, scores_b
        for k in range(XS):
            if k + 1 < XS:
                score(pair[(k + 1) % 2], k + 1, slots)
            absorb(pair[k % 2], k, slots)

    def take_keys(i):
        d = i // 2 + 1
        @pl.when(z + d >= ZS)
        def _():
            visit(i + 2, i + 8)

        @pl.when((z >= d) & (z + d < ZS))
        def _():
            visit(i + 2)

    set_bias(0)
    set_bias(1)
    attend(x, (0, 1), masked=True)
    receive_plus(0)
    receive_minus(0, z < ZS - 1)
    receive_minus(1, last_row)

    @pl.when(sp > 0)
    def _():
        tail.wait_recv()

    @pl.when(sp == 0)
    def _():
        halo[...] = jnp.zeros_like(halo)

    for load in later_loads:
        load.wait()
    lru_input = lru_own[...].astype(jnp.float32)
    before = halo[8:16, :].astype(jnp.float32)
    joined = jnp.concatenate([before, lru_input], axis=0)
    channels = pl.ds(pl.multiple_of(tp * 128, 128), 128)
    taps = conv_ref[:, channels].astype(jnp.float32)
    conv = jnp.zeros((BLK, 128), jnp.float32)
    for j in range(4):
        shifted = joined if j == 3 else pltpu.roll(joined, 3 - j, 0)
        conv = conv + taps[j : j + 1, :] * shifted[8:, :]
    conv = conv.astype(jnp.bfloat16)
    column = lax.broadcasted_iota(jnp.int32, (64, 128), 1)
    row = lax.broadcasted_iota(jnp.int32, (64, 128), 0)
    left = jnp.where(column == row, 1.0, 0.0).astype(jnp.bfloat16)
    right = jnp.where(column == row + 64, 1.0, 0.0).astype(jnp.bfloat16)

    def block_diagonal(ref):
        return jnp.concatenate([dot(ref[0], left), dot(ref[1], right)], axis=0)

    gates_w = jnp.concatenate([block_diagonal(recur_ref), block_diagonal(input_ref)], axis=1)
    gates = dot(conv, gates_w.astype(jnp.bfloat16))
    gates = 1.0 / (1.0 + jnp.exp(-gates))
    rate = log1p_unit(jnp.exp(-rate_ref[pl.ds(tp, 1), :]))
    log_decay = (-decay_sharpness * rate) * gates[:, :128] + extra_ref[...]
    drive = jnp.sqrt(minus_expm1(2.0 * log_decay)) * gates[:, 128:] * conv.astype(jnp.float32)
    decay = jnp.exp(log_decay)
    place = lax.broadcasted_iota(jnp.int32, (BLK, 128), 0)
    step = 1
    while step < BLK:
        if step < 8:
            inside = place >= step
            decay_back = jnp.where(inside, pltpu.roll(decay, step, 0), 1.0)
            drive_back = jnp.where(inside, pltpu.roll(drive, step, 0), 0.0)
        else:
            decay_back = jnp.concatenate([jnp.ones((step, 128), jnp.float32), decay[:-step]], axis=0)
            drive_back = jnp.concatenate([jnp.zeros((step, 128), jnp.float32), drive[:-step]], axis=0)
        drive = decay * drive_back + drive
        decay = decay * decay_back
        step *= 2
    decays[...] = decay
    drives[...] = drive

    def tile_of(a, b):
        return jnp.concatenate([a, b, jnp.zeros((6, 128), jnp.float32)], axis=0)

    row_tiles[0] = tile_of(decays[BLK - 1 :, :], drives[BLK - 1 :, :])
    row_sems = semaphore(), semaphore()
    row_copies = {
        r: copy(row_tiles.at[0], row_tiles.at[r], *row_sems, sp=along_x(r)) for r in (1, 2, 3)
    }
    others_rows = row_tiles.at[pl.ds(1, XS - 1)]
    for r in (1, 3, 2):
        row_copies[r].start()

    receive_minus(1, z < ZS - 1)
    receive_plus(1, z < ZS - 1)
    receive_minus(2, z >= ZS - 2)
    await_bytes(others_queries, query_sems[1])
    visit_rest((0, 1), x + 1)

    columns_sent = semaphore()
    column_copies = {
        r: copy(col_tiles.at[0], col_tiles.at[r], columns_sent, sp=along_z(r)) for r in range(1, ZS)
    }
    branch = Gather(copy, gather_sems[0], lru_out, lru_g, along_y(1, c), along_y(3, c), partner)
    one, zero = jnp.ones((1, 128), jnp.float32), jnp.zeros((1, 128), jnp.float32)

    def total_of_row():
        await_bytes(others_rows, row_sems[1])
        whole_decay, whole_state, state = one, zero, zero
        for k in range(XS):
            block = row_tiles[lax.rem(x + XS - k, XS)]
            a, b = block[0:1], block[1:2]
            state = jnp.where(k < x, a * state + b, state)
            whole_state = a * whole_state + b
            whole_decay = whole_decay * a
        col_tiles[0] = tile_of(whole_decay, whole_state)
        for r in range(1, ZS):

            @pl.when(z + r < ZS)
            def _():
                column_copies[r].start()

    def recurrence_out():
        for r in range(1, ZS):

            @pl.when(z >= r)
            def _():
                column_copies[r].wait_recv()

        def row_above(k, state):
            block = col_tiles[z - k]
            return block[0:1] * state + block[1:2]

        state = lax.fori_loop(0, z, row_above, zero)
        for k in range(XS):
            block = row_tiles[lax.rem(x + XS - k, XS)]
            state = jnp.where(k < x, block[0:1] * state + block[1:2], state)
        gate = gate_own[...].astype(jnp.float32)
        inner = 0.7978845608028654 * (gate + 0.044715 * gate * gate * gate)
        gelu = 0.5 * gate * (1.0 + jnp.tanh(inner))
        lru_out[...] = ((drives[...] + decays[...] * state) * gelu).astype(jnp.bfloat16)
        branch.begin()

    beside = {0: total_of_row, 2: recurrence_out, 4: branch.relay}
    receive_minus(2, z < ZS - 2)
    for i in range(6):
        take_keys(i)
        if i in beside:
            beside[i]()
        if i == 0:
            receive_plus(1, last_row)
        if i < 4:
            receive_plus(i + 2)
        if i < 5:
            receive_minus(i + 3)

    right, left = along_x(1), along_x(3)
    out_sent, out_sent_on = semaphore(), semaphore()
    relay_sems, out_sems = [semaphore(), semaphore()], [semaphore(), semaphore()]
    out_copies = []
    for h in (0, 1):
        rows = pl.ds(h * HALF, HALF)
        quarters = [pl.ds(h * HALF + k * 128, 128) for k in (0, 1)]
        out_copies.append(
            {
                "relay": [
                    copy(o_send.at[2, part], o_relay.at[k, part], out_sent, relay_sems[h], sp=to)
                    for k, (part, to) in enumerate(zip(quarters, (right, left)))
                ],
                "near": {
                    r: copy(o_send.at[r, rows], o_recv.at[r, rows], out_sent, out_sems[h], sp=along_x(r))
                    for r in (1, 3)
                },
                "far": [
                    copy(o_relay.at[k, part], o_recv.at[2, part], out_sent_on, out_sems[h], sp=to)
                    for k, (part, to) in enumerate(zip(quarters, (right, left)))
                ],
            }
        )
    stat_sems = semaphore(), semaphore()
    stat_copies = {r: copy(st_send.at[r], st_recv.at[r], *stat_sems, sp=along_x(r)) for r in (1, 2, 3)}
    others_stats = st_recv.at[pl.ds(1, XS - 1)]

    def stats(rows):
        return packed_rows(m_ref[rows, :]), packed_rows(acc[rows, 128:])

    def relay_on(h):
        await_bytes(o_relay.at[0, pl.ds(0, HALF)], relay_sems[h])
        for each in out_copies[h]["far"]:
            each.start()

    def block_of(r):
        return lax.rem(x + r, XS)

    @pl.when(z >= 4)
    def _():
        set_bias(14)
        set_bias(15)
        score(scores_a, block_of(2), (14, 15))

    buffers = (scores_a, scores_b)
    turns = (2, 1, 3, 0)
    for k, r in enumerate(turns):

        @pl.when(z >= 4)
        def _():
            if k + 1 < len(turns):
                score(buffers[(k + 1) % 2], block_of(turns[k + 1]), (14, 15))
            absorb(buffers[k % 2], block_of(r), (14, 15))

        if r > 0:
            rows = pl.ds(pl.multiple_of(block_of(r) * BLK, BLK), BLK)
            st_send[r] = jnp.concatenate(stats(rows), axis=0)
            stat_copies[r].start()
            o_send[r] = acc[rows, :128].astype(jnp.bfloat16)
            if r == 2:
                for h in (0, 1):
                    for each in out_copies[h]["relay"]:
                        each.start()
            else:
                for h in (0, 1):
                    out_copies[h]["near"][r].start()
    tops, sums = [None] * 4, [None] * 4
    tops[0], sums[0] = stats(own_rows)
    branch.relay_last()

    relay_on(0)

    sources = [(0, c), (0, 1 - c), (3, c), (3, 1 - c), (1, c), (1, 1 - c), (2, c), (2, 1 - c)]

    def branch_product(k, own, slots, which, rows):
        lookup = [None, 0, 1, 4, 2, 5, 3, 6]
        blocks = [own[rows, :] if lookup[i] is None else slots[lookup[i], rows, :] for i in which]
        rights = [w_out[k, along_y(*sources[i])] for i in which]
        return dot(jnp.concatenate(blocks, axis=1), jnp.concatenate(rights, axis=0))

    await_bytes(others_weights, weight_sems[1])
    branch.arrived(0)
    branch.arrived_from_partner(4, 5, 6)
    relay_on(1)
    acc_out[...] = branch_product(0, lru_out, lru_g, range(8), pl.ds(0, BLK))

    await_bytes(others_stats, stat_sems[1])
    for r in (1, 2, 3):
        both = st_recv[r]
        tops[r], sums[r] = both[0:4], both[4:8]
    top = jnp.maximum(jnp.maximum(tops[0], tops[1]), jnp.maximum(tops[2], tops[3]))
    shares = [jnp.exp2(t - top) for t in tops]
    whole = shares[0] * sums[0] + shares[1] * sums[1] + shares[2] * sums[2] + shares[3] * sums[3]
    shares = [s / whole for s in shares]
    heads = [
        Gather(
            copy, gather_sems[1 + h], fox_out, fox_g, along_y(1, c), along_y(3, c), partner, h * HALF, HALF,
            last=(along_y(1, 1 - c), along_y(3, 1 - c)),
        )
        for h in (0, 1)
    ]

    def merge(h):
        await_bytes(qb.at[pl.ds(0, (XS - 1) * HALF)], out_sems[h])
        for g in (2 * h, 2 * h + 1):
            part = pl.ds(g * 128, 128)
            mine = pl.ds(pl.multiple_of(x * BLK + g * 128, 128), 128)
            total = unpacked_row(shares[0][g : g + 1]) * acc[mine, :128]
            for r in (1, 2, 3):
                total = total + unpacked_row(shares[r][g : g + 1]) * o_recv[r, part, :].astype(jnp.float32)
            fox_out[part, :] = total.astype(jnp.bfloat16)
        heads[h].begin()

    def head_product(h, which):
        rows = pl.ds(h * HALF, HALF)
        return branch_product(1, fox_out, fox_g, which, rows)

    halves = [pl.ds(h * HALF, HALF) for h in (0, 1)]
    out_loads = [
        pltpu.make_async_copy(out_rows.at[half], o_ref.at[half], load_sems.at[7 + h])
        for h, half in enumerate(halves)
    ]

    def write(h):
        heads[h].arrived_from_partner(6)
        out_rows[halves[h], :] = (acc_out[halves[h], :] + head_product(h, (6, 7))).astype(out_rows.dtype)
        out_loads[h].start()

    merge(0)
    merge(1)
    heads[0].relay()
    heads[0].arrived(0)
    acc_out[halves[0], :] += head_product(0, (0, 1))
    heads[1].relay_first()
    heads[0].relay_last()
    heads[1].relay_second()
    heads[1].arrived(0)
    acc_out[halves[1], :] += head_product(1, (0, 1))
    heads[0].arrived_from_partner(4, 5)
    acc_out[halves[0], :] += head_product(0, (2, 3, 4, 5))
    write(0)
    heads[1].relay_last()
    heads[1].arrived_from_partner(4, 5)
    acc_out[halves[1], :] += head_product(1, (2, 3, 4, 5))
    write(1)

    for n in (1, 2, 3):

        @pl.when((z < ZS - 1) & (jnp.minimum(z + 1, 3) == n))
        def _():
            await_bytes(kv.at[pl.ds(0, 2 * n)], plus_sent)

    for n in (1, 2, 3, 4):

        @pl.when((z == 4 - n) | (z == 4 + n))
        def _():
            await_bytes(kv.at[pl.ds(0, 2 * n)], minus_sent)

    @pl.when(sp < SP - 1)
    def _():
        tail.wait_send()

    for n in range(1, ZS):

        @pl.when(z == ZS - 1 - n)
        def _():
            await_bytes(col_tiles.at[pl.ds(0, n)], columns_sent)

    await_bytes(others_weights, weight_sems[0])
    await_bytes(others_queries, query_sems[0])
    await_bytes(others_rows, row_sems[0])
    await_bytes(others_stats, stat_sems[0])
    await_bytes(o_recv.at[pl.ds(1, XS - 1)], out_sent)
    await_bytes(o_relay.at[0], out_sent_on)
    for group in [branch] + heads:
        group.finish()
    for each in out_loads:
        each.wait()


def layer(
    tokens, lru_in, lru_gate_in, query_w, key_w, value_w, conv_weight, recur_gate_w, input_gate_w,
    rate_param, decay_extra, forget_cum, out_lru, out_fox,
):
    vmem = pl.BlockSpec(memory_space=pltpu.VMEM)
    hbm = pl.BlockSpec(memory_space=pl.ANY)
    bf16, f32 = jnp.bfloat16, jnp.float32
    return pl.pallas_call(
        layer_kernel,
        out_shape=pltpu.VMEM((BLK, OUT), f32),
        in_specs=[hbm] * 6 + [vmem, hbm, hbm, vmem, hbm, vmem, hbm, hbm],
        out_specs=hbm,
        scratch_shapes=[
            pltpu.VMEM((BLK, FEAT), bf16),
            pltpu.VMEM((2, 64, 64), bf16),
            pltpu.VMEM((2, 64, 64), bf16),
            pltpu.VMEM((BLK, 128), f32),
            pltpu.VMEM((5, D, 128), bf16),
            pltpu.VMEM((7, BLK, FEAT), bf16),
            pltpu.VMEM((BLK, 384), f32),
            pltpu.VMEM((BLK, 256), f32),
            pltpu.VMEM((BLK, BLK), f32),
            pltpu.VMEM((BLK, BLK), f32),
            pltpu.VMEM((BLK, 128), f32),
            pltpu.VMEM((2 * ZS, PIECE, 128), bf16),
            pltpu.VMEM((XS * BLK, 128), bf16),
            pltpu.VMEM((2 * ZS, HALF), f32),
            pltpu.VMEM((XS * BLK, 128), f32),
            pltpu.VMEM((XS * BLK, 256), f32),
            pltpu.VMEM((XS, BLK, 128), bf16),
            pltpu.VMEM((XS, 8, 128), f32),
            pltpu.VMEM((2, BLK, 128), bf16),
            pltpu.VMEM((XS, BLK, 128), bf16),
            pltpu.VMEM((XS, 8, 128), f32),
            pltpu.VMEM((BLK, 128), bf16),
            pltpu.VMEM((16, 128), bf16),
            pltpu.VMEM((BLK, 128), bf16),
            pltpu.VMEM((BLK, 128), f32),
            pltpu.VMEM((BLK, 128), f32),
            pltpu.VMEM((XS, 8, 128), f32),
            pltpu.VMEM((ZS, 8, 128), f32),
            pltpu.VMEM((BLK, 128), bf16),
            pltpu.VMEM((7, BLK, 128), bf16),
            pltpu.VMEM((BLK, 128), bf16),
            pltpu.VMEM((7, BLK, 128), bf16),
            pltpu.VMEM((2, TP, 128, OUT), bf16),
            pltpu.VMEM((BLK, OUT), f32),
            pltpu.VMEM((BLK, OUT), f32),
            pltpu.SemaphoreType.DMA((COPIES,)),
            pltpu.SemaphoreType.DMA((9,)),
            pltpu.SemaphoreType.REGULAR,
        ],
        compiler_params=pltpu.CompilerParams(collective_id=1, has_side_effects=True),
        cost_estimate=pl.CostEstimate(flops=5_000_000_000, bytes_accessed=8_000_000, transcendentals=9_000_000),
    )(
        tokens, lru_in, lru_gate_in, query_w, key_w, value_w, conv_weight, recur_gate_w, input_gate_w,
        rate_param.reshape(TP, 128), decay_extra, forget_cum.reshape(4, 128), out_lru, out_fox,
    ).astype(bf16)


def solution(mesh):
    placed = (
        P("sp", "tp"),
        P(None, "tp"),
        P(None, "tp"),
        P(None, "tp"),
        P(None, "tp"),
        P(None, "tp"),
        P(),
        P(),
        P(),
        P(),
        P("sp", "tp"),
        P("sp", "tp"),
        P("tp", None),
        P("tp", None),
    )
    return jax.shard_map(
        layer, mesh=mesh, in_specs=placed, out_specs=P("sp", "tp"), check_vma=False
    )
```
